256 devices in a mesh: ep: 64 (over z, x, core), tp: 4 (over y).
Axes of the slice: x: 4, y: 4, z: 8, core: 2. Of those that a mesh axis runs over, the one named last changes fastest.
Arguments:
- receptance: bfloat16 [32768, 2048], P('ep', 'tp'), may hold values from -6 to 6
- key_rows: bfloat16 [32768, 2048], P('ep', 'tp'), may hold values from -6 to 6
- value_rows: bfloat16 [32768, 2048], P('ep', 'tp'), may hold values from -6 to 6
- decay_input: bfloat16 [32768, 2048], P('ep', 'tp'), may hold values from -2.796875 to 2.796875
- learn_input: bfloat16 [32768, 2048], P('ep', 'tp'), may hold values from -12 to 4
- decay_base: float32 [2048], P('tp'), may hold values from -20 to -2
- decay_shift: float32 [32768, 32], P('ep', 'tp'), may hold values from -1 to 20
- channel_gain: float32 [2048], P('tp'), may hold values from 0.1 to 1.9
- out_weight: bfloat16 [2048, 2048], P('tp'), may hold values from -0.125 to 0.125
- expert_input: bfloat16 [32768, 2048], P(('ep', 'tp')), may hold values from -6 to 6
- expert_gain: float32 [2048], replicated, may hold values from 0.1 to 1.9
- routes: int32 [32768, 2], P(('ep', 'tp')), may hold values from 0 to 63, all different within a row; in each aligned block of 128 rows (0 to 127, 128 to 255, ...) at most 8 rows name the same one
- route_weight: float32 [32768, 2], P(('ep', 'tp')), may hold values from 0.1 to 1
- gate_weight: bfloat16 [64, 2048, 1024], P('ep', None, 'tp'), may hold values from -0.125 to 0.125
- up_weight: bfloat16 [64, 2048, 1024], P('ep', None, 'tp'), may hold values from -0.125 to 0.125
- down_weight: bfloat16 [64, 1024, 2048], P('ep', 'tp'), may hold values from -0.1875 to 0.1875
Outputs:
- mixer_out: bfloat16 [32768, 2048], P(('ep', 'tp'))
- expert_out: bfloat16 [32768, 2048], P(('ep', 'tp'))
The draws below stay inside these ranges and needn't reach their ends.
Inputs may be any that keep to these rules, and one draw needn't show every extreme that they name: `routes`: within the rows of one device (aligned blocks of 128 rows) no expert is named by more than 8 rows, and in every draw some block names some expert exactly 8 times. Each row names 2 different experts.
All inputs are finite; a program needn't handle non-finite values.
Results may differ from the reference program's by a relative error of at most 0.024.
Values may be sent and summed in bfloat16 or wider, within the bound.
No kernel may reach another device: no remote copies, remote signals or barrier semaphores. Data moves between devices by JAX's collectives and lax.ppermute only.
A program may use at most 128 MiB of HBM per device.

```python
import math
import jax
import jax.numpy as jnp
import numpy as np
from jax import lax

D = 2048
HEADS = 32
HEAD = 64
CHANNELS = 2048
FF = 1024
EXPERTS = 64
TOPK = 2
TOK_DEV = 128
MIX_ROWS = 512
MICRO_TOKENS = 32768
CAP = 8
N_TP = 4


def fast_heads(key):
    ranking = jax.random.permutation(jax.random.fold_in(key, 101), HEADS)
    quick_count = HEADS // 2
    return jnp.repeat(ranking < quick_count, HEAD)


def draw_decay_base(key, part):
    quick = fast_heads(key)
    spread = jax.random.uniform(jax.random.fold_in(key, 102), (CHANNELS,), jnp.float32)
    slow_rates = -jnp.log(jnp.float32(MICRO_TOKENS)) - 2.0 - spread
    quick_rates = -3.9 + 1.3 * spread
    return jnp.where(quick, quick_rates, slow_rates).astype(jnp.float32)


def draw_decay_shift(key, part):
    blocks = MICRO_TOKENS // MIX_ROWS
    reach = 0.5
    levels = jax.random.uniform(jax.random.fold_in(key, 103), (blocks, HEADS), jnp.float32, -reach, reach)
    each_row_amount = jnp.repeat(levels, MIX_ROWS, axis=0)
    surge_locations = jax.random.randint(jax.random.fold_in(key, 104), (3,), 0, MICRO_TOKENS)
    surge_groups = jnp.any(jnp.arange(MICRO_TOKENS, dtype=jnp.int32)[:, None] == surge_locations[None, :], axis=1)
    table_height = jnp.log(jnp.float32(MICRO_TOKENS)) + 3.0
    return (each_row_amount + jnp.where(surge_groups, table_height, 0.0)[:, None]).astype(jnp.float32)


def draw_learn_input(key, part):
    quick = fast_heads(key)
    slow_mean = -jnp.log(jnp.float32(MICRO_TOKENS) / HEAD) - 1.0
    centre = jnp.where(quick, 0.0, slow_mean)
    jitter = jnp.clip(jax.random.normal(jax.random.fold_in(key, 105), (MICRO_TOKENS, CHANNELS), jnp.float32), -3.0, 3.0)
    return (centre[None, :] + jitter).astype(jnp.bfloat16)


def block_scale(own_key, shape, cuts, smallest, top_value):
    factor_of = 1.0
    for dim, shards_of in cuts:
        draws = jax.random.uniform(jax.random.fold_in(jax.random.fold_in(own_key, 6), dim), (shards_of,), jnp.float32, smallest / len(cuts), top_value / len(cuts))
        factor_of = factor_of * jnp.repeat(jnp.exp(draws), shape[dim] // shards_of).reshape((-1,) + (1,) * (len(shape) - 1 - dim))
    return factor_of


def assign_block(own_key, own, number, rows, count, top, most, lean):
    sequence = jax.random.permutation(own_key, count)
    packed, ordinary = load_shares(count, rows * top, most, lean, True), load_shares(count, rows * top, most, lean, False)
    places = jnp.arange(count)

    def named(lengths, turn):
        used = int((lengths > 0).sum())
        fixed = max(1, used // 4)
        shifted = fixed + (places - fixed + turn * (used - fixed)) % max(1, count - fixed)
        return jnp.zeros((count,), jnp.int32).at[sequence[jnp.where(places < fixed, places, shifted)]].set(jnp.asarray(lengths, jnp.int32))

    lengths = jnp.where(number % 4 == 0, named(packed, number // 4), named(ordinary, number - number // 4 - 1))
    mixed = jax.random.permutation(jax.random.fold_in(own, 3), count)
    giver, sink = mixed[0:count // 2 * 2:2], mixed[1:count // 2 * 2:2]
    slack = jnp.minimum(lengths[giver] - 1, most - lengths[sink]) // 2
    slack = jnp.where((giver == sequence[0]) | (sink == sequence[0]) | (lengths[sink] == 0), 0, jnp.maximum(slack, 0))
    shifted = jax.random.randint(jax.random.fold_in(own, 4), (count // 2,), 0, 1 << 20) % (slack + 1)
    lengths = lengths.at[giver].add(-shifted).at[sink].add(shifted)
    items = jnp.searchsorted(jnp.cumsum(lengths), jnp.arange(rows * top), side="right").astype(jnp.int32)
    listing = items.reshape(top, rows).T
    listing = listing[jax.random.permutation(jax.random.fold_in(own, 1), rows)]
    turn = jax.random.randint(jax.random.fold_in(own, 2), (rows, 1), 0, top)
    return jnp.take_along_axis(listing, (jnp.arange(top)[None, :] + turn) % top, axis=1)


def load_shares(number_of, total, most, lean, full):
    loads = [(1 << 20) // math.isqrt(grade ** lean) + 1 for grade in range(1, number_of + 1)]
    largest = most if full else min(most, max(-(-total // number_of), total * loads[0] // sum(loads)))
    least = 1 if total - largest >= number_of - 1 else 0
    given, rest = [largest] + [least] * (number_of - 1), total - largest - least * (number_of - 1)
    while rest > 0:
        free = [i for i in range(1, number_of) if given[i] < largest] or [i for i in range(1, number_of) if given[i] < most]
        mass, left = sum([loads[i] for i in free]), rest
        for i in free:
            addition = min(most - given[i], max(1, left * loads[i] // mass), rest)
            given[i] = given[i] + addition
            rest = rest - addition
    return np.array(given)


def noise(own_key, dims, deviation, limit, pieces=(), held_as=jnp.bfloat16):
    entries = deviation * jax.random.normal(own_key, dims, jnp.float32)
    if pieces:
        entries = entries * block_scale(own_key, dims, pieces, -0.22, 0.18)
    return jnp.clip(entries, -limit, limit).astype(held_as)


def setup_inputs(seed: int = 0) -> dict:
    key_list = jax.random.split(jax.random.key(seed), 17)
    receptance = noise(key_list[0], (MICRO_TOKENS, CHANNELS), 1.0, 6.0, ((0, 64), (1, 4)))
    key_rows = noise(key_list[1], (MICRO_TOKENS, CHANNELS), 1.0, 6.0, ((0, 64), (1, 4)))
    value_rows = noise(key_list[2], (MICRO_TOKENS, CHANNELS), 1.0, 6.0, ((0, 64), (1, 4)))
    decay_input = noise(key_list[3], (MICRO_TOKENS, CHANNELS), 0.7, 2.796875, ((0, 64), (1, 4)))
    learn_input = draw_learn_input(jax.random.fold_in(key_list[16], 71), 0)
    decay_base = draw_decay_base(jax.random.fold_in(key_list[16], 71), 0)
    decay_shift = draw_decay_shift(jax.random.fold_in(key_list[16], 71), 0)
    channel_gain = jnp.clip(1.0 + 0.18 * jax.random.normal(key_list[7], (CHANNELS,), jnp.float32), 0.1, 1.9)
    out_weight = noise(key_list[8], (CHANNELS, D), CHANNELS ** -0.5, 0.125, ((0, 4),))
    expert_input = noise(key_list[9], (MICRO_TOKENS, D), 1.0, 6.0, ((0, 256),))
    expert_gain = jnp.clip(1.0 + 0.18 * jax.random.normal(key_list[10], (D,), jnp.float32), 0.1, 1.9)
    routes_keys = jax.random.split(jax.random.fold_in(key_list[11], 1), MICRO_TOKENS // TOK_DEV)
    routes_turns = jax.random.permutation(jax.random.fold_in(key_list[11], 3), MICRO_TOKENS // TOK_DEV)
    routes = jax.vmap(lambda own, number: assign_block(jax.random.fold_in(key_list[11], 2), own, number, TOK_DEV, EXPERTS, TOPK, CAP, 1))(routes_keys, routes_turns).reshape((MICRO_TOKENS, TOPK))
    route_weight = jnp.clip(jnp.exp(math.log(1.0) - 2.3025851 * jax.random.uniform(key_list[12], (MICRO_TOKENS, TOPK), jnp.float32) ** block_scale(key_list[12], (MICRO_TOKENS, TOPK), ((0, 256),), -0.2, 0.2)), 0.1, 1.0)
    gate_weight = noise(key_list[13], (EXPERTS, D, FF), D ** -0.5, 0.125, ((0, 64), (2, 4)))
    up_weight = noise(key_list[14], (EXPERTS, D, FF), D ** -0.5, 0.125, ((0, 64), (2, 4)))
    down_weight = noise(key_list[15], (EXPERTS, FF, D), FF ** -0.5, 0.1875, ((0, 64), (1, 4)))
    return {"receptance": receptance, "key_rows": key_rows, "value_rows": value_rows, "decay_input": decay_input, "learn_input": learn_input, "decay_base": decay_base, "decay_shift": decay_shift, "channel_gain": channel_gain, "out_weight": out_weight, "expert_input": expert_input, "expert_gain": expert_gain, "routes": routes, "route_weight": route_weight, "gate_weight": gate_weight, "up_weight": up_weight, "down_weight": down_weight}


NORM_EPS = 1e-06
GROUP_EPS = 0.00064
KEY_EPS = 1e-06
PRECISE = lax.Precision.HIGHEST

def rounded_sum(inputs, weight, groups):
    group_size = inputs.shape[1] // groups
    result = jnp.zeros((inputs.shape[0], weight.shape[1]), jnp.float32)
    for part_index in range(groups):
        lower = part_index * group_size
        partial_value = jnp.dot(inputs[:, lower:lower + group_size], weight[lower:lower + group_size], preferred_element_type=jnp.float32)
        result = result + lax.optimization_barrier(partial_value.astype(jnp.bfloat16)).astype(jnp.float32)
    return result.astype(jnp.bfloat16)

def slot_targets(block_routes, experts, capacity):
    flat_routes = block_routes.reshape(-1)
    matches = (flat_routes[:, None] == jnp.arange(experts, dtype=jnp.int32)[None, :]).astype(jnp.int32)
    earlier = jnp.cumsum(matches, axis=0) - matches
    slots = lax.optimization_barrier(jnp.sum(earlier * matches, axis=1)).reshape(block_routes.shape)
    return (block_routes * capacity + slots).astype(jnp.int32)

def token_mixer(receptance, key_rows, value_rows, decay_input, learn_input, decay_base, decay_shift, channel_gain, out_weight):
    head_shape = (MICRO_TOKENS, HEADS, HEAD)
    recept = receptance.astype(jnp.float32).reshape(head_shape)
    key_data = key_rows.astype(jnp.float32).reshape(head_shape)
    value_data = value_rows.astype(jnp.float32).reshape(head_shape)
    pre_decay = decay_input.astype(jnp.float32).reshape(head_shape) + decay_base.reshape(1, HEADS, HEAD) + decay_shift[:, :, None]
    decays = jnp.exp(-jnp.exp(-jax.nn.softplus(-pre_decay) - 0.5))
    rates = jax.nn.sigmoid(learn_input.astype(jnp.float32)).reshape(head_shape)
    unit_keys = key_data / jnp.sqrt(lax.optimization_barrier(jnp.sum(key_data * key_data, axis=2, keepdims=True)) + KEY_EPS)
    removal = unit_keys * rates

    def advance(state, inputs):
        recept_now, decay_now, key_now, value_now, unit_now, removal_now = inputs
        probes = jnp.einsum('hij,hj->hi', state, unit_now, precision=PRECISE)
        state = state * decay_now[:, None, :] - probes[:, :, None] * removal_now[:, None, :] + value_now[:, :, None] * key_now[:, None, :]
        return (state, jnp.einsum('hij,hj->hi', state, recept_now, precision=PRECISE))
    start_state = jnp.zeros((HEADS, HEAD, HEAD), jnp.float32)
    _, readout = lax.scan(advance, start_state, (recept, decays, key_data, value_data, unit_keys, removal))
    centred = readout - lax.optimization_barrier(jnp.mean(readout, axis=2, keepdims=True))
    variance = lax.optimization_barrier(jnp.mean(centred * centred, axis=2, keepdims=True))
    normed = (centred * lax.rsqrt(variance + GROUP_EPS)).reshape(MICRO_TOKENS, CHANNELS) * channel_gain
    return rounded_sum(normed.astype(jnp.bfloat16), out_weight, N_TP)

def expert_layer(expert_input, expert_gain, routes, route_weight, gate_weight, up_weight, down_weight):
    inputs = expert_input.astype(jnp.float32)
    normed = (inputs * lax.rsqrt(lax.optimization_barrier(jnp.mean(inputs * inputs, axis=1, keepdims=True)) + NORM_EPS) * expert_gain).astype(jnp.bfloat16)
    blocks = MICRO_TOKENS // TOK_DEV
    block_routes = routes.reshape(blocks, TOK_DEV, TOPK)
    targets = jax.vmap(lambda member: slot_targets(member, EXPERTS, CAP))(block_routes)
    slots = targets - block_routes * CAP
    block_index = jnp.arange(blocks, dtype=jnp.int32)[:, None, None]
    places = ((block_routes * blocks + block_index) * CAP + slots).astype(jnp.int32)
    token_index = jnp.broadcast_to(jnp.arange(MICRO_TOKENS, dtype=jnp.int32).reshape(blocks, TOK_DEV, 1), places.shape)
    owners = jnp.full((EXPERTS * blocks * CAP,), MICRO_TOKENS, jnp.int32).at[places.reshape(-1)].set(token_index.reshape(-1))
    padded = jnp.concatenate([normed, jnp.zeros((1, D), jnp.bfloat16)], axis=0)

    def run_expert(operands):
        owner_rows, w_gate, w_up, w_down = operands
        gathered = padded[owner_rows]
        gates = jnp.dot(gathered, w_gate, preferred_element_type=jnp.float32)
        uppers = jnp.dot(gathered, w_up, preferred_element_type=jnp.float32)
        hidden = (jax.nn.silu(gates) * uppers).astype(jnp.bfloat16)
        return rounded_sum(hidden, w_down, N_TP)
    outputs = lax.map(run_expert, (owners.reshape(EXPERTS, blocks * CAP), gate_weight, up_weight, down_weight))
    flat_rows = outputs.reshape(EXPERTS * blocks * CAP, D)
    picks = places.reshape(MICRO_TOKENS, TOPK)
    combined = jnp.zeros((MICRO_TOKENS, D), jnp.float32)
    for picked in range(TOPK):
        combined = combined + flat_rows[picks[:, picked]].astype(jnp.float32) * route_weight[:, picked:picked + 1]
    return combined.astype(jnp.bfloat16)

def reference(receptance, key_rows, value_rows, decay_input, learn_input, decay_base, decay_shift, channel_gain, out_weight, expert_input, expert_gain, routes, route_weight, gate_weight, up_weight, down_weight):
    mixer_out = token_mixer(receptance, key_rows, value_rows, decay_input, learn_input, decay_base, decay_shift, channel_gain, out_weight)
    expert_out = expert_layer(expert_input, expert_gain, routes, route_weight, gate_weight, up_weight, down_weight)
    return (mixer_out, expert_out)
```

```python
import jax
import jax.numpy as jnp
from jax import lax
from jax.experimental import pallas as pl
from jax.experimental.pallas import tpu as pltpu
from jax.sharding import Mesh
from jax.sharding import PartitionSpec as P


SPAN = 128
EP = ("ep_0", "ep_1", "ep_2")
GROUP = ("ep_1", "ep_2")
EP_TP = ("ep_0", "ep_1", "ep_2", "tp")
GROUPS = 8
HEAD = 64
PAIR = 128
MSG_ROWS = 80
CAPACITY = 8

NORM_EPS = 1e-06
GROUP_EPS = 0.00064
KEY_EPS = 1e-06
DECAY_SCALE = 0.6065306597126334

F32 = jnp.float32
BF16 = jnp.bfloat16


def dot(a, b):
    return lax.dot_general(a, b, (((1,), (0,)), ((), ())), preferred_element_type=F32)


def dot_nt(a, b):
    return lax.dot_general(a, b, (((1,), (1,)), ((), ())), preferred_element_type=F32)


def dot_tn(a, b):
    return lax.dot_general(a, b, (((0,), (0,)), ((), ())), preferred_element_type=F32)


def two_parts(x):
    high = x.astype(BF16)
    return high, (x - high.astype(F32)).astype(BF16)


def iota(shape, dim):
    return lax.broadcasted_iota(jnp.int32, shape, dim)


def block_ones():
    rows, cols = iota((PAIR, PAIR), 0), iota((PAIR, PAIR), 1)
    return (rows // HEAD) == (cols // HEAD)


def unit_lower_inverses(parts):
    size = parts[0].shape[0]
    rows, cols = iota((size, size), 0), iota((size, size), 1)
    eye = (rows == cols).astype(F32)
    start = 16
    inside = (rows // start) == (cols // start)
    powers = [jnp.where(inside, -a, 0.0) for a in parts]
    inverses = [eye + p for p in powers]
    reach = 2
    while reach < start:
        narrow = [p.astype(BF16) for p in powers]
        powers = [dot(p, p) for p in narrow]
        inverses = [
            inv + dot(inv.astype(BF16), p.astype(BF16))
            for inv, p in zip(inverses, powers)
        ]
        reach *= 2
    block = start
    while block < size:
        joined = ((rows // (2 * block)) == (cols // (2 * block))) & (
            (rows // block) != (cols // block)
        )
        narrow = [inv.astype(BF16) for inv in inverses]
        corners = [jnp.where(joined, a, 0.0).astype(BF16) for a in parts]
        moved = [dot(c, inv).astype(BF16) for c, inv in zip(corners, narrow)]
        inverses = [
            inv - dot(short, m) for inv, short, m in zip(inverses, narrow, moved)
        ]
        block *= 2
    return inverses


def summary_kernel(
    q_ref, k_ref, v_ref, di_ref, li_ref, base_ref, shift_ref,
    reader_ref, local_ref, gather_ref, add_ref, fade_ref, msg_ref,
    maps_ref, total_ref,
):
    step = pl.program_id(0)
    rows, channels = q_ref.shape
    heads = shift_ref.shape[1]
    pairs = heads // 2
    same = block_ones()
    same_f = same.astype(F32)
    same_b = same_f.astype(BF16)
    row2, col2 = iota((PAIR, PAIR), 0), iota((PAIR, PAIR), 1)
    eye = (row2 == col2).astype(F32)

    @pl.when(step == 0)
    def _():
        for p in range(pairs):
            maps_ref[p, :PAIR, :] = eye
            maps_ref[p, PAIR:, :] = jnp.zeros((PAIR, PAIR), F32)
        total_ref[...] = jnp.ones_like(total_ref)

    spread = (
        (iota((heads, channels), 1) // HEAD) == iota((heads, channels), 0)
    ).astype(F32).astype(BF16)
    shift_high, shift_low = two_parts(shift_ref[...])
    pre = (
        di_ref[...].astype(F32)
        + base_ref[...]
        + (dot(shift_high, spread) + dot(shift_low, spread))
    )
    log_decay = -DECAY_SCALE / (1.0 + jnp.exp(-pre))
    tri_rows, tri_cols = iota((rows, rows), 0), iota((rows, rows), 1)
    inclusive = tri_rows >= tri_cols
    strict = tri_rows > tri_cols
    tri = inclusive.astype(F32).astype(BF16)
    decay_high, decay_low = two_parts(log_decay)
    cum = dot(tri, decay_high) + dot(tri, decay_low)
    middle = cum[rows // 2 - 1 : rows // 2, :]
    ending = cum[rows - 1 : rows, :]
    grow = jnp.exp(cum - middle)
    grow_before = grow * jnp.exp(-log_decay)
    shrink = jnp.exp(middle - cum)
    from_start = jnp.exp(middle)
    to_end = jnp.exp(ending - middle)
    fade = jnp.exp(ending)
    fade_ref[0] = fade

    keys = k_ref[...].astype(F32)
    recept = q_ref[...].astype(F32)
    squares_high, squares_low = two_parts(keys * keys)
    lengths = jnp.concatenate(
        [
            dot(squares_high[:, p * PAIR : (p + 1) * PAIR], same_b)
            + dot(squares_low[:, p * PAIR : (p + 1) * PAIR], same_b)
            for p in range(pairs)
        ],
        axis=1,
    )
    unit = keys * lax.rsqrt(lengths + KEY_EPS)
    removal = unit / (1.0 + jnp.exp(-li_ref[...].astype(F32)))

    probes_f = unit * grow_before
    queries_f = recept * grow
    back_removal_f = removal * shrink
    back_keys_f = keys * shrink
    probes = probes_f.astype(BF16)
    queries = queries_f.astype(BF16)
    back_removal = back_removal_f.astype(BF16)
    back_keys = back_keys_f.astype(BF16)
    carried_in = (probes_f * from_start).astype(BF16)
    read_in = queries_f * from_start
    tail_removal = (back_removal_f * to_end).astype(BF16)
    tail_keys = (back_keys_f * to_end).astype(BF16)
    values = v_ref[...]

    first = iota((rows, PAIR), 1) < HEAD
    none = jnp.zeros((rows, PAIR), BF16)

    def left(x):
        return jnp.where(first, x, none)

    def right(x):
        return jnp.where(first, none, x)

    kept = []
    strict_parts = []
    for p in range(pairs):
        lanes = slice(p * PAIR, (p + 1) * PAIR)
        pr, qu = probes[:, lanes], queries[:, lanes]
        outer = jnp.concatenate([left(pr), right(pr), left(qu), right(qu)], axis=0)
        inner = jnp.concatenate([back_removal[:, lanes], back_keys[:, lanes]], axis=0)
        products = dot_nt(outer, inner)
        strict_parts.append(jnp.where(strict, products[0:rows, 0:rows], 0.0))
        strict_parts.append(jnp.where(strict, products[rows : 2 * rows, 0:rows], 0.0))
        pair_keys = jnp.concatenate(
            [
                jnp.where(strict, products[0:rows, rows:], 0.0),
                jnp.where(strict, products[rows : 2 * rows, rows:], 0.0),
            ],
            axis=1,
        ).astype(BF16)
        read_keys = jnp.concatenate(
            [
                jnp.where(inclusive, products[2 * rows : 3 * rows, rows:], 0.0),
                jnp.where(inclusive, products[3 * rows :, rows:], 0.0),
            ],
            axis=1,
        ).astype(BF16)
        read_removal = jnp.concatenate(
            [
                jnp.where(inclusive, products[2 * rows : 3 * rows, 0:rows], 0.0),
                jnp.where(inclusive, products[3 * rows :, 0:rows], 0.0),
            ],
            axis=1,
        ).astype(BF16)
        va = values[:, lanes]
        stacked = jnp.concatenate([left(va), right(va)], axis=0)
        sums = dot(jnp.concatenate([pair_keys, read_keys], axis=0), stacked)
        kept.append((read_removal, sums))

    inverses = unit_lower_inverses(strict_parts)

    for p in range(pairs):
        lanes = slice(p * PAIR, (p + 1) * PAIR)
        read_removal, sums = kept[p]
        weights = sums[:rows].astype(BF16)
        carry = carried_in[:, lanes]
        sides = jnp.concatenate(
            [
                jnp.concatenate([left(carry), left(weights)], axis=1),
                jnp.concatenate([right(carry), right(weights)], axis=1),
            ],
            axis=0,
        )
        inverse = jnp.concatenate([inverses[2 * p], inverses[2 * p + 1]], axis=1)
        solved = dot(inverse.astype(BF16), sides).astype(BF16)
        carried, local = solved[:, :PAIR], solved[:, PAIR:]
        halves = jnp.concatenate(
            [
                jnp.concatenate([left(carried), left(local)], axis=1),
                jnp.concatenate([right(carried), right(local)], axis=1),
            ],
            axis=0,
        )
        taken = dot(read_removal, halves)
        reader_ref[:, lanes] = (read_in[:, lanes] - taken[:, :PAIR]).astype(BF16)
        local_ref[:, lanes] = sums[rows:] - taken[:, PAIR:]
        ends = dot_tn(solved, tail_removal[:, lanes])
        gathered = jnp.where(same, ends[:PAIR], 0.0).astype(BF16)
        added = jnp.where(
            same, dot_tn(values[:, lanes], tail_keys[:, lanes]) - ends[PAIR:], 0.0
        )
        gather_ref[0, p] = gathered
        add_ref[0, p] = added
        maps = maps_ref[p]
        maps = maps * fade[:, lanes] - dot(maps.astype(BF16), gathered)
        maps_ref[p, :PAIR, :] = maps[:PAIR]
        maps_ref[p, PAIR:, :] = maps[PAIR:] + added
    total_ref[...] = total_ref[...] * fade

    @pl.when(step == pl.num_programs(0) - 1)
    def _():
        low = iota((PAIR, PAIR), 1) < HEAD
        low_row = iota((1, PAIR), 1) < HEAD
        for p in range(pairs):
            lanes = slice(p * PAIR, (p + 1) * PAIR)
            total = total_ref[:, lanes]
            lost = eye * total - maps_ref[p, :PAIR, :]
            gained = maps_ref[p, PAIR:, :]
            lost = lost + pltpu.roll(lost, HEAD, 1)
            gained = gained + pltpu.roll(gained, HEAD, 1)
            both = jnp.where(low, lost, gained).astype(BF16)
            msg_ref[2 * p, :HEAD, :] = both[:HEAD]
            msg_ref[2 * p + 1, :HEAD, :] = both[HEAD:]
            for side in range(2):
                own = jnp.where(low_row == (side == 0), total, 0.0)
                own = jnp.broadcast_to(own, (16, PAIR))
                own = own + pltpu.roll(own, HEAD, 1)
                high, rest = two_parts(own)
                msg_ref[2 * p + side, HEAD:, :] = jnp.where(
                    iota((16, PAIR), 1) < HEAD, high.astype(F32), rest.astype(F32)
                ).astype(BF16)


def message_parts(message):
    lost = message[:HEAD, :HEAD]
    gained = message[:HEAD, HEAD:].astype(F32)
    fades = message[HEAD : HEAD + 1, :].astype(F32)
    return lost, gained, fades[:, :HEAD] + fades[:, HEAD:]


def group_kernel(in_ref, prefix_ref, out_ref):
    rows, cols = iota((HEAD, HEAD), 0), iota((HEAD, HEAD), 1)
    eye = (rows == cols).astype(F32)
    maps = jnp.concatenate([eye, jnp.zeros((HEAD, HEAD), F32)], axis=0)
    total = jnp.ones((1, HEAD), F32)
    for m in range(in_ref.shape[0]):
        lost, gained, fade = message_parts(in_ref[m])
        prefix_ref[m] = maps
        moved = maps * fade - dot(maps.astype(BF16), lost)
        maps = jnp.concatenate([moved[:HEAD], moved[HEAD:] + gained], axis=0)
        total = total * fade
    both = jnp.concatenate([eye * total - maps[:HEAD], maps[HEAD:]], axis=1).astype(BF16)
    high, rest = two_parts(jnp.broadcast_to(total, (16, HEAD)))
    ends = jnp.concatenate([high.astype(F32), rest.astype(F32)], axis=1).astype(BF16)
    for z in range(out_ref.shape[0]):
        out_ref[z, :HEAD, :] = both
        out_ref[z, HEAD:, :] = ends


def enter_kernel(here_ref, in_ref, prefix_ref, out_ref):
    here = here_ref[0]
    state = jnp.zeros((HEAD, HEAD), F32)
    for z in range(in_ref.shape[0]):
        lost, gained, fade = message_parts(in_ref[z])
        passed = state * fade - dot(state.astype(BF16), lost) + gained
        state = jnp.where(z < here, passed, state)
    narrow = state.astype(BF16)
    for m in range(out_ref.shape[0]):
        entering = dot(narrow, prefix_ref[m, :HEAD, :].astype(BF16)) + prefix_ref[m, HEAD:, :]
        out_ref[m] = jnp.concatenate([entering, entering], axis=1).astype(BF16)


def readout_kernel(
    enter_ref, reader_ref, local_ref, gather_ref, add_ref, fade_ref, gain_ref, weight_ref,
    out_ref, state_ref,
):
    step = pl.program_id(0)
    channels = reader_ref.shape[1]
    pairs = channels // PAIR
    same = block_ones()
    means = jnp.where(same, 1.0 / HEAD, 0.0).astype(BF16)

    @pl.when(step == 0)
    def _():
        for p in range(pairs):
            entering = jnp.concatenate([enter_ref[2 * p], enter_ref[2 * p + 1]], axis=0)
            state_ref[p] = jnp.where(same, entering.astype(F32), 0.0)

    pieces = []
    for p in range(pairs):
        lanes = slice(p * PAIR, (p + 1) * PAIR)
        state = state_ref[p]
        narrow = state.astype(BF16)
        read = dot_nt(reader_ref[:, lanes], narrow) + local_ref[:, lanes]
        state_ref[p] = state * fade_ref[0, :, lanes] - dot(narrow, gather_ref[0, p]) + add_ref[0, p]
        centred = read - dot(read.astype(BF16), means)
        spread = dot((centred * centred).astype(BF16), means)
        pieces.append(
            (centred * lax.rsqrt(spread + GROUP_EPS) * gain_ref[:, lanes]).astype(BF16)
        )
    normed = jnp.concatenate(pieces, axis=1)
    out_ref[...] = dot(normed, weight_ref[...]).astype(BF16)


def hidden_kernel(x_ref, gate_ref, up_ref, out_ref):
    x = x_ref[...]
    gates = dot(x, gate_ref[...])
    uppers = dot(x, up_ref[...])
    out_ref[...] = (gates / (1.0 + jnp.exp(-gates)) * uppers).astype(BF16)


def down_kernel(h0, h1, h2, h3, own, top_r, low_r, top_l, low_l, top_f, low_f, out_ref):
    units = jnp.concatenate([h0[...], h1[...], h2[...], h3[...]], axis=1)
    weights = jnp.concatenate(
        [w[...] for w in (own, top_r, low_r, top_l, low_l, top_f, low_f)], axis=0
    )
    out_ref[...] = dot(units, weights).astype(BF16)


def pack_kernel(x_ref, gain_ref, routes_ref, mix_ref, out_ref, high_ref, rest_ref):
    tokens = x_ref.shape[0]
    places = out_ref.shape[0]
    x = x_ref[...].astype(F32)
    normed = (
        x * lax.rsqrt(jnp.mean(x * x, axis=1, keepdims=True) + NORM_EPS) * gain_ref[...]
    ).astype(BF16)
    experts = places // CAPACITY
    listed = iota((tokens, experts), 1)
    first, second = routes_ref[:, 0:1], routes_ref[:, 1:2]
    first_mark = (first == listed).astype(F32)
    second_mark = (second == listed).astype(F32)
    before = (iota((tokens, tokens), 0) > iota((tokens, tokens), 1)).astype(F32).astype(BF16)
    earlier = dot(before, (first_mark + second_mark).astype(BF16))
    columns = iota((tokens, places), 1)
    table = jnp.zeros((tokens, places), F32)
    mix = jnp.zeros((tokens, places), F32)
    for named, mark, weight in (
        (first, first_mark, mix_ref[:, 0:1]),
        (second, second_mark, mix_ref[:, 1:2]),
    ):
        slot = jnp.sum(earlier * mark, axis=1, keepdims=True).astype(jnp.int32)
        here = columns == named * CAPACITY + slot
        table = table + here.astype(F32)
        mix = jnp.where(here, weight, mix)
    out_ref[...] = dot_tn(table.astype(BF16), normed).astype(BF16)
    high, rest = two_parts(mix)
    high_ref[...] = high
    rest_ref[...] = rest


def combine_kernel(high_ref, rest_ref, rows_ref, out_ref):
    rows = rows_ref[...]
    out_ref[...] = (dot(high_ref[...], rows) + dot(rest_ref[...], rows)).astype(BF16)


def whole(shape):
    return pl.BlockSpec(shape, lambda *_: (0,) * len(shape))


def estimate(flops, moved, transcendentals=0):
    return pl.CostEstimate(
        flops=int(flops), bytes_accessed=int(moved), transcendentals=int(transcendentals)
    )


def summarize(q, k, v, di, li, base, shift):
    rows, channels = q.shape
    heads = shift.shape[1]
    pairs = heads // 2
    spans = rows // SPAN
    block = pl.BlockSpec((SPAN, channels), lambda i: (i, 0))
    square = (1, pairs, PAIR, PAIR)
    return pl.pallas_call(
        summary_kernel,
        grid=(spans,),
        in_specs=[block] * 5
        + [whole((1, channels)), pl.BlockSpec((SPAN, heads), lambda i: (i, 0))],
        out_specs=[
            block,
            block,
            pl.BlockSpec(square, lambda i: (i, 0, 0, 0)),
            pl.BlockSpec(square, lambda i: (i, 0, 0, 0)),
            pl.BlockSpec((1, 1, channels), lambda i: (i, 0, 0)),
            whole((heads, MSG_ROWS, PAIR)),
        ],
        out_shape=[
            jax.ShapeDtypeStruct((rows, channels), BF16),
            jax.ShapeDtypeStruct((rows, channels), F32),
            jax.ShapeDtypeStruct((spans, pairs, PAIR, PAIR), BF16),
            jax.ShapeDtypeStruct((spans, pairs, PAIR, PAIR), F32),
            jax.ShapeDtypeStruct((spans, 1, channels), F32),
            jax.ShapeDtypeStruct((heads, MSG_ROWS, PAIR), BF16),
        ],
        scratch_shapes=[
            pltpu.VMEM((pairs, 2 * PAIR, PAIR), F32),
            pltpu.VMEM((1, channels), F32),
        ],
        compiler_params=pltpu.CompilerParams(dimension_semantics=("arbitrary",)),
        cost_estimate=estimate(2.0e10, 6 << 20, 2 << 20),
        name="summary",
    )(q, k, v, di, li, base, shift)


def group_scan(messages):
    count = messages.shape[0]
    return pl.pallas_call(
        group_kernel,
        out_shape=[
            jax.ShapeDtypeStruct((count, 2 * HEAD, HEAD), F32),
            jax.ShapeDtypeStruct((GROUPS, MSG_ROWS, PAIR), BF16),
        ],
        cost_estimate=estimate(2.0e9, 1 << 20),
        name="group_scan",
    )(messages)


def enter_states(here, totals, prefixes):
    return pl.pallas_call(
        enter_kernel,
        in_specs=[
            pl.BlockSpec(memory_space=pltpu.SMEM),
            pl.BlockSpec(memory_space=pltpu.VMEM),
            pl.BlockSpec(memory_space=pltpu.VMEM),
        ],
        out_shape=jax.ShapeDtypeStruct((prefixes.shape[0], HEAD, PAIR), BF16),
        cost_estimate=estimate(2.0e9, 1 << 20),
        name="enter_states",
    )(here, totals, prefixes)


def read_and_project(entering, reader, local, gather, add, fade, gain, weight):
    rows, channels = reader.shape
    pairs = channels // PAIR
    spans = rows // SPAN
    width = weight.shape[1]
    block = pl.BlockSpec((SPAN, channels), lambda i: (i, 0))
    square = pl.BlockSpec((1, pairs, PAIR, PAIR), lambda i: (i, 0, 0, 0))
    return pl.pallas_call(
        readout_kernel,
        grid=(spans,),
        in_specs=[
            whole(entering.shape),
            block,
            block,
            square,
            square,
            pl.BlockSpec((1, 1, channels), lambda i: (i, 0, 0)),
            whole((1, channels)),
            whole(weight.shape),
        ],
        out_specs=pl.BlockSpec((SPAN, width), lambda i: (i, 0)),
        out_shape=jax.ShapeDtypeStruct((rows, width), BF16),
        scratch_shapes=[pltpu.VMEM((pairs, PAIR, PAIR), F32)],
        compiler_params=pltpu.CompilerParams(dimension_semantics=("arbitrary",)),
        cost_estimate=estimate(5.0e9, 8 << 20),
        name="readout",
    )(entering, reader, local, gather, add, fade, gain, weight)


def expert_hidden(x, gate, up):
    rows, width = x.shape
    units = gate.shape[1]
    tile = rows // 2
    return pl.pallas_call(
        hidden_kernel,
        grid=(2,),
        in_specs=[
            pl.BlockSpec((tile, width), lambda i: (i, 0)),
            whole(gate.shape),
            whole(up.shape),
        ],
        out_specs=pl.BlockSpec((tile, units), lambda i: (i, 0)),
        out_shape=jax.ShapeDtypeStruct((rows, units), BF16),
        compiler_params=pltpu.CompilerParams(dimension_semantics=("arbitrary",)),
        cost_estimate=estimate(4 * rows * width * units, 5 << 20, rows * units),
        name="hidden",
    )(x, gate, up)


def expert_down(hiddens, weights):
    rows = hiddens[0].shape[0]
    width = weights[0].shape[1]
    tile = width // 4
    return pl.pallas_call(
        down_kernel,
        grid=(4,),
        in_specs=[whole(h.shape) for h in hiddens]
        + [pl.BlockSpec((w.shape[0], tile), lambda i: (0, i)) for w in weights],
        out_specs=pl.BlockSpec((rows, tile), lambda i: (0, i)),
        out_shape=jax.ShapeDtypeStruct((rows, width), BF16),
        compiler_params=pltpu.CompilerParams(dimension_semantics=("arbitrary",)),
        cost_estimate=estimate(8 * rows * 256 * width, 7 << 20),
        name="down",
    )(*hiddens, *weights)


def pack_rows(x, gain, routes, mix, places):
    tokens, width = x.shape
    return pl.pallas_call(
        pack_kernel,
        out_shape=[
            jax.ShapeDtypeStruct((places, width), BF16),
            jax.ShapeDtypeStruct((tokens, places), BF16),
            jax.ShapeDtypeStruct((tokens, places), BF16),
        ],
        cost_estimate=estimate(2.0e9, 3 << 20),
        name="pack",
    )(x, gain, routes, mix)


def combine_rows(high, rest, rows):
    tokens, places = high.shape
    width = rows.shape[1]
    tile = width // 4
    return pl.pallas_call(
        combine_kernel,
        grid=(4,),
        in_specs=[
            whole(high.shape),
            whole(rest.shape),
            pl.BlockSpec((places, tile), lambda i: (0, i)),
        ],
        out_specs=pl.BlockSpec((tokens, tile), lambda i: (0, i)),
        out_shape=jax.ShapeDtypeStruct((tokens, width), BF16),
        compiler_params=pltpu.CompilerParams(dimension_semantics=("arbitrary",)),
        cost_estimate=estimate(1.0e9, 3 << 20),
        name="combine",
    )(high, rest, rows)


def ring(x, shift):
    count = lax.axis_size("tp")
    return lax.ppermute(x, "tp", [(i, (i + shift) % count) for i in range(count)])


def exchange(x, axis):
    return lax.all_to_all(x, axis, 0, 0, tiled=True)


def on_device(
    receptance,
    key_rows,
    value_rows,
    decay_input,
    learn_input,
    decay_base,
    decay_shift,
    channel_gain,
    out_weight,
    expert_input,
    expert_gain,
    routes,
    route_weight,
    gate_weight,
    up_weight,
    down_weight,
):
    ep_count = lax.axis_size(EP)
    token_rows, model_width = expert_input.shape
    experts = gate_weight.shape[0] * ep_count
    places = experts * CAPACITY

    w_gate = gate_weight[0]
    w_up = up_weight[0]
    w_down = down_weight[0]
    cut = w_down.shape[0] // 2
    down_top, down_low = w_down[:cut], w_down[cut:]
    gate_r, up_l = ring(w_gate, 1), ring(w_up, -1)
    gate_l, up_r = ring(w_gate, -1), ring(w_up, 1)
    top_r, low_l = ring(down_top, 1), ring(down_low, -1)
    low_r, top_l = ring(down_low, 1), ring(down_top, -1)
    gate_f, up_f = ring(gate_r, 1), ring(up_l, -1)
    top_f, low_f = ring(top_r, 1), ring(low_l, -1)

    outgoing, high, rest = pack_rows(
        expert_input, expert_gain.reshape(1, -1), routes, route_weight, places
    )
    arrived = exchange(
        outgoing.reshape(experts, CAPACITY, model_width), EP
    ).reshape(places, model_width)

    reader, local, gather, add, fade, messages = summarize(
        receptance,
        key_rows,
        value_rows,
        decay_input,
        learn_input,
        decay_base.reshape(1, -1),
        decay_shift,
    )
    prefixes, totals = group_scan(exchange(messages, GROUP))
    entered = enter_states(
        lax.axis_index("ep_0").astype(jnp.int32).reshape(1),
        exchange(totals, "ep_0"),
        prefixes,
    )
    partial = read_and_project(
        exchange(entered, GROUP),
        reader,
        local,
        gather,
        add,
        fade,
        channel_gain.reshape(1, -1),
        out_weight,
    )
    tp_count = lax.axis_size("tp")
    shares = exchange(partial.reshape(tp_count, token_rows, model_width), "tp")
    mixer_out = jnp.sum(shares.astype(F32), axis=0).astype(BF16)

    hiddens = []
    for g, u in ((w_gate, w_up), (gate_r, up_r), (gate_l, up_l), (gate_f, up_f)):
        hiddens.append(expert_hidden(arrived, g, u))
    returning = expert_down(hiddens, [w_down, top_r, low_r, top_l, low_l, top_f, low_f])
    returned = exchange(returning.reshape(ep_count, CAPACITY, model_width), EP)
    combined = combine_rows(high, rest, returned.reshape(places, model_width))
    return (mixer_out, combined)


def solution(mesh):
    finer = Mesh(mesh.devices.reshape(8, 4, 2, mesh.shape["tp"]), ("ep_0", "ep_1", "ep_2", "tp"))
    placed = (
        P(EP, "tp"),
        P(EP, "tp"),
        P(EP, "tp"),
        P(EP, "tp"),
        P(EP, "tp"),
        P("tp"),
        P(EP, "tp"),
        P("tp"),
        P("tp", None),
        P(EP_TP, None),
        P(),
        P(EP_TP, None),
        P(EP_TP, None),
        P(EP, None, "tp"),
        P(EP, None, "tp"),
        P(EP, "tp", None),
    )

    return jax.shard_map(
        on_device,
        mesh=finer,
        in_specs=placed,
        out_specs=(P(EP_TP, None), P(EP_TP, None)),
        check_vma=False,
    )
```

```python
import jax
import jax.numpy as jnp
from jax import lax
from jax.experimental import pallas as pl
from jax.experimental.pallas import tpu as pltpu
from jax.sharding import Mesh
from jax.sharding import PartitionSpec as P


SPAN = 128
EP = ("ep_0", "ep_1", "ep_2")
GROUP = ("ep_1", "ep_2")
EP_TP = ("ep_0", "ep_1", "ep_2", "tp")
GROUPS = 8
HEAD = 64
PAIR = 128
MSG_ROWS = 80
CAPACITY = 8

NORM_EPS = 1e-06
GROUP_EPS = 0.00064
KEY_EPS = 1e-06
DECAY_SCALE = 0.6065306597126334

F32 = jnp.float32
BF16 = jnp.bfloat16


def dot(a, b):
    return lax.dot_general(a, b, (((1,), (0,)), ((), ())), preferred_element_type=F32)


def dot_nt(a, b):
    return lax.dot_general(a, b, (((1,), (1,)), ((), ())), preferred_element_type=F32)


def dot_tn(a, b):
    return lax.dot_general(a, b, (((0,), (0,)), ((), ())), preferred_element_type=F32)


def two_parts(x):
    high = x.astype(BF16)
    return high, (x - high.astype(F32)).astype(BF16)


def iota(shape, dim):
    return lax.broadcasted_iota(jnp.int32, shape, dim)


def block_ones():
    rows, cols = iota((PAIR, PAIR), 0), iota((PAIR, PAIR), 1)
    return (rows // HEAD) == (cols // HEAD)


def unit_lower_inverses(parts):
    size = parts[0].shape[0]
    rows, cols = iota((size, size), 0), iota((size, size), 1)
    eye = (rows == cols).astype(F32)
    start = 16
    inside = (rows // start) == (cols // start)
    powers = [jnp.where(inside, -a, 0.0) for a in parts]
    inverses = [eye + p for p in powers]
    reach = 2
    while reach < start:
        narrow = [p.astype(BF16) for p in powers]
        powers = [dot(p, p) for p in narrow]
        inverses = [
            inv + dot(inv.astype(BF16), p.astype(BF16))
            for inv, p in zip(inverses, powers)
        ]
        reach *= 2
    block = start
    while block < size:
        joined = ((rows // (2 * block)) == (cols // (2 * block))) & (
            (rows // block) != (cols // block)
        )
        narrow = [inv.astype(BF16) for inv in inverses]
        corners = [jnp.where(joined, a, 0.0).astype(BF16) for a in parts]
        moved = [dot(c, inv).astype(BF16) for c, inv in zip(corners, narrow)]
        inverses = [
            inv - dot(short, m) for inv, short, m in zip(inverses, narrow, moved)
        ]
        block *= 2
    return inverses


def summary_kernel(
    here_ref, q_ref, k_ref, v_ref, di_ref, li_ref, base_ref, shift_ref,
    reader_ref, local_ref, gather_ref, add_ref, fade_ref, *rest_refs,
):
    sent_refs, (maps_ref, total_ref, msg_ref) = rest_refs[:GROUPS], rest_refs[GROUPS:]
    step = pl.program_id(0)
    rows, channels = q_ref.shape
    heads = shift_ref.shape[1]
    pairs = heads // 2
    same = block_ones()
    same_f = same.astype(F32)
    same_b = same_f.astype(BF16)
    row2, col2 = iota((PAIR, PAIR), 0), iota((PAIR, PAIR), 1)
    eye = (row2 == col2).astype(F32)

    @pl.when(step == 0)
    def _():
        for p in range(pairs):
            maps_ref[p, :PAIR, :] = eye
            maps_ref[p, PAIR:, :] = jnp.zeros((PAIR, PAIR), F32)
        total_ref[...] = jnp.ones_like(total_ref)

    spread = (
        (iota((heads, channels), 1) // HEAD) == iota((heads, channels), 0)
    ).astype(F32).astype(BF16)
    shift_high, shift_low = two_parts(shift_ref[...])
    pre = (
        di_ref[...].astype(F32)
        + base_ref[...]
        + (dot(shift_high, spread) + dot(shift_low, spread))
    )
    log_decay = -DECAY_SCALE / (1.0 + jnp.exp(-pre))
    tri_rows, tri_cols = iota((rows, rows), 0), iota((rows, rows), 1)
    inclusive = tri_rows >= tri_cols
    strict = tri_rows > tri_cols
    tri = inclusive.astype(F32).astype(BF16)
    decay_high, decay_low = two_parts(log_decay)
    cum = dot(tri, decay_high) + dot(tri, decay_low)
    middle = cum[rows // 2 - 1 : rows // 2, :]
    ending = cum[rows - 1 : rows, :]
    grow = jnp.exp(cum - middle)
    grow_before = grow * jnp.exp(-log_decay)
    shrink = jnp.exp(middle - cum)
    from_start = jnp.exp(middle)
    to_end = jnp.exp(ending - middle)
    fade = jnp.exp(ending)
    fade_ref[0] = fade

    keys = k_ref[...].astype(F32)
    recept = q_ref[...].astype(F32)
    squares_high, squares_low = two_parts(keys * keys)
    lengths = jnp.concatenate(
        [
            dot(squares_high[:, p * PAIR : (p + 1) * PAIR], same_b)
            + dot(squares_low[:, p * PAIR : (p + 1) * PAIR], same_b)
            for p in range(pairs)
        ],
        axis=1,
    )
    unit = keys * lax.rsqrt(lengths + KEY_EPS)
    removal = unit / (1.0 + jnp.exp(-li_ref[...].astype(F32)))

    probes_f = unit * grow_before
    queries_f = recept * grow
    back_removal_f = removal * shrink
    back_keys_f = keys * shrink
    probes = probes_f.astype(BF16)
    queries = queries_f.astype(BF16)
    back_removal = back_removal_f.astype(BF16)
    back_keys = back_keys_f.astype(BF16)
    carried_in = (probes_f * from_start).astype(BF16)
    read_in = queries_f * from_start
    tail_removal = (back_removal_f * to_end).astype(BF16)
    tail_keys = (back_keys_f * to_end).astype(BF16)
    values = v_ref[...]

    first = iota((rows, PAIR), 1) < HEAD
    none = jnp.zeros((rows, PAIR), BF16)

    def left(x):
        return jnp.where(first, x, none)

    def right(x):
        return jnp.where(first, none, x)

    kept = []
    strict_parts = []
    for p in range(pairs):
        lanes = slice(p * PAIR, (p + 1) * PAIR)
        pr, qu = probes[:, lanes], queries[:, lanes]
        outer = jnp.concatenate([left(pr), right(pr), left(qu), right(qu)], axis=0)
        inner = jnp.concatenate([back_removal[:, lanes], back_keys[:, lanes]], axis=0)
        products = dot_nt(outer, inner)
        strict_parts.append(jnp.where(strict, products[0:rows, 0:rows], 0.0))
        strict_parts.append(jnp.where(strict, products[rows : 2 * rows, 0:rows], 0.0))
        pair_keys = jnp.concatenate(
            [
                jnp.where(strict, products[0:rows, rows:], 0.0),
                jnp.where(strict, products[rows : 2 * rows, rows:], 0.0),
            ],
            axis=1,
        ).astype(BF16)
        read_keys = jnp.concatenate(
            [
                jnp.where(inclusive, products[2 * rows : 3 * rows, rows:], 0.0),
                jnp.where(inclusive, products[3 * rows :, rows:], 0.0),
            ],
            axis=1,
        ).astype(BF16)
        read_removal = jnp.concatenate(
            [
                jnp.where(inclusive, products[2 * rows : 3 * rows, 0:rows], 0.0),
                jnp.where(inclusive, products[3 * rows :, 0:rows], 0.0),
            ],
            axis=1,
        ).astype(BF16)
        va = values[:, lanes]
        stacked = jnp.concatenate([left(va), right(va)], axis=0)
        sums = dot(jnp.concatenate([pair_keys, read_keys], axis=0), stacked)
        kept.append((read_removal, sums))

    inverses = unit_lower_inverses(strict_parts)

    for p in range(pairs):
        lanes = slice(p * PAIR, (p + 1) * PAIR)
        read_removal, sums = kept[p]
        weights = sums[:rows].astype(BF16)
        carry = carried_in[:, lanes]
        sides = jnp.concatenate(
            [
                jnp.concatenate([left(carry), left(weights)], axis=1),
                jnp.concatenate([right(carry), right(weights)], axis=1),
            ],
            axis=0,
        )
        inverse = jnp.concatenate([inverses[2 * p], inverses[2 * p + 1]], axis=1)
        solved = dot(inverse.astype(BF16), sides).astype(BF16)
        carried, local = solved[:, :PAIR], solved[:, PAIR:]
        halves = jnp.concatenate(
            [
                jnp.concatenate([left(carried), left(local)], axis=1),
                jnp.concatenate([right(carried), right(local)], axis=1),
            ],
            axis=0,
        )
        taken = dot(read_removal, halves)
        reader_ref[:, lanes] = (read_in[:, lanes] - taken[:, :PAIR]).astype(BF16)
        local_ref[:, lanes] = sums[rows:] - taken[:, PAIR:]
        ends = dot_tn(solved, tail_removal[:, lanes])
        gathered = jnp.where(same, ends[:PAIR], 0.0).astype(BF16)
        added = jnp.where(
            same, dot_tn(values[:, lanes], tail_keys[:, lanes]) - ends[PAIR:], 0.0
        )
        gather_ref[0, p] = gathered
        add_ref[0, p] = added
        maps = maps_ref[p]
        maps = maps * fade[:, lanes] - dot(maps.astype(BF16), gathered)
        maps_ref[p, :PAIR, :] = maps[:PAIR]
        maps_ref[p, PAIR:, :] = maps[PAIR:] + added
    total_ref[...] = total_ref[...] * fade

    @pl.when(step == pl.num_programs(0) - 1)
    def _():
        low = iota((PAIR, PAIR), 1) < HEAD
        low_row = iota((1, PAIR), 1) < HEAD
        for p in range(pairs):
            lanes = slice(p * PAIR, (p + 1) * PAIR)
            total = total_ref[:, lanes]
            lost = eye * total - maps_ref[p, :PAIR, :]
            gained = maps_ref[p, PAIR:, :]
            lost = lost + pltpu.roll(lost, HEAD, 1)
            gained = gained + pltpu.roll(gained, HEAD, 1)
            both = jnp.where(low, lost, gained).astype(BF16)
            msg_ref[2 * p, :HEAD, :] = both[:HEAD]
            msg_ref[2 * p + 1, :HEAD, :] = both[HEAD:]
            for side in range(2):
                own = jnp.where(low_row == (side == 0), total, 0.0)
                own = jnp.broadcast_to(own, (16, PAIR))
                own = own + pltpu.roll(own, HEAD, 1)
                high, rest = two_parts(own)
                msg_ref[2 * p + side, HEAD:, :] = jnp.where(
                    iota((16, PAIR), 1) < HEAD, high.astype(F32), rest.astype(F32)
                ).astype(BF16)
        for s in range(GROUPS):
            sent_refs[s][...] = msg_ref[lax.rem(here_ref[0] + s, GROUPS)]


def message_parts(message):
    lost = message[:HEAD, :HEAD]
    gained = message[:HEAD, HEAD:].astype(F32)
    fades = message[HEAD : HEAD + 1, :].astype(F32)
    return lost, gained, fades[:, :HEAD] + fades[:, HEAD:]


def group_kernel(here_ref, *refs):
    in_refs, (prefix_ref, out_ref, met_ref) = refs[:GROUPS], refs[GROUPS:]
    for s in range(GROUPS):
        met_ref[lax.rem(here_ref[0] + GROUPS - s, GROUPS)] = in_refs[s][...]
    rows, cols = iota((HEAD, HEAD), 0), iota((HEAD, HEAD), 1)
    eye = (rows == cols).astype(F32)
    maps = jnp.concatenate([eye, jnp.zeros((HEAD, HEAD), F32)], axis=0)
    total = jnp.ones((1, HEAD), F32)
    for m in range(GROUPS):
        lost, gained, fade = message_parts(met_ref[m])
        prefix_ref[m] = maps
        moved = maps * fade - dot(maps.astype(BF16), lost)
        maps = jnp.concatenate([moved[:HEAD], moved[HEAD:] + gained], axis=0)
        total = total * fade
    both = jnp.concatenate([eye * total - maps[:HEAD], maps[HEAD:]], axis=1).astype(BF16)
    high, rest = two_parts(jnp.broadcast_to(total, (16, HEAD)))
    ends = jnp.concatenate([high.astype(F32), rest.astype(F32)], axis=1).astype(BF16)
    out_ref[:HEAD, :] = both
    out_ref[HEAD:, :] = ends


def enter_kernel(place_ref, *refs):
    in_refs = refs[: GROUPS - 1]
    prefix_ref = refs[GROUPS - 1]
    sent_refs, made_ref = refs[GROUPS:-1], refs[-1]
    state = jnp.zeros((HEAD, HEAD), F32)
    for s in range(GROUPS - 1, 0, -1):
        lost, gained, fade = message_parts(in_refs[s - 1][...])
        passed = state * fade - dot(state.astype(BF16), lost) + gained
        state = jnp.where(s <= place_ref[0], passed, state)
    narrow = state.astype(BF16)
    for m in range(GROUPS):
        entering = dot(narrow, prefix_ref[m, :HEAD, :].astype(BF16)) + prefix_ref[m, HEAD:, :]
        made_ref[m] = jnp.concatenate([entering, entering], axis=1).astype(BF16)
    for s in range(GROUPS):
        sent_refs[s][...] = made_ref[lax.rem(place_ref[1] + s, GROUPS)]


def readout_kernel(place_ref, *refs):
    enter_refs = refs[:GROUPS]
    reader_ref, local_ref, gather_ref, add_ref, fade_ref, gain_ref, weight_ref = refs[
        GROUPS : GROUPS + 7
    ]
    out_refs = refs[GROUPS + 7 : -2]
    state_ref, heads_ref = refs[-2:]
    step = pl.program_id(0)
    spans = len(out_refs)
    channels = reader_ref.shape[1]
    pairs = channels // PAIR
    same = block_ones()
    means = jnp.where(same, 1.0 / HEAD, 0.0).astype(BF16)

    @pl.when(step == 0)
    def _():
        for s in range(GROUPS):
            heads_ref[lax.rem(place_ref[1] + GROUPS - s, GROUPS)] = enter_refs[s][...]
        for p in range(pairs):
            entering = jnp.concatenate([heads_ref[2 * p], heads_ref[2 * p + 1]], axis=0)
            state_ref[p] = jnp.where(same, entering.astype(F32), 0.0)

    pieces = []
    for p in range(pairs):
        lanes = slice(p * PAIR, (p + 1) * PAIR)
        state = state_ref[p]
        narrow = state.astype(BF16)
        read = dot_nt(reader_ref[:, lanes], narrow) + local_ref[:, lanes]
        state_ref[p] = state * fade_ref[0, :, lanes] - dot(narrow, gather_ref[0, p]) + add_ref[0, p]
        centred = read - dot(read.astype(BF16), means)
        spread = dot((centred * centred).astype(BF16), means)
        pieces.append(
            (centred * lax.rsqrt(spread + GROUP_EPS) * gain_ref[:, lanes]).astype(BF16)
        )
    normed = jnp.concatenate(pieces, axis=1)
    result = dot(normed, weight_ref[...]).astype(BF16)
    for s in range(spans):

        @pl.when(lax.rem(step + spans - place_ref[2], spans) == s)
        def _():
            out_refs[s][...] = result


def hidden_kernel(x_ref, gate_ref, up_ref, out_ref):
    x = x_ref[...]
    gates = dot(x, gate_ref[...])
    uppers = dot(x, up_ref[...])
    out_ref[...] = (gates / (1.0 + jnp.exp(-gates)) * uppers).astype(BF16)


def down_kernel(h0, h1, h2, h3, own, before, after, far, out_ref):
    units = jnp.concatenate([h0[...], h1[...], h2[...], h3[...]], axis=1)
    weights = jnp.concatenate([own[...], before[...], after[...], far[...]], axis=0)
    out_ref[...] = dot(units, weights).astype(BF16)


def pack_kernel(x_ref, gain_ref, routes_ref, mix_ref, out_ref, high_ref, rest_ref):
    tokens = x_ref.shape[0]
    places = out_ref.shape[0]
    x = x_ref[...].astype(F32)
    normed = (
        x * lax.rsqrt(jnp.mean(x * x, axis=1, keepdims=True) + NORM_EPS) * gain_ref[...]
    ).astype(BF16)
    experts = places // CAPACITY
    listed = iota((tokens, experts), 1)
    first, second = routes_ref[:, 0:1], routes_ref[:, 1:2]
    first_mark = (first == listed).astype(F32)
    second_mark = (second == listed).astype(F32)
    before = (iota((tokens, tokens), 0) > iota((tokens, tokens), 1)).astype(F32).astype(BF16)
    earlier = dot(before, (first_mark + second_mark).astype(BF16))
    columns = iota((tokens, places), 1)
    table = jnp.zeros((tokens, places), F32)
    mix = jnp.zeros((tokens, places), F32)
    for named, mark, weight in (
        (first, first_mark, mix_ref[:, 0:1]),
        (second, second_mark, mix_ref[:, 1:2]),
    ):
        slot = jnp.sum(earlier * mark, axis=1, keepdims=True).astype(jnp.int32)
        here = columns == named * CAPACITY + slot
        table = table + here.astype(F32)
        mix = jnp.where(here, weight, mix)
    out_ref[...] = dot_tn(table.astype(BF16), normed).astype(BF16)
    high, rest = two_parts(mix)
    high_ref[...] = high
    rest_ref[...] = rest


def combine_kernel(high_ref, rest_ref, rows_ref, *refs):
    rows = rows_ref[...]
    refs[-1][...] = (dot(high_ref[...], rows) + dot(rest_ref[...], rows)).astype(BF16)


def whole(shape):
    return pl.BlockSpec(shape, lambda *_: (0,) * len(shape))


def estimate(flops, moved, transcendentals=0):
    return pl.CostEstimate(
        flops=int(flops), bytes_accessed=int(moved), transcendentals=int(transcendentals)
    )


SCALARS = pl.BlockSpec(memory_space=pltpu.SMEM)


def summarize(here, q, k, v, di, li, base, shift):
    rows, channels = q.shape
    heads = shift.shape[1]
    pairs = heads // 2
    spans = rows // SPAN
    block = pl.BlockSpec((SPAN, channels), lambda i: (i, 0))
    square = (1, pairs, PAIR, PAIR)
    return pl.pallas_call(
        summary_kernel,
        grid=(spans,),
        in_specs=[SCALARS]
        + [block] * 5
        + [whole((1, channels)), pl.BlockSpec((SPAN, heads), lambda i: (i, 0))],
        out_specs=[
            block,
            block,
            pl.BlockSpec(square, lambda i: (i, 0, 0, 0)),
            pl.BlockSpec(square, lambda i: (i, 0, 0, 0)),
            pl.BlockSpec((1, 1, channels), lambda i: (i, 0, 0)),
        ]
        + [whole((MSG_ROWS, PAIR))] * GROUPS,
        out_shape=[
            jax.ShapeDtypeStruct((rows, channels), BF16),
            jax.ShapeDtypeStruct((rows, channels), F32),
            jax.ShapeDtypeStruct((spans, pairs, PAIR, PAIR), BF16),
            jax.ShapeDtypeStruct((spans, pairs, PAIR, PAIR), F32),
            jax.ShapeDtypeStruct((spans, 1, channels), F32),
        ]
        + [jax.ShapeDtypeStruct((MSG_ROWS, PAIR), BF16)] * GROUPS,
        scratch_shapes=[
            pltpu.VMEM((pairs, 2 * PAIR, PAIR), F32),
            pltpu.VMEM((1, channels), F32),
            pltpu.VMEM((heads, MSG_ROWS, PAIR), BF16),
        ],
        compiler_params=pltpu.CompilerParams(dimension_semantics=("arbitrary",)),
        cost_estimate=estimate(2.0e10, 6 << 20, 2 << 20),
        name="summary",
    )(here, q, k, v, di, li, base, shift)


def group_scan(here, messages):
    return pl.pallas_call(
        group_kernel,
        in_specs=[SCALARS] + [pl.BlockSpec(memory_space=pltpu.VMEM)] * GROUPS,
        out_shape=[
            jax.ShapeDtypeStruct((GROUPS, 2 * HEAD, HEAD), F32),
            jax.ShapeDtypeStruct((MSG_ROWS, PAIR), BF16),
        ],
        scratch_shapes=[pltpu.VMEM((GROUPS, MSG_ROWS, PAIR), BF16)],
        cost_estimate=estimate(2.0e9, 1 << 20),
        name="group_scan",
    )(here, *messages)


def enter_states(place, totals, prefixes):
    return pl.pallas_call(
        enter_kernel,
        in_specs=[SCALARS] + [pl.BlockSpec(memory_space=pltpu.VMEM)] * GROUPS,
        out_shape=[jax.ShapeDtypeStruct((HEAD, PAIR), BF16)] * GROUPS,
        scratch_shapes=[pltpu.VMEM((GROUPS, HEAD, PAIR), BF16)],
        cost_estimate=estimate(2.0e9, 1 << 20),
        name="enter_states",
    )(place, *totals, prefixes)


def read_and_project(place, entering, reader, local, gather, add, fade, gain, weight):
    rows, channels = reader.shape
    pairs = channels // PAIR
    spans = rows // SPAN
    width = weight.shape[1]
    block = pl.BlockSpec((SPAN, channels), lambda i: (i, 0))
    square = pl.BlockSpec((1, pairs, PAIR, PAIR), lambda i: (i, 0, 0, 0))
    return pl.pallas_call(
        readout_kernel,
        grid=(spans,),
        in_specs=[SCALARS]
        + [whole((HEAD, PAIR))] * GROUPS
        + [
            block,
            block,
            square,
            square,
            pl.BlockSpec((1, 1, channels), lambda i: (i, 0, 0)),
            whole((1, channels)),
            whole(weight.shape),
        ],
        out_specs=[whole((SPAN, width))] * spans,
        out_shape=[jax.ShapeDtypeStruct((SPAN, width), BF16)] * spans,
        scratch_shapes=[
            pltpu.VMEM((pairs, PAIR, PAIR), F32),
            pltpu.VMEM((2 * pairs, HEAD, PAIR), BF16),
        ],
        compiler_params=pltpu.CompilerParams(dimension_semantics=("arbitrary",)),
        cost_estimate=estimate(5.0e9, 8 << 20),
        name="readout",
    )(place, *entering, reader, local, gather, add, fade, gain, weight)


def expert_hidden(x, gate, up):
    rows, width = x.shape
    units = gate.shape[1]
    tile = rows // 2
    return pl.pallas_call(
        hidden_kernel,
        grid=(2,),
        in_specs=[
            pl.BlockSpec((tile, width), lambda i: (i, 0)),
            whole(gate.shape),
            whole(up.shape),
        ],
        out_specs=pl.BlockSpec((tile, units), lambda i: (i, 0)),
        out_shape=jax.ShapeDtypeStruct((rows, units), BF16),
        compiler_params=pltpu.CompilerParams(dimension_semantics=("arbitrary",)),
        cost_estimate=estimate(4 * rows * width * units, 5 << 20, rows * units),
        name="hidden",
    )(x, gate, up)


def expert_down(hiddens, own, others, part):
    rows, units = hiddens[0].shape
    width = others[0].shape[1]
    tile = width // 2
    return pl.pallas_call(
        down_kernel,
        grid=(2,),
        in_specs=[whole(h.shape) for h in hiddens]
        + [pl.BlockSpec((units, tile), lambda i: (0, i + 2 * part))]
        + [pl.BlockSpec((units, tile), lambda i: (0, i))] * 3,
        out_specs=pl.BlockSpec((rows, tile), lambda i: (0, i)),
        out_shape=jax.ShapeDtypeStruct((rows, width), BF16),
        compiler_params=pltpu.CompilerParams(dimension_semantics=("arbitrary",)),
        cost_estimate=estimate(8 * rows * units * width, 4 << 20),
        name="down",
    )(*hiddens, own, *others)


def pack_rows(x, gain, routes, mix, places):
    tokens, width = x.shape
    return pl.pallas_call(
        pack_kernel,
        out_shape=[
            jax.ShapeDtypeStruct((places, width), BF16),
            jax.ShapeDtypeStruct((tokens, places), BF16),
            jax.ShapeDtypeStruct((tokens, places), BF16),
        ],
        cost_estimate=estimate(2.0e9, 3 << 20),
        name="pack",
    )(x, gain, routes, mix)


def combine_rows(high, rest, rows, part, into=()):
    tokens, places = high.shape
    width = rows.shape[1]
    tile = width // 2
    return pl.pallas_call(
        combine_kernel,
        grid=(2,),
        in_specs=[
            whole(high.shape),
            whole(rest.shape),
            pl.BlockSpec((places, tile), lambda i: (0, i)),
        ]
        + [pl.BlockSpec(memory_space=pl.ANY)] * len(into),
        out_specs=pl.BlockSpec((tokens, tile), lambda i: (0, i + 2 * part)),
        out_shape=jax.ShapeDtypeStruct((tokens, 2 * width), BF16),
        input_output_aliases={3: 0} if into else {},
        compiler_params=pltpu.CompilerParams(dimension_semantics=("arbitrary",)),
        cost_estimate=estimate(1.0e9, 3 << 20),
        name="combine",
    )(high, rest, rows, *into)


def ring(x, shift, axis="tp"):
    count = lax.axis_size(axis)
    return lax.ppermute(x, axis, [(i, (i + shift) % count) for i in range(count)])


def onward(x, shift, axis):
    count = lax.axis_size(axis)
    return lax.ppermute(x, axis, [(i, i + shift) for i in range(count - shift)])


def around(parts, axis):
    return [parts[0]] + [ring(part, n, axis) for n, part in enumerate(parts) if n]


def exchange(x, axis):
    return lax.all_to_all(x, axis, 0, 0, tiled=True)


def on_device(
    receptance,
    key_rows,
    value_rows,
    decay_input,
    learn_input,
    decay_base,
    decay_shift,
    channel_gain,
    out_weight,
    expert_input,
    expert_gain,
    routes,
    route_weight,
    gate_weight,
    up_weight,
    down_weight,
):
    ep_count = lax.axis_size(EP)
    _, model_width = expert_input.shape
    experts = gate_weight.shape[0] * ep_count
    places = experts * CAPACITY

    w_gate = gate_weight[0]
    w_up = up_weight[0]
    w_down = down_weight[0]
    cut = model_width // 2
    down_0, down_1 = w_down[:, :cut], w_down[:, cut:]
    gate_r, up_l = ring(w_gate, 1), ring(w_up, -1)
    gate_l, up_r = ring(w_gate, -1), ring(w_up, 1)
    gate_f, up_f = ring(gate_r, 1), ring(up_l, -1)
    down_0r, down_0l = ring(down_0, 1), ring(down_0, -1)
    down_1r, down_1l = ring(down_1, 1), ring(down_1, -1)
    down_0f, down_1f = ring(down_0r, 1), ring(down_1l, -1)

    outgoing, high, rest = pack_rows(
        expert_input, expert_gain.reshape(1, -1), routes, route_weight, places
    )
    arrived = exchange(
        outgoing.reshape(experts, CAPACITY, model_width), EP
    ).reshape(places, model_width)

    place = jnp.stack(
        [lax.axis_index("ep_0"), lax.axis_index(GROUP), lax.axis_index("tp")]
    ).astype(jnp.int32)
    reader, local, gather, add, fade, *messages = summarize(
        place[1:2],
        receptance,
        key_rows,
        value_rows,
        decay_input,
        learn_input,
        decay_base.reshape(1, -1),
        decay_shift,
    )
    prefixes, total = group_scan(place[1:2], around(messages, GROUP))
    totals = [onward(total, n, "ep_0") for n in range(1, GROUPS)]
    entered = enter_states(place, totals, prefixes)
    partial = read_and_project(
        place,
        around(entered, GROUP),
        reader,
        local,
        gather,
        add,
        fade,
        channel_gain.reshape(1, -1),
        out_weight,
    )
    shares = around(partial, "tp")
    mixer_out = sum(share.astype(F32) for share in shares).astype(BF16)

    hiddens = []
    for g, u in ((w_gate, w_up), (gate_r, up_r), (gate_l, up_l), (gate_f, up_f)):
        hiddens.append(expert_hidden(arrived, g, u))
    combined = ()
    for n, others in enumerate(((down_0r, down_0l, down_0f), (down_1r, down_1l, down_1f))):
        returning = expert_down(hiddens, w_down, others, n)
        if n:
            returning, returned = lax.optimization_barrier((returning, returned))
            combined = (combine_rows(high, rest, returned, 0),)
        returned = exchange(
            returning.reshape(ep_count, CAPACITY, cut), EP
        ).reshape(places, cut)
    return (mixer_out, combine_rows(high, rest, returned, 1, combined))


def solution(mesh):
    finer = Mesh(mesh.devices.reshape(8, 4, 2, mesh.shape["tp"]), ("ep_0", "ep_1", "ep_2", "tp"))
    placed = (
        P(EP, "tp"),
        P(EP, "tp"),
        P(EP, "tp"),
        P(EP, "tp"),
        P(EP, "tp"),
        P("tp"),
        P(EP, "tp"),
        P("tp"),
        P("tp", None),
        P(EP_TP, None),
        P(),
        P(EP_TP, None),
        P(EP_TP, None),
        P(EP, None, "tp"),
        P(EP, None, "tp"),
        P(EP, "tp", None),
    )

    return jax.shard_map(
        on_device,
        mesh=finer,
        in_specs=placed,
        out_specs=(P(EP_TP, None), P(EP_TP, None)),
        check_vma=False,
    )
```

```python
import functools

import jax
import jax.numpy as jnp
from jax import lax
from jax.experimental import pallas as pl
from jax.experimental.pallas import tpu as pltpu
from jax.sharding import Mesh
from jax.sharding import PartitionSpec as P


SPAN = 128
EP = ("ep_0", "ep_1", "ep_2")
GROUP = ("ep_1", "ep_2")
EP_TP = ("ep_0", "ep_1", "ep_2", "tp")
GROUPS = 8
HEAD = 64
PAIR = 128
MSG_ROWS = 80
CAPACITY = 8

NORM_EPS = 1e-06
GROUP_EPS = 0.00064
KEY_EPS = 1e-06
DECAY_SCALE = 0.6065306597126334

F32 = jnp.float32
BF16 = jnp.bfloat16


def dot(a, b):
    return lax.dot_general(a, b, (((1,), (0,)), ((), ())), preferred_element_type=F32)


def dot_nt(a, b):
    return lax.dot_general(a, b, (((1,), (1,)), ((), ())), preferred_element_type=F32)


def dot_tn(a, b):
    return lax.dot_general(a, b, (((0,), (0,)), ((), ())), preferred_element_type=F32)


def two_parts(x):
    high = x.astype(BF16)
    return high, (x - high.astype(F32)).astype(BF16)


def iota(shape, dim):
    return lax.broadcasted_iota(jnp.int32, shape, dim)


def block_ones():
    rows, cols = iota((PAIR, PAIR), 0), iota((PAIR, PAIR), 1)
    return (rows // HEAD) == (cols // HEAD)


def unit_lower_inverses(parts):
    size = parts[0].shape[0]
    rows, cols = iota((size, size), 0), iota((size, size), 1)
    eye = (rows == cols).astype(F32)
    start = 16
    inside = (rows // start) == (cols // start)
    powers = [jnp.where(inside, -a, 0.0) for a in parts]
    inverses = [eye + p for p in powers]
    reach = 2
    while reach < start:
        narrow = [p.astype(BF16) for p in powers]
        powers = [dot(p, p) for p in narrow]
        inverses = [
            inv + dot(inv.astype(BF16), p.astype(BF16))
            for inv, p in zip(inverses, powers)
        ]
        reach *= 2
    block = start
    while block < size:
        joined = ((rows // (2 * block)) == (cols // (2 * block))) & (
            (rows // block) != (cols // block)
        )
        narrow = [inv.astype(BF16) for inv in inverses]
        corners = [jnp.where(joined, a, 0.0).astype(BF16) for a in parts]
        moved = [dot(c, inv).astype(BF16) for c, inv in zip(corners, narrow)]
        inverses = [
            inv - dot(short, m) for inv, short, m in zip(inverses, narrow, moved)
        ]
        block *= 2
    return inverses


def summary_kernel(
    here_ref, q_ref, k_ref, v_ref, di_ref, li_ref, base_ref, shift_ref,
    reader_ref, local_ref, gather_ref, add_ref, fade_ref, *rest_refs,
):
    sent_refs, (maps_ref, total_ref, msg_ref) = rest_refs[:GROUPS], rest_refs[GROUPS:]
    step = pl.program_id(0)
    rows, channels = q_ref.shape
    heads = shift_ref.shape[0]
    pairs = heads // 2
    same = block_ones()
    same_f = same.astype(F32)
    same_b = same_f.astype(BF16)
    row2, col2 = iota((PAIR, PAIR), 0), iota((PAIR, PAIR), 1)
    eye = (row2 == col2).astype(F32)

    @pl.when(step == 0)
    def _():
        for p in range(pairs):
            maps_ref[p, :PAIR, :] = eye
            maps_ref[p, PAIR:, :] = jnp.zeros((PAIR, PAIR), F32)
        total_ref[...] = jnp.ones_like(total_ref)

    spread = (
        (iota((heads, channels), 1) // HEAD) == iota((heads, channels), 0)
    ).astype(F32).astype(BF16)
    shift_high, shift_low = two_parts(shift_ref[...])
    pre = (
        di_ref[...].astype(F32)
        + base_ref[...]
        + (dot_tn(shift_high, spread) + dot_tn(shift_low, spread))
    )
    log_decay = -DECAY_SCALE / (1.0 + jnp.exp(-pre))
    tri_rows, tri_cols = iota((rows, rows), 0), iota((rows, rows), 1)
    inclusive = tri_rows >= tri_cols
    strict = tri_rows > tri_cols
    tri = inclusive.astype(F32).astype(BF16)
    decay_high, decay_low = two_parts(log_decay)
    cum = dot(tri, decay_high) + dot(tri, decay_low)
    middle = cum[rows // 2 - 1 : rows // 2, :]
    ending = cum[rows - 1 : rows, :]
    grow = jnp.exp(cum - middle)
    grow_before = grow * jnp.exp(-log_decay)
    shrink = jnp.exp(middle - cum)
    from_start = jnp.exp(middle)
    to_end = jnp.exp(ending - middle)
    fade = jnp.exp(ending)
    fade_ref[0] = fade

    keys = k_ref[...].astype(F32)
    recept = q_ref[...].astype(F32)
    squares_high, squares_low = two_parts(keys * keys)
    lengths = jnp.concatenate(
        [
            dot(squares_high[:, p * PAIR : (p + 1) * PAIR], same_b)
            + dot(squares_low[:, p * PAIR : (p + 1) * PAIR], same_b)
            for p in range(pairs)
        ],
        axis=1,
    )
    unit = keys * lax.rsqrt(lengths + KEY_EPS)
    removal = unit / (1.0 + jnp.exp(-li_ref[...].astype(F32)))

    probes_f = unit * grow_before
    queries_f = recept * grow
    back_removal_f = removal * shrink
    back_keys_f = keys * shrink
    probes = probes_f.astype(BF16)
    queries = queries_f.astype(BF16)
    back_removal = back_removal_f.astype(BF16)
    back_keys = back_keys_f.astype(BF16)
    carried_in = (probes_f * from_start).astype(BF16)
    read_in = queries_f * from_start
    tail_removal = (back_removal_f * to_end).astype(BF16)
    tail_keys = (back_keys_f * to_end).astype(BF16)
    values = v_ref[...]

    first = iota((rows, PAIR), 1) < HEAD
    none = jnp.zeros((rows, PAIR), BF16)

    def left(x):
        return jnp.where(first, x, none)

    def right(x):
        return jnp.where(first, none, x)

    kept = []
    strict_parts = []
    for p in range(pairs):
        lanes = slice(p * PAIR, (p + 1) * PAIR)
        pr, qu = probes[:, lanes], queries[:, lanes]
        outer = jnp.concatenate([left(pr), right(pr), left(qu), right(qu)], axis=0)
        inner = jnp.concatenate([back_removal[:, lanes], back_keys[:, lanes]], axis=0)
        products = dot_nt(outer, inner)
        strict_parts.append(jnp.where(strict, products[0:rows, 0:rows], 0.0))
        strict_parts.append(jnp.where(strict, products[rows : 2 * rows, 0:rows], 0.0))
        pair_keys = jnp.concatenate(
            [
                jnp.where(strict, products[0:rows, rows:], 0.0),
                jnp.where(strict, products[rows : 2 * rows, rows:], 0.0),
            ],
            axis=1,
        ).astype(BF16)
        read_keys = jnp.concatenate(
            [
                jnp.where(inclusive, products[2 * rows : 3 * rows, rows:], 0.0),
                jnp.where(inclusive, products[3 * rows :, rows:], 0.0),
            ],
            axis=1,
        ).astype(BF16)
        read_removal = jnp.concatenate(
            [
                jnp.where(inclusive, products[2 * rows : 3 * rows, 0:rows], 0.0),
                jnp.where(inclusive, products[3 * rows :, 0:rows], 0.0),
            ],
            axis=1,
        ).astype(BF16)
        va = values[:, lanes]
        stacked = jnp.concatenate([left(va), right(va)], axis=0)
        sums = dot(jnp.concatenate([pair_keys, read_keys], axis=0), stacked)
        kept.append((read_removal, sums))

    inverses = unit_lower_inverses(strict_parts)

    for p in range(pairs):
        lanes = slice(p * PAIR, (p + 1) * PAIR)
        read_removal, sums = kept[p]
        weights = sums[:rows].astype(BF16)
        carry = carried_in[:, lanes]
        sides = jnp.concatenate(
            [
                jnp.concatenate([left(carry), left(weights)], axis=1),
                jnp.concatenate([right(carry), right(weights)], axis=1),
            ],
            axis=0,
        )
        inverse = jnp.concatenate([inverses[2 * p], inverses[2 * p + 1]], axis=1)
        solved = dot(inverse.astype(BF16), sides).astype(BF16)
        carried, local = solved[:, :PAIR], solved[:, PAIR:]
        halves = jnp.concatenate(
            [
                jnp.concatenate([left(carried), left(local)], axis=1),
                jnp.concatenate([right(carried), right(local)], axis=1),
            ],
            axis=0,
        )
        taken = dot(read_removal, halves)
        reader_ref[:, lanes] = (read_in[:, lanes] - taken[:, :PAIR]).astype(BF16)
        local_ref[:, lanes] = sums[rows:] - taken[:, PAIR:]
        ends = dot_tn(solved, tail_removal[:, lanes])
        gathered = jnp.where(same, ends[:PAIR], 0.0).astype(BF16)
        added = jnp.where(
            same, dot_tn(values[:, lanes], tail_keys[:, lanes]) - ends[PAIR:], 0.0
        )
        gather_ref[0, p] = gathered
        add_ref[0, p] = added
        maps = maps_ref[p]
        maps = maps * fade[:, lanes] - dot(maps.astype(BF16), gathered)
        maps_ref[p, :PAIR, :] = maps[:PAIR]
        maps_ref[p, PAIR:, :] = maps[PAIR:] + added
    total_ref[...] = total_ref[...] * fade

    @pl.when(step == pl.num_programs(0) - 1)
    def _():
        low = iota((PAIR, PAIR), 1) < HEAD
        low_row = iota((1, PAIR), 1) < HEAD
        for p in range(pairs):
            lanes = slice(p * PAIR, (p + 1) * PAIR)
            total = total_ref[:, lanes]
            lost = eye * total - maps_ref[p, :PAIR, :]
            gained = maps_ref[p, PAIR:, :]
            lost = lost + pltpu.roll(lost, HEAD, 1)
            gained = gained + pltpu.roll(gained, HEAD, 1)
            both = jnp.where(low, lost, gained).astype(BF16)
            msg_ref[2 * p, :HEAD, :] = both[:HEAD]
            msg_ref[2 * p + 1, :HEAD, :] = both[HEAD:]
            for side in range(2):
                own = jnp.where(low_row == (side == 0), total, 0.0)
                own = jnp.broadcast_to(own, (16, PAIR))
                own = own + pltpu.roll(own, HEAD, 1)
                high, rest = two_parts(own)
                msg_ref[2 * p + side, HEAD:, :] = jnp.where(
                    iota((16, PAIR), 1) < HEAD, high.astype(F32), rest.astype(F32)
                ).astype(BF16)
        for s in range(GROUPS):
            sent_refs[s][...] = msg_ref[lax.rem(here_ref[0] + s, GROUPS)]


def message_parts(message):
    lost = message[:HEAD, :HEAD]
    gained = message[:HEAD, HEAD:].astype(F32)
    fades = message[HEAD : HEAD + 1, :].astype(F32)
    return lost, gained, fades[:, :HEAD] + fades[:, HEAD:]


def group_kernel(here_ref, *refs):
    in_refs, (prefix_ref, out_ref, met_ref) = refs[:GROUPS], refs[GROUPS:]
    for s in range(GROUPS):
        met_ref[lax.rem(here_ref[0] + GROUPS - s, GROUPS)] = in_refs[s][...]
    rows, cols = iota((HEAD, HEAD), 0), iota((HEAD, HEAD), 1)
    eye = (rows == cols).astype(F32)
    maps = jnp.concatenate([eye, jnp.zeros((HEAD, HEAD), F32)], axis=0)
    total = jnp.ones((1, HEAD), F32)
    for m in range(GROUPS):
        lost, gained, fade = message_parts(met_ref[m])
        prefix_ref[m] = maps
        moved = maps * fade - dot(maps.astype(BF16), lost)
        maps = jnp.concatenate([moved[:HEAD], moved[HEAD:] + gained], axis=0)
        total = total * fade
    both = jnp.concatenate([eye * total - maps[:HEAD], maps[HEAD:]], axis=1).astype(BF16)
    high, rest = two_parts(jnp.broadcast_to(total, (16, HEAD)))
    ends = jnp.concatenate([high.astype(F32), rest.astype(F32)], axis=1).astype(BF16)
    for z in range(out_ref.shape[0]):
        out_ref[z, :HEAD, :] = both
        out_ref[z, HEAD:, :] = ends


def enter_kernel(here_ref, in_ref, prefix_ref, out_ref):
    state = jnp.zeros((HEAD, HEAD), F32)
    for z in range(in_ref.shape[0]):
        lost, gained, fade = message_parts(in_ref[z])
        passed = state * fade - dot(state.astype(BF16), lost) + gained
        state = jnp.where(z < here_ref[0], passed, state)
    narrow = state.astype(BF16)
    for m in range(out_ref.shape[0]):
        entering = dot(narrow, prefix_ref[m, :HEAD, :].astype(BF16)) + prefix_ref[m, HEAD:, :]
        out_ref[m] = jnp.concatenate([entering, entering], axis=1).astype(BF16)


def readout_kernel(
    here_ref, enter_ref, reader_ref, local_ref, gather_ref, add_ref, fade_ref, gain_ref,
    weight_ref, *refs,
):
    out_refs, state_ref = refs[:-1], refs[-1]
    step = pl.program_id(0)
    spans = len(out_refs)
    channels = reader_ref.shape[1]
    pairs = channels // PAIR
    same = block_ones()
    means = jnp.where(same, 1.0 / HEAD, 0.0).astype(BF16)

    @pl.when(step == 0)
    def _():
        for p in range(pairs):
            entering = jnp.concatenate([enter_ref[2 * p], enter_ref[2 * p + 1]], axis=0)
            state_ref[p] = jnp.where(same, entering.astype(F32), 0.0)

    pieces = []
    for p in range(pairs):
        lanes = slice(p * PAIR, (p + 1) * PAIR)
        state = state_ref[p]
        narrow = state.astype(BF16)
        read = dot_nt(reader_ref[:, lanes], narrow) + local_ref[:, lanes]
        state_ref[p] = state * fade_ref[0, :, lanes] - dot(narrow, gather_ref[0, p]) + add_ref[0, p]
        centred = read - dot(read.astype(BF16), means)
        spread = dot((centred * centred).astype(BF16), means)
        pieces.append(
            (centred * lax.rsqrt(spread + GROUP_EPS) * gain_ref[:, lanes]).astype(BF16)
        )
    normed = jnp.concatenate(pieces, axis=1)
    result = dot(normed, weight_ref[...]).astype(BF16)
    for s in range(spans):

        @pl.when(lax.rem(step + spans - here_ref[0], spans) == s)
        def _():
            out_refs[s][...] = result


def hidden_kernel(x_hbm, *refs):
    weights, (out_ref, x_ref, weight_refs, sems) = refs[:8], refs[8:]
    fetch_x = pltpu.make_async_copy(x_hbm, x_ref, sems.at[8])
    fetch_x.start()
    fetches = [
        pltpu.make_async_copy(w, weight_refs.at[n], sems.at[n]) for n, w in enumerate(weights)
    ]
    for fetch in fetches:
        fetch.start()
    fetch_x.wait()
    units = weight_refs.shape[2]
    for q in range(4):
        fetches[2 * q].wait()
        gates = dot(x_ref[...], weight_refs[2 * q])
        fetches[2 * q + 1].wait()
        uppers = dot(x_ref[...], weight_refs[2 * q + 1])
        out_ref[:, q * units : (q + 1) * units] = (
            gates / (1.0 + jnp.exp(-gates)) * uppers
        ).astype(BF16)


def down_kernel(part, hidden_ref, own_hbm, before, after, far, out_ref, own_ref, sem):
    units, width = before.shape
    fetch = pltpu.make_async_copy(
        own_hbm.at[:, part * width : (part + 1) * width], own_ref, sem
    )
    fetch.start()
    others = jnp.concatenate([before[...], after[...], far[...]], axis=0)
    result = dot(hidden_ref[:, units:], others)
    fetch.wait()
    out_ref[...] = (result + dot(hidden_ref[:, :units], own_ref[...])).astype(BF16)


def pack_kernel(x_ref, gain_ref, routes_ref, mix_ref, out_ref, high_ref, rest_ref):
    tokens = x_ref.shape[0]
    places = out_ref.shape[0]
    x = x_ref[...].astype(F32)
    normed = (
        x * lax.rsqrt(jnp.mean(x * x, axis=1, keepdims=True) + NORM_EPS) * gain_ref[...]
    ).astype(BF16)
    experts = places // CAPACITY
    listed = iota((experts, tokens), 0)
    first, second = routes_ref[0:1, :], routes_ref[1:2, :]
    first_mark = (first == listed).astype(F32)
    second_mark = (second == listed).astype(F32)
    before = (iota((tokens, tokens), 0) < iota((tokens, tokens), 1)).astype(F32).astype(BF16)
    earlier = dot((first_mark + second_mark).astype(BF16), before)
    rows = iota((places, tokens), 0)
    table = jnp.zeros((places, tokens), F32)
    mix = jnp.zeros((places, tokens), F32)
    for named, mark, weight in (
        (first, first_mark, mix_ref[0:1, :]),
        (second, second_mark, mix_ref[1:2, :]),
    ):
        slot = jnp.sum(earlier * mark, axis=0, keepdims=True).astype(jnp.int32)
        here = rows == named * CAPACITY + slot
        table = table + here.astype(F32)
        mix = jnp.where(here, weight, mix)
    out_ref[...] = dot(table.astype(BF16), normed).astype(BF16)
    high, rest = two_parts(mix)
    high_ref[...] = high
    rest_ref[...] = rest


def combine_kernel(high_ref, rest_ref, rows_ref, *refs):
    rows = rows_ref[...]
    refs[-1][...] = (dot_tn(high_ref[...], rows) + dot_tn(rest_ref[...], rows)).astype(BF16)


def whole(shape):
    return pl.BlockSpec(shape, lambda *_: (0,) * len(shape))


def estimate(flops, moved, transcendentals=0):
    return pl.CostEstimate(
        flops=int(flops), bytes_accessed=int(moved), transcendentals=int(transcendentals)
    )


SCALARS = pl.BlockSpec(memory_space=pltpu.SMEM)


def summarize(here, q, k, v, di, li, base, shift):
    rows, channels = q.shape
    heads = shift.shape[0]
    pairs = heads // 2
    spans = rows // SPAN
    block = pl.BlockSpec((SPAN, channels), lambda i: (i, 0))
    square = (1, pairs, PAIR, PAIR)
    return pl.pallas_call(
        summary_kernel,
        grid=(spans,),
        in_specs=[SCALARS]
        + [block] * 5
        + [whole((1, channels)), pl.BlockSpec((heads, SPAN), lambda i: (0, i))],
        out_specs=[
            block,
            block,
            pl.BlockSpec(square, lambda i: (i, 0, 0, 0)),
            pl.BlockSpec(square, lambda i: (i, 0, 0, 0)),
            pl.BlockSpec((1, 1, channels), lambda i: (i, 0, 0)),
        ]
        + [whole((MSG_ROWS, PAIR))] * GROUPS,
        out_shape=[
            jax.ShapeDtypeStruct((rows, channels), BF16),
            jax.ShapeDtypeStruct((rows, channels), F32),
            jax.ShapeDtypeStruct((spans, pairs, PAIR, PAIR), BF16),
            jax.ShapeDtypeStruct((spans, pairs, PAIR, PAIR), F32),
            jax.ShapeDtypeStruct((spans, 1, channels), F32),
        ]
        + [jax.ShapeDtypeStruct((MSG_ROWS, PAIR), BF16)] * GROUPS,
        scratch_shapes=[
            pltpu.VMEM((pairs, 2 * PAIR, PAIR), F32),
            pltpu.VMEM((1, channels), F32),
            pltpu.VMEM((heads, MSG_ROWS, PAIR), BF16),
        ],
        compiler_params=pltpu.CompilerParams(dimension_semantics=("arbitrary",)),
        cost_estimate=estimate(2.0e10, 6 << 20, 2 << 20),
        name="summary",
    )(here, q, k, v, di, li, base, shift)


def group_scan(here, messages, copies):
    return pl.pallas_call(
        group_kernel,
        in_specs=[SCALARS] + [pl.BlockSpec(memory_space=pltpu.VMEM)] * GROUPS,
        out_shape=[
            jax.ShapeDtypeStruct((GROUPS, 2 * HEAD, HEAD), F32),
            jax.ShapeDtypeStruct((copies, MSG_ROWS, PAIR), BF16),
        ],
        scratch_shapes=[pltpu.VMEM((GROUPS, MSG_ROWS, PAIR), BF16)],
        cost_estimate=estimate(2.0e9, 1 << 20),
        name="group_scan",
    )(here, *map(in_vmem, messages))


def enter_states(here, totals, prefixes):
    return pl.pallas_call(
        enter_kernel,
        in_specs=[SCALARS] + [pl.BlockSpec(memory_space=pltpu.VMEM)] * 2,
        out_shape=jax.ShapeDtypeStruct((prefixes.shape[0], HEAD, PAIR), BF16),
        cost_estimate=estimate(2.0e9, 1 << 20),
        name="enter_states",
    )(here, in_vmem(totals), prefixes)


def read_and_project(here, entering, reader, local, gather, add, fade, gain, weight):
    rows, channels = reader.shape
    pairs = channels // PAIR
    spans = rows // SPAN
    width = weight.shape[1]
    block = pl.BlockSpec((SPAN, channels), lambda i: (i, 0))
    square = pl.BlockSpec((1, pairs, PAIR, PAIR), lambda i: (i, 0, 0, 0))
    return pl.pallas_call(
        readout_kernel,
        grid=(spans,),
        in_specs=[
            SCALARS,
            IN_VMEM,
            block,
            block,
            square,
            square,
            pl.BlockSpec((1, 1, channels), lambda i: (i, 0, 0)),
            whole((1, channels)),
            whole(weight.shape),
        ],
        out_specs=[whole((SPAN, width))] * spans,
        out_shape=[jax.ShapeDtypeStruct((SPAN, width), BF16)] * spans,
        scratch_shapes=[pltpu.VMEM((pairs, PAIR, PAIR), F32)],
        compiler_params=pltpu.CompilerParams(dimension_semantics=("arbitrary",)),
        cost_estimate=estimate(5.0e9, 8 << 20),
        name="readout",
    )(here, in_vmem(entering), reader, local, gather, add, fade, gain, weight)


IN_HBM = pl.BlockSpec(memory_space=pltpu.HBM)
IN_VMEM = pl.BlockSpec(memory_space=pltpu.VMEM)


def expert_hidden(x, weights):
    rows, width = x.shape
    units = weights[0].shape[1]
    count = len(weights)
    return pl.pallas_call(
        hidden_kernel,
        in_specs=[IN_HBM] * (1 + count),
        out_specs=IN_VMEM,
        out_shape=jax.ShapeDtypeStruct((rows, units * count // 2), BF16),
        scratch_shapes=[
            pltpu.VMEM((rows, width), BF16),
            pltpu.VMEM((count, width, units), BF16),
            pltpu.SemaphoreType.DMA((count + 1,)),
        ],
        cost_estimate=estimate(2 * rows * width * units * count, 11 << 20, rows * units * 4),
        name="hidden",
    )(pltpu.with_memory_space_constraint(x, pltpu.HBM), *weights)


def expert_down(hidden, own, others, part):
    rows = hidden.shape[0]
    units, width = others[0].shape
    return pl.pallas_call(
        functools.partial(down_kernel, part),
        in_specs=[IN_VMEM, IN_HBM] + [IN_VMEM] * 3,
        out_specs=IN_VMEM,
        out_shape=jax.ShapeDtypeStruct((rows, width), BF16),
        scratch_shapes=[
            pltpu.VMEM((units, width), BF16),
            pltpu.SemaphoreType.DMA,
        ],
        cost_estimate=estimate(8 * rows * units * width, 4 << 20),
        name="down",
    )(hidden, own, *map(in_vmem, others))


def pack_rows(x, gain, routes, mix, places):
    tokens, width = x.shape
    return pl.pallas_call(
        pack_kernel,
        out_shape=[
            jax.ShapeDtypeStruct((places, width), BF16),
            jax.ShapeDtypeStruct((places, tokens), BF16),
            jax.ShapeDtypeStruct((places, tokens), BF16),
        ],
        cost_estimate=estimate(2.0e9, 3 << 20),
        name="pack",
    )(x, gain, routes, mix)


def combine_rows(high, rest, rows, part, into=()):
    _, tokens = high.shape
    width = rows.shape[1]
    return pl.pallas_call(
        combine_kernel,
        grid=(1,),
        in_specs=[IN_VMEM] * 3 + [IN_HBM] * len(into),
        out_specs=pl.BlockSpec((tokens, width), lambda i: (0, part)),
        out_shape=jax.ShapeDtypeStruct((tokens, 2 * width), BF16),
        input_output_aliases={3: 0} if into else {},
        compiler_params=pltpu.CompilerParams(dimension_semantics=("arbitrary",)),
        cost_estimate=estimate(1.0e9, 3 << 20),
        name="combine",
    )(high, rest, in_vmem(rows), *into)


def ring(x, shift, axis="tp"):
    count = lax.axis_size(axis)
    return lax.ppermute(x, axis, [(i, (i + shift) % count) for i in range(count)])


def around(parts, axis):
    return [parts[0]] + [ring(part, n, axis) for n, part in enumerate(parts) if n]


def in_vmem(x):
    return pltpu.with_memory_space_constraint(x, pltpu.VMEM)


def exchange(x, axis):
    return lax.all_to_all(x, axis, 0, 0, tiled=True)


def on_device(
    receptance,
    key_rows,
    value_rows,
    decay_input,
    learn_input,
    decay_base,
    decay_shift,
    channel_gain,
    out_weight,
    expert_input,
    expert_gain,
    routes,
    route_weight,
    gate_weight,
    up_weight,
    down_weight,
):
    ep_count = lax.axis_size(EP)
    _, model_width = expert_input.shape
    experts = gate_weight.shape[0] * ep_count
    places = experts * CAPACITY

    w_gate = gate_weight[0]
    w_up = up_weight[0]
    w_down = down_weight[0]
    cut = model_width // 2
    down_0, down_1 = w_down[:, :cut], w_down[:, cut:]
    gate_r, up_l = ring(w_gate, 1), ring(w_up, -1)
    gate_l, up_r = ring(w_gate, -1), ring(w_up, 1)
    gate_f, up_f = ring(gate_r, 1), ring(up_l, -1)
    down_0r, down_0l = ring(down_0, 1), ring(down_0, -1)
    down_1r, down_1l = ring(down_1, 1), ring(down_1, -1)
    down_0f, down_1f = ring(down_0r, 1), ring(down_1l, -1)

    outgoing, high, rest = pack_rows(
        expert_input, expert_gain.reshape(1, -1), routes.T, route_weight.T, places
    )
    arrived = exchange(
        outgoing.reshape(experts, CAPACITY, model_width), EP
    ).reshape(places, model_width)

    def here(axis):
        return lax.axis_index(axis).astype(jnp.int32).reshape(1)

    reader, local, gather, add, fade, *messages = summarize(
        here(GROUP),
        receptance,
        key_rows,
        value_rows,
        decay_input,
        learn_input,
        decay_base.reshape(1, -1),
        decay_shift.T,
    )
    prefixes, totals = group_scan(
        here(GROUP), around(messages, GROUP), lax.axis_size("ep_0")
    )
    entered = enter_states(here("ep_0"), exchange(totals, "ep_0"), prefixes)
    partial = read_and_project(
        here("tp"),
        exchange(entered, GROUP),
        reader,
        local,
        gather,
        add,
        fade,
        channel_gain.reshape(1, -1),
        out_weight,
    )
    shares = around(partial, "tp")
    mixer_out = sum(share.astype(F32) for share in shares).astype(BF16)

    hiddens = expert_hidden(
        arrived, [w_gate, w_up, gate_r, up_r, gate_l, up_l, gate_f, up_f]
    )
    combined = ()
    for n, others in enumerate(((down_0r, down_0l, down_0f), (down_1r, down_1l, down_1f))):
        returning = expert_down(hiddens, w_down, others, n)
        if n:
            returning, returned = lax.optimization_barrier((returning, returned))
            combined = (combine_rows(high, rest, returned, 0),)
        returned = exchange(
            returning.reshape(ep_count, CAPACITY, cut), EP
        ).reshape(places, cut)
    return (mixer_out, combine_rows(high, rest, returned, 1, combined))


def solution(mesh):
    finer = Mesh(mesh.devices.reshape(8, 4, 2, mesh.shape["tp"]), ("ep_0", "ep_1", "ep_2", "tp"))
    placed = (
        P(EP, "tp"),
        P(EP, "tp"),
        P(EP, "tp"),
        P(EP, "tp"),
        P(EP, "tp"),
        P("tp"),
        P(EP, "tp"),
        P("tp"),
        P("tp", None),
        P(EP_TP, None),
        P(),
        P(EP_TP, None),
        P(EP_TP, None),
        P(EP, None, "tp"),
        P(EP, None, "tp"),
        P(EP, "tp", None),
    )

    return jax.shard_map(
        on_device,
        mesh=finer,
        in_specs=placed,
        out_specs=(P(EP_TP, None), P(EP_TP, None)),
        check_vma=False,
    )
```

```python
import jax
import jax.numpy as jnp
from jax import lax
from jax.experimental import pallas as pl
from jax.experimental.pallas import tpu as pltpu
from jax.sharding import Mesh
from jax.sharding import PartitionSpec as P


SPAN = 128
EP = ("ep_0", "ep_1", "ep_2")
GROUP = ("ep_1", "ep_2")
EP_TP = ("ep_0", "ep_1", "ep_2", "tp")
GROUPS = 8
HEAD = 64
PAIR = 128
MSG_ROWS = 80
CAPACITY = 8

NORM_EPS = 1e-06
GROUP_EPS = 0.00064
KEY_EPS = 1e-06
DECAY_SCALE = 0.6065306597126334

F32 = jnp.float32
BF16 = jnp.bfloat16


def dot(a, b):
    return lax.dot_general(a, b, (((1,), (0,)), ((), ())), preferred_element_type=F32)


def dot_nt(a, b):
    return lax.dot_general(a, b, (((1,), (1,)), ((), ())), preferred_element_type=F32)


def dot_tn(a, b):
    return lax.dot_general(a, b, (((0,), (0,)), ((), ())), preferred_element_type=F32)


def two_parts(x):
    high = x.astype(BF16)
    return high, (x - high.astype(F32)).astype(BF16)


def iota(shape, dim):
    return lax.broadcasted_iota(jnp.int32, shape, dim)


def block_ones():
    rows, cols = iota((PAIR, PAIR), 0), iota((PAIR, PAIR), 1)
    return (rows // HEAD) == (cols // HEAD)


def unit_lower_inverses(parts):
    size = parts[0].shape[0]
    rows, cols = iota((size, size), 0), iota((size, size), 1)
    eye = (rows == cols).astype(F32)
    start = 16
    inside = (rows // start) == (cols // start)
    powers = [jnp.where(inside, -a, 0.0) for a in parts]
    inverses = [eye + p for p in powers]
    reach = 2
    while reach < start:
        narrow = [p.astype(BF16) for p in powers]
        powers = [dot(p, p) for p in narrow]
        inverses = [
            inv + dot(inv.astype(BF16), p.astype(BF16))
            for inv, p in zip(inverses, powers)
        ]
        reach *= 2
    block = start
    while block < size:
        joined = ((rows // (2 * block)) == (cols // (2 * block))) & (
            (rows // block) != (cols // block)
        )
        narrow = [inv.astype(BF16) for inv in inverses]
        corners = [jnp.where(joined, a, 0.0).astype(BF16) for a in parts]
        moved = [dot(c, inv).astype(BF16) for c, inv in zip(corners, narrow)]
        inverses = [
            inv - dot(short, m) for inv, short, m in zip(inverses, narrow, moved)
        ]
        block *= 2
    return inverses


def summary_kernel(
    here_ref, q_ref, k_ref, v_ref, di_ref, li_ref, base_ref, shift_ref,
    reader_ref, local_ref, gather_ref, add_ref, fade_ref, *rest_refs,
):
    sent_refs, (maps_ref, total_ref, msg_ref) = rest_refs[:GROUPS], rest_refs[GROUPS:]
    step = pl.program_id(0)
    rows, channels = q_ref.shape
    heads = shift_ref.shape[0]
    pairs = heads // 2
    same = block_ones()
    same_f = same.astype(F32)
    same_b = same_f.astype(BF16)
    row2, col2 = iota((PAIR, PAIR), 0), iota((PAIR, PAIR), 1)
    eye = (row2 == col2).astype(F32)

    @pl.when(step == 0)
    def _():
        for p in range(pairs):
            maps_ref[p, :PAIR, :] = eye
            maps_ref[p, PAIR:, :] = jnp.zeros((PAIR, PAIR), F32)
        total_ref[...] = jnp.ones_like(total_ref)

    spread = (
        (iota((heads, channels), 1) // HEAD) == iota((heads, channels), 0)
    ).astype(F32).astype(BF16)
    shift_high, shift_low = two_parts(shift_ref[...])
    pre = (
        di_ref[...].astype(F32)
        + base_ref[...]
        + (dot_tn(shift_high, spread) + dot_tn(shift_low, spread))
    )
    log_decay = -DECAY_SCALE / (1.0 + jnp.exp(-pre))
    tri_rows, tri_cols = iota((rows, rows), 0), iota((rows, rows), 1)
    inclusive = tri_rows >= tri_cols
    strict = tri_rows > tri_cols
    tri = inclusive.astype(F32).astype(BF16)
    decay_high, decay_low = two_parts(log_decay)
    cum = dot(tri, decay_high) + dot(tri, decay_low)
    middle = cum[rows // 2 - 1 : rows // 2, :]
    ending = cum[rows - 1 : rows, :]
    grow = jnp.exp(cum - middle)
    grow_before = grow * jnp.exp(-log_decay)
    shrink = jnp.exp(middle - cum)
    from_start = jnp.exp(middle)
    to_end = jnp.exp(ending - middle)
    fade = jnp.exp(ending)
    fade_ref[0] = fade

    keys = k_ref[...].astype(F32)
    recept = q_ref[...].astype(F32)
    squares_high, squares_low = two_parts(keys * keys)
    lengths = jnp.concatenate(
        [
            dot(squares_high[:, p * PAIR : (p + 1) * PAIR], same_b)
            + dot(squares_low[:, p * PAIR : (p + 1) * PAIR], same_b)
            for p in range(pairs)
        ],
        axis=1,
    )
    unit = keys * lax.rsqrt(lengths + KEY_EPS)
    removal = unit / (1.0 + jnp.exp(-li_ref[...].astype(F32)))

    probes_f = unit * grow_before
    queries_f = recept * grow
    back_removal_f = removal * shrink
    back_keys_f = keys * shrink
    probes = probes_f.astype(BF16)
    queries = queries_f.astype(BF16)
    back_removal = back_removal_f.astype(BF16)
    back_keys = back_keys_f.astype(BF16)
    carried_in = (probes_f * from_start).astype(BF16)
    read_in = queries_f * from_start
    tail_removal = (back_removal_f * to_end).astype(BF16)
    tail_keys = (back_keys_f * to_end).astype(BF16)
    values = v_ref[...]

    first = iota((rows, PAIR), 1) < HEAD
    none = jnp.zeros((rows, PAIR), BF16)

    def left(x):
        return jnp.where(first, x, none)

    def right(x):
        return jnp.where(first, none, x)

    kept = []
    strict_parts = []
    for p in range(pairs):
        lanes = slice(p * PAIR, (p + 1) * PAIR)
        pr, qu = probes[:, lanes], queries[:, lanes]
        outer = jnp.concatenate([left(pr), right(pr), left(qu), right(qu)], axis=0)
        inner = jnp.concatenate([back_removal[:, lanes], back_keys[:, lanes]], axis=0)
        products = dot_nt(outer, inner)
        strict_parts.append(jnp.where(strict, products[0:rows, 0:rows], 0.0))
        strict_parts.append(jnp.where(strict, products[rows : 2 * rows, 0:rows], 0.0))
        pair_keys = jnp.concatenate(
            [
                jnp.where(strict, products[0:rows, rows:], 0.0),
                jnp.where(strict, products[rows : 2 * rows, rows:], 0.0),
            ],
            axis=1,
        ).astype(BF16)
        read_keys = jnp.concatenate(
            [
                jnp.where(inclusive, products[2 * rows : 3 * rows, rows:], 0.0),
                jnp.where(inclusive, products[3 * rows :, rows:], 0.0),
            ],
            axis=1,
        ).astype(BF16)
        read_removal = jnp.concatenate(
            [
                jnp.where(inclusive, products[2 * rows : 3 * rows, 0:rows], 0.0),
                jnp.where(inclusive, products[3 * rows :, 0:rows], 0.0),
            ],
            axis=1,
        ).astype(BF16)
        va = values[:, lanes]
        stacked = jnp.concatenate([left(va), right(va)], axis=0)
        sums = dot(jnp.concatenate([pair_keys, read_keys], axis=0), stacked)
        kept.append((read_removal, sums))

    inverses = unit_lower_inverses(strict_parts)

    for p in range(pairs):
        lanes = slice(p * PAIR, (p + 1) * PAIR)
        read_removal, sums = kept[p]
        weights = sums[:rows].astype(BF16)
        carry = carried_in[:, lanes]
        sides = jnp.concatenate(
            [
                jnp.concatenate([left(carry), left(weights)], axis=1),
                jnp.concatenate([right(carry), right(weights)], axis=1),
            ],
            axis=0,
        )
        inverse = jnp.concatenate([inverses[2 * p], inverses[2 * p + 1]], axis=1)
        solved = dot(inverse.astype(BF16), sides).astype(BF16)
        carried, local = solved[:, :PAIR], solved[:, PAIR:]
        halves = jnp.concatenate(
            [
                jnp.concatenate([left(carried), left(local)], axis=1),
                jnp.concatenate([right(carried), right(local)], axis=1),
            ],
            axis=0,
        )
        taken = dot(read_removal, halves)
        reader_ref[:, lanes] = (read_in[:, lanes] - taken[:, :PAIR]).astype(BF16)
        local_ref[:, lanes] = sums[rows:] - taken[:, PAIR:]
        ends = dot_tn(solved, tail_removal[:, lanes])
        gathered = jnp.where(same, ends[:PAIR], 0.0).astype(BF16)
        added = jnp.where(
            same, dot_tn(values[:, lanes], tail_keys[:, lanes]) - ends[PAIR:], 0.0
        )
        gather_ref[0, p] = gathered
        add_ref[0, p] = added
        maps = maps_ref[p]
        maps = maps * fade[:, lanes] - dot(maps.astype(BF16), gathered)
        maps_ref[p, :PAIR, :] = maps[:PAIR]
        maps_ref[p, PAIR:, :] = maps[PAIR:] + added
    total_ref[...] = total_ref[...] * fade

    @pl.when(step == pl.num_programs(0) - 1)
    def _():
        low = iota((PAIR, PAIR), 1) < HEAD
        low_row = iota((1, PAIR), 1) < HEAD
        for p in range(pairs):
            lanes = slice(p * PAIR, (p + 1) * PAIR)
            total = total_ref[:, lanes]
            lost = eye * total - maps_ref[p, :PAIR, :]
            gained = maps_ref[p, PAIR:, :]
            lost = lost + pltpu.roll(lost, HEAD, 1)
            gained = gained + pltpu.roll(gained, HEAD, 1)
            both = jnp.where(low, lost, gained).astype(BF16)
            msg_ref[2 * p, :HEAD, :] = both[:HEAD]
            msg_ref[2 * p + 1, :HEAD, :] = both[HEAD:]
            for side in range(2):
                own = jnp.where(low_row == (side == 0), total, 0.0)
                own = jnp.broadcast_to(own, (16, PAIR))
                own = own + pltpu.roll(own, HEAD, 1)
                high, rest = two_parts(own)
                msg_ref[2 * p + side, HEAD:, :] = jnp.where(
                    iota((16, PAIR), 1) < HEAD, high.astype(F32), rest.astype(F32)
                ).astype(BF16)
        for s in range(GROUPS):
            sent_refs[s][...] = msg_ref[lax.rem(here_ref[0] + s, GROUPS)]


def message_parts(message):
    lost = message[:HEAD, :HEAD]
    gained = message[:HEAD, HEAD:].astype(F32)
    fades = message[HEAD : HEAD + 1, :].astype(F32)
    return lost, gained, fades[:, :HEAD] + fades[:, HEAD:]


def group_kernel(here_ref, *refs):
    in_refs, (prefix_ref, out_ref, met_ref) = refs[:GROUPS], refs[GROUPS:]
    for s in range(GROUPS):
        met_ref[lax.rem(here_ref[0] + GROUPS - s, GROUPS)] = in_refs[s][...]
    rows, cols = iota((HEAD, HEAD), 0), iota((HEAD, HEAD), 1)
    eye = (rows == cols).astype(F32)
    maps = jnp.concatenate([eye, jnp.zeros((HEAD, HEAD), F32)], axis=0)
    total = jnp.ones((1, HEAD), F32)
    for m in range(GROUPS):
        lost, gained, fade = message_parts(met_ref[m])
        prefix_ref[m] = maps
        moved = maps * fade - dot(maps.astype(BF16), lost)
        maps = jnp.concatenate([moved[:HEAD], moved[HEAD:] + gained], axis=0)
        total = total * fade
    both = jnp.concatenate([eye * total - maps[:HEAD], maps[HEAD:]], axis=1).astype(BF16)
    high, rest = two_parts(jnp.broadcast_to(total, (16, HEAD)))
    ends = jnp.concatenate([high.astype(F32), rest.astype(F32)], axis=1).astype(BF16)
    for z in range(out_ref.shape[0]):
        out_ref[z, :HEAD, :] = both
        out_ref[z, HEAD:, :] = ends


def enter_kernel(here_ref, in_ref, prefix_ref, out_ref):
    state = jnp.zeros((HEAD, HEAD), F32)
    for z in range(in_ref.shape[0]):
        lost, gained, fade = message_parts(in_ref[z])
        passed = state * fade - dot(state.astype(BF16), lost) + gained
        state = jnp.where(z < here_ref[0], passed, state)
    narrow = state.astype(BF16)
    for m in range(out_ref.shape[0]):
        entering = dot(narrow, prefix_ref[m, :HEAD, :].astype(BF16)) + prefix_ref[m, HEAD:, :]
        out_ref[m] = jnp.concatenate([entering, entering], axis=1).astype(BF16)


def readout_kernel(
    here_ref, enter_ref, reader_ref, local_ref, gather_ref, add_ref, fade_ref, gain_ref,
    weight_ref, *refs,
):
    out_refs, state_ref = refs[:-1], refs[-1]
    step = pl.program_id(0)
    spans = len(out_refs)
    channels = reader_ref.shape[1]
    pairs = channels // PAIR
    same = block_ones()
    means = jnp.where(same, 1.0 / HEAD, 0.0).astype(BF16)

    @pl.when(step == 0)
    def _():
        for p in range(pairs):
            entering = jnp.concatenate([enter_ref[2 * p], enter_ref[2 * p + 1]], axis=0)
            state_ref[p] = jnp.where(same, entering.astype(F32), 0.0)

    pieces = []
    for p in range(pairs):
        lanes = slice(p * PAIR, (p + 1) * PAIR)
        state = state_ref[p]
        narrow = state.astype(BF16)
        read = dot_nt(reader_ref[:, lanes], narrow) + local_ref[:, lanes]
        state_ref[p] = state * fade_ref[0, :, lanes] - dot(narrow, gather_ref[0, p]) + add_ref[0, p]
        centred = read - dot(read.astype(BF16), means)
        spread = dot((centred * centred).astype(BF16), means)
        pieces.append(
            (centred * lax.rsqrt(spread + GROUP_EPS) * gain_ref[:, lanes]).astype(BF16)
        )
    normed = jnp.concatenate(pieces, axis=1)
    result = dot(normed, weight_ref[...]).astype(BF16)
    for s in range(spans):

        @pl.when(lax.rem(step + spans - here_ref[0], spans) == s)
        def _():
            out_refs[s][...] = result


def hidden_kernel(x_hbm, *refs):
    weights, (out_ref, x_ref, weight_refs, sems) = refs[:8], refs[8:]
    fetch_x = pltpu.make_async_copy(x_hbm, x_ref, sems.at[8])
    fetch_x.start()
    fetches = [
        pltpu.make_async_copy(w, weight_refs.at[n], sems.at[n]) for n, w in enumerate(weights)
    ]
    for fetch in fetches:
        fetch.start()
    fetch_x.wait()
    units = weight_refs.shape[2]
    for q in range(4):
        fetches[2 * q].wait()
        fetches[2 * q + 1].wait()
        gates = dot(x_ref[...], weight_refs[2 * q])
        uppers = dot(x_ref[...], weight_refs[2 * q + 1])
        out_ref[:, q * units : (q + 1) * units] = (
            gates / (1.0 + jnp.exp(-gates)) * uppers
        ).astype(BF16)


def down_early_kernel(hidden_ref, own, before_0, before_1, after_0, after_1, out_ref):
    count = 3 * own.shape[0]
    halves = pl.num_programs(0) // 2
    for half, before, after in ((0, before_0, after_0), (1, before_1, after_1)):

        @pl.when(pl.program_id(0) // halves == half)
        def _():
            weights = jnp.concatenate([own[...], before[...], after[...]], axis=0)
            out_ref[...] = dot(hidden_ref[:, :count], weights).astype(BF16)


def down_late_kernel(early_ref, hidden_ref, far_0, far_1, out_ref):
    tile = out_ref.shape[1]
    for part in range(4):
        far = (far_0, far_1)[part // 2]

        @pl.when(pl.program_id(0) == part)
        def _():
            low = (part % 2) * tile
            out_ref[...] = (
                early_ref[...].astype(F32) + dot(hidden_ref[...], far[:, low : low + tile])
            ).astype(BF16)


def pack_kernel(x_ref, gain_ref, routes_ref, mix_ref, out_ref, mix_out_ref):
    tokens = x_ref.shape[0]
    places = out_ref.shape[0]
    x = x_ref[...].astype(F32)
    normed = (
        x * lax.rsqrt(jnp.mean(x * x, axis=1, keepdims=True) + NORM_EPS) * gain_ref[...]
    ).astype(BF16)
    experts = places // CAPACITY
    listed = iota((experts, tokens), 0)
    first, second = routes_ref[0:1, :], routes_ref[1:2, :]
    first_mark = (first == listed).astype(F32)
    second_mark = (second == listed).astype(F32)
    before = (iota((tokens, tokens), 0) < iota((tokens, tokens), 1)).astype(F32).astype(BF16)
    earlier = dot((first_mark + second_mark).astype(BF16), before)
    rows = iota((places, tokens), 0)
    table = jnp.zeros((places, tokens), F32)
    mix = jnp.zeros((places, tokens), F32)
    for named, mark, weight in (
        (first, first_mark, mix_ref[0:1, :]),
        (second, second_mark, mix_ref[1:2, :]),
    ):
        slot = jnp.sum(earlier * mark, axis=0, keepdims=True).astype(jnp.int32)
        here = rows == named * CAPACITY + slot
        table = table + here.astype(F32)
        mix = jnp.where(here, weight, mix)
    out_ref[...] = dot(table.astype(BF16), normed).astype(BF16)
    high, rest = two_parts(jnp.transpose(mix))
    mix_out_ref[:tokens, :] = high
    mix_out_ref[tokens:, :] = rest


def combine_kernel(mix_ref, rows_ref, out_ref):
    tokens = out_ref.shape[0]
    both = dot(mix_ref[...], rows_ref[...])
    out_ref[...] = (both[:tokens] + both[tokens:]).astype(BF16)


def whole(shape):
    return pl.BlockSpec(shape, lambda *_: (0,) * len(shape))


def estimate(flops, moved, transcendentals=0):
    return pl.CostEstimate(
        flops=int(flops), bytes_accessed=int(moved), transcendentals=int(transcendentals)
    )


SCALARS = pl.BlockSpec(memory_space=pltpu.SMEM)


def summarize(here, q, k, v, di, li, base, shift):
    rows, channels = q.shape
    heads = shift.shape[0]
    pairs = heads // 2
    spans = rows // SPAN
    block = pl.BlockSpec((SPAN, channels), lambda i: (i, 0))
    square = (1, pairs, PAIR, PAIR)
    return pl.pallas_call(
        summary_kernel,
        grid=(spans,),
        in_specs=[SCALARS]
        + [block] * 5
        + [whole((1, channels)), pl.BlockSpec((heads, SPAN), lambda i: (0, i))],
        out_specs=[
            block,
            block,
            pl.BlockSpec(square, lambda i: (i, 0, 0, 0)),
            pl.BlockSpec(square, lambda i: (i, 0, 0, 0)),
            pl.BlockSpec((1, 1, channels), lambda i: (i, 0, 0)),
        ]
        + [whole((MSG_ROWS, PAIR))] * GROUPS,
        out_shape=[
            jax.ShapeDtypeStruct((rows, channels), BF16),
            jax.ShapeDtypeStruct((rows, channels), F32),
            jax.ShapeDtypeStruct((spans, pairs, PAIR, PAIR), BF16),
            jax.ShapeDtypeStruct((spans, pairs, PAIR, PAIR), F32),
            jax.ShapeDtypeStruct((spans, 1, channels), F32),
        ]
        + [jax.ShapeDtypeStruct((MSG_ROWS, PAIR), BF16)] * GROUPS,
        scratch_shapes=[
            pltpu.VMEM((pairs, 2 * PAIR, PAIR), F32),
            pltpu.VMEM((1, channels), F32),
            pltpu.VMEM((heads, MSG_ROWS, PAIR), BF16),
        ],
        compiler_params=pltpu.CompilerParams(dimension_semantics=("arbitrary",)),
        cost_estimate=estimate(2.0e10, 6 << 20, 2 << 20),
        name="summary",
    )(here, q, k, v, di, li, base, shift)


def group_scan(here, messages, copies):
    return pl.pallas_call(
        group_kernel,
        in_specs=[SCALARS] + [pl.BlockSpec(memory_space=pltpu.VMEM)] * GROUPS,
        out_shape=[
            jax.ShapeDtypeStruct((GROUPS, 2 * HEAD, HEAD), F32),
            jax.ShapeDtypeStruct((copies, MSG_ROWS, PAIR), BF16),
        ],
        scratch_shapes=[pltpu.VMEM((GROUPS, MSG_ROWS, PAIR), BF16)],
        cost_estimate=estimate(2.0e9, 1 << 20),
        name="group_scan",
    )(here, *map(in_vmem, messages))


def enter_states(here, totals, prefixes):
    return pl.pallas_call(
        enter_kernel,
        in_specs=[SCALARS] + [pl.BlockSpec(memory_space=pltpu.VMEM)] * 2,
        out_shape=jax.ShapeDtypeStruct((prefixes.shape[0], HEAD, PAIR), BF16),
        cost_estimate=estimate(2.0e9, 1 << 20),
        name="enter_states",
    )(here, in_vmem(totals), prefixes)


def read_and_project(here, entering, reader, local, gather, add, fade, gain, weight):
    rows, channels = reader.shape
    pairs = channels // PAIR
    spans = rows // SPAN
    width = weight.shape[1]
    block = pl.BlockSpec((SPAN, channels), lambda i: (i, 0))
    square = pl.BlockSpec((1, pairs, PAIR, PAIR), lambda i: (i, 0, 0, 0))
    return pl.pallas_call(
        readout_kernel,
        grid=(spans,),
        in_specs=[
            SCALARS,
            IN_VMEM,
            block,
            block,
            square,
            square,
            pl.BlockSpec((1, 1, channels), lambda i: (i, 0, 0)),
            whole((1, channels)),
            whole(weight.shape),
        ],
        out_specs=[whole((SPAN, width))] * spans,
        out_shape=[jax.ShapeDtypeStruct((SPAN, width), BF16)] * spans,
        scratch_shapes=[pltpu.VMEM((pairs, PAIR, PAIR), F32)],
        compiler_params=pltpu.CompilerParams(dimension_semantics=("arbitrary",)),
        cost_estimate=estimate(5.0e9, 8 << 20),
        name="readout",
    )(here, in_vmem(entering), reader, local, gather, add, fade, gain, weight)


IN_HBM = pl.BlockSpec(memory_space=pltpu.HBM)
IN_VMEM = pl.BlockSpec(memory_space=pltpu.VMEM)


def expert_hidden(x, weights):
    rows, width = x.shape
    units = weights[0].shape[1]
    count = len(weights)
    return pl.pallas_call(
        hidden_kernel,
        in_specs=[IN_HBM] * (1 + count),
        out_specs=IN_VMEM,
        out_shape=jax.ShapeDtypeStruct((rows, units * count // 2), BF16),
        scratch_shapes=[
            pltpu.VMEM((rows, width), BF16),
            pltpu.VMEM((count, width, units), BF16),
            pltpu.SemaphoreType.DMA((count + 1,)),
        ],
        cost_estimate=estimate(2 * rows * width * units * count, 11 << 20, rows * units * 4),
        name="hidden",
    )(pltpu.with_memory_space_constraint(x, pltpu.HBM), *weights)


def first_half(units, tile):
    return pl.BlockSpec((units, tile), lambda i: (0, jnp.minimum(i, 1)))


def last_half(units, tile):
    return pl.BlockSpec((units, tile), lambda i: (0, jnp.maximum(i - 2, 0)))


def expert_down_early(hidden, own, before, after):
    rows = hidden.shape[0]
    units, width = own.shape
    tile = width // 4
    halves = [first_half(units, tile), last_half(units, tile)]
    return pl.pallas_call(
        down_early_kernel,
        grid=(4,),
        in_specs=[whole(hidden.shape), pl.BlockSpec((units, tile), lambda i: (0, i))]
        + 2 * halves,
        out_specs=pl.BlockSpec((rows, tile), lambda i: (0, i)),
        out_shape=jax.ShapeDtypeStruct((rows, width), BF16),
        cost_estimate=estimate(6 * rows * units * width, 6 << 20),
        name="down_early",
    )(hidden, own, *before, *after)


def expert_down_late(early, hidden, far):
    rows, width = early.shape
    units = far[0].shape[0]
    tile = width // 4
    column = pl.BlockSpec((rows, tile), lambda i: (0, i))
    return pl.pallas_call(
        down_late_kernel,
        grid=(4,),
        in_specs=[
            column,
            pl.BlockSpec((rows, units), lambda i: (0, 3)),
            IN_VMEM,
            IN_VMEM,
        ],
        out_specs=column,
        out_shape=jax.ShapeDtypeStruct((rows, width), BF16),
        cost_estimate=estimate(2 * rows * units * width, 5 << 20),
        name="down_late",
    )(early, hidden, *map(in_vmem, far))


def pack_rows(x, gain, routes, mix, places):
    tokens, width = x.shape
    return pl.pallas_call(
        pack_kernel,
        out_shape=[
            jax.ShapeDtypeStruct((places, width), BF16),
            jax.ShapeDtypeStruct((2 * tokens, places), BF16),
        ],
        cost_estimate=estimate(2.0e9, 3 << 20),
        name="pack",
    )(x, gain, routes, mix)


def combine_rows(mix, rows):
    tokens = mix.shape[0] // 2
    return pl.pallas_call(
        combine_kernel,
        in_specs=[IN_VMEM, IN_VMEM],
        out_specs=IN_VMEM,
        out_shape=jax.ShapeDtypeStruct((tokens, rows.shape[1]), BF16),
        cost_estimate=estimate(1.0e9, 3 << 20),
        name="combine",
    )(mix, in_vmem(rows))


def ring(x, shift, axis="tp"):
    count = lax.axis_size(axis)
    return lax.ppermute(x, axis, [(i, (i + shift) % count) for i in range(count)])


def around(parts, axis):
    return [parts[0]] + [ring(part, n, axis) for n, part in enumerate(parts) if n]


def in_vmem(x):
    return pltpu.with_memory_space_constraint(x, pltpu.VMEM)


def exchange(x, axis):
    return lax.all_to_all(x, axis, 0, 0, tiled=True)


def on_device(
    receptance,
    key_rows,
    value_rows,
    decay_input,
    learn_input,
    decay_base,
    decay_shift,
    channel_gain,
    out_weight,
    expert_input,
    expert_gain,
    routes,
    route_weight,
    gate_weight,
    up_weight,
    down_weight,
):
    ep_count = lax.axis_size(EP)
    _, model_width = expert_input.shape
    experts = gate_weight.shape[0] * ep_count
    places = experts * CAPACITY

    w_gate = gate_weight[0]
    w_up = up_weight[0]
    w_down = down_weight[0]
    cut = model_width // 2
    down_0, down_1 = w_down[:, :cut], w_down[:, cut:]
    gate_r, up_l = ring(w_gate, 1), ring(w_up, -1)
    up_r, gate_l = ring(w_up, 1), ring(w_gate, -1)
    gate_f, up_f = ring(gate_r, 1), ring(up_l, -1)
    down_0r, down_1l = ring(down_0, 1), ring(down_1, -1)
    down_1r, down_0l = ring(down_1, 1), ring(down_0, -1)
    down_0f, down_1f = ring(down_0r, 1), ring(down_1l, -1)

    outgoing, mix = pack_rows(
        expert_input, expert_gain.reshape(1, -1), routes.T, route_weight.T, places
    )
    arrived = exchange(
        outgoing.reshape(experts, CAPACITY, model_width), EP
    ).reshape(places, model_width)

    def here(axis):
        return lax.axis_index(axis).astype(jnp.int32).reshape(1)

    reader, local, gather, add, fade, *messages = summarize(
        here(GROUP),
        receptance,
        key_rows,
        value_rows,
        decay_input,
        learn_input,
        decay_base.reshape(1, -1),
        decay_shift.T,
    )
    prefixes, totals = group_scan(
        here(GROUP), around(messages, GROUP), lax.axis_size("ep_0")
    )
    entered = enter_states(here("ep_0"), exchange(totals, "ep_0"), prefixes)
    partial = read_and_project(
        here("tp"),
        exchange(entered, GROUP),
        reader,
        local,
        gather,
        add,
        fade,
        channel_gain.reshape(1, -1),
        out_weight,
    )
    shares = around(partial, "tp")
    mixer_out = sum(share.astype(F32) for share in shares).astype(BF16)

    hiddens = expert_hidden(
        arrived, [w_gate, w_up, gate_r, up_r, gate_l, up_l, gate_f, up_f]
    )
    early = expert_down_early(hiddens, w_down, (down_0r, down_1r), (down_0l, down_1l))
    returning = expert_down_late(early, hiddens, (down_0f, down_1f))
    returned = exchange(returning.reshape(ep_count, CAPACITY, model_width), EP)
    return (mixer_out, combine_rows(mix, returned.reshape(places, model_width)))


def solution(mesh):
    finer = Mesh(mesh.devices.reshape(8, 4, 2, mesh.shape["tp"]), ("ep_0", "ep_1", "ep_2", "tp"))
    placed = (
        P(EP, "tp"),
        P(EP, "tp"),
        P(EP, "tp"),
        P(EP, "tp"),
        P(EP, "tp"),
        P("tp"),
        P(EP, "tp"),
        P("tp"),
        P("tp", None),
        P(EP_TP, None),
        P(),
        P(EP_TP, None),
        P(EP_TP, None),
        P(EP, None, "tp"),
        P(EP, None, "tp"),
        P(EP, "tp", None),
    )

    return jax.shard_map(
        on_device,
        mesh=finer,
        in_specs=placed,
        out_specs=(P(EP_TP, None), P(EP_TP, None)),
        check_vma=False,
    )
```

```python
import jax
import jax.numpy as jnp
from jax import lax
from jax.experimental import pallas as pl
from jax.experimental.pallas import tpu as pltpu
from jax.sharding import Mesh
from jax.sharding import PartitionSpec as P


SPAN = 128
EP = ("ep_0", "ep_1", "ep_2")
GROUP = ("ep_1", "ep_2")
EP_TP = ("ep_0", "ep_1", "ep_2", "tp")
GROUPS = 8
HEAD = 64
PAIR = 128
MSG_ROWS = 80
CAPACITY = 8

NORM_EPS = 1e-06
GROUP_EPS = 0.00064
KEY_EPS = 1e-06
DECAY_SCALE = 0.6065306597126334

F32 = jnp.float32
BF16 = jnp.bfloat16


def dot(a, b):
    return lax.dot_general(a, b, (((1,), (0,)), ((), ())), preferred_element_type=F32)


def dot_nt(a, b):
    return lax.dot_general(a, b, (((1,), (1,)), ((), ())), preferred_element_type=F32)


def dot_tn(a, b):
    return lax.dot_general(a, b, (((0,), (0,)), ((), ())), preferred_element_type=F32)


def two_parts(x):
    high = x.astype(BF16)
    return high, (x - high.astype(F32)).astype(BF16)


def iota(shape, dim):
    return lax.broadcasted_iota(jnp.int32, shape, dim)


def block_ones():
    rows, cols = iota((PAIR, PAIR), 0), iota((PAIR, PAIR), 1)
    return (rows // HEAD) == (cols // HEAD)


def unit_lower_inverses(parts):
    size = parts[0].shape[0]
    rows, cols = iota((size, size), 0), iota((size, size), 1)
    eye = (rows == cols).astype(F32)
    start = 16
    inside = (rows // start) == (cols // start)
    powers = [jnp.where(inside, -a, 0.0) for a in parts]
    inverses = [eye + p for p in powers]
    reach = 2
    while reach < start:
        narrow = [p.astype(BF16) for p in powers]
        powers = [dot(p, p) for p in narrow]
        inverses = [
            inv + dot(inv.astype(BF16), p.astype(BF16))
            for inv, p in zip(inverses, powers)
        ]
        reach *= 2
    block = start
    while block < size:
        joined = ((rows // (2 * block)) == (cols // (2 * block))) & (
            (rows // block) != (cols // block)
        )
        narrow = [inv.astype(BF16) for inv in inverses]
        corners = [jnp.where(joined, a, 0.0).astype(BF16) for a in parts]
        moved = [dot(c, inv).astype(BF16) for c, inv in zip(corners, narrow)]
        inverses = [
            inv - dot(short, m) for inv, short, m in zip(inverses, narrow, moved)
        ]
        block *= 2
    return inverses


def summary_kernel(
    here_ref, q_ref, k_ref, v_ref, di_ref, li_ref, base_ref, shift_ref,
    reader_ref, local_ref, gather_ref, add_ref, fade_ref, *rest_refs,
):
    sent_refs, (maps_ref, total_ref, msg_ref) = rest_refs[:GROUPS], rest_refs[GROUPS:]
    step = pl.program_id(0)
    rows, channels = q_ref.shape
    heads = shift_ref.shape[0]
    pairs = heads // 2
    same = block_ones()
    same_f = same.astype(F32)
    same_b = same_f.astype(BF16)
    row2, col2 = iota((PAIR, PAIR), 0), iota((PAIR, PAIR), 1)
    eye = (row2 == col2).astype(F32)

    @pl.when(step == 0)
    def _():
        for p in range(pairs):
            maps_ref[p, :PAIR, :] = eye
            maps_ref[p, PAIR:, :] = jnp.zeros((PAIR, PAIR), F32)
        total_ref[...] = jnp.ones_like(total_ref)

    spread = (
        (iota((heads, channels), 1) // HEAD) == iota((heads, channels), 0)
    ).astype(F32).astype(BF16)
    shift_high, shift_low = two_parts(shift_ref[...])
    pre = (
        di_ref[...].astype(F32)
        + base_ref[...]
        + (dot_tn(shift_high, spread) + dot_tn(shift_low, spread))
    )
    log_decay = -DECAY_SCALE / (1.0 + jnp.exp(-pre))
    tri_rows, tri_cols = iota((rows, rows), 0), iota((rows, rows), 1)
    inclusive = tri_rows >= tri_cols
    strict = tri_rows > tri_cols
    tri = inclusive.astype(F32).astype(BF16)
    decay_high, decay_low = two_parts(log_decay)
    cum = dot(tri, decay_high) + dot(tri, decay_low)
    middle = cum[rows // 2 - 1 : rows // 2, :]
    ending = cum[rows - 1 : rows, :]
    grow = jnp.exp(cum - middle)
    grow_before = grow * jnp.exp(-log_decay)
    shrink = jnp.exp(middle - cum)
    from_start = jnp.exp(middle)
    to_end = jnp.exp(ending - middle)
    fade = jnp.exp(ending)
    fade_ref[0] = fade

    keys = k_ref[...].astype(F32)
    recept = q_ref[...].astype(F32)
    squares_high, squares_low = two_parts(keys * keys)
    lengths = jnp.concatenate(
        [
            dot(squares_high[:, p * PAIR : (p + 1) * PAIR], same_b)
            + dot(squares_low[:, p * PAIR : (p + 1) * PAIR], same_b)
            for p in range(pairs)
        ],
        axis=1,
    )
    unit = keys * lax.rsqrt(lengths + KEY_EPS)
    removal = unit / (1.0 + jnp.exp(-li_ref[...].astype(F32)))

    probes_f = unit * grow_before
    queries_f = recept * grow
    back_removal_f = removal * shrink
    back_keys_f = keys * shrink
    probes = probes_f.astype(BF16)
    queries = queries_f.astype(BF16)
    back_removal = back_removal_f.astype(BF16)
    back_keys = back_keys_f.astype(BF16)
    carried_in = (probes_f * from_start).astype(BF16)
    read_in = queries_f * from_start
    tail_removal = (back_removal_f * to_end).astype(BF16)
    tail_keys = (back_keys_f * to_end).astype(BF16)
    values = v_ref[...]

    first = iota((rows, PAIR), 1) < HEAD
    none = jnp.zeros((rows, PAIR), BF16)

    def left(x):
        return jnp.where(first, x, none)

    def right(x):
        return jnp.where(first, none, x)

    kept = []
    strict_parts = []
    for p in range(pairs):
        lanes = slice(p * PAIR, (p + 1) * PAIR)
        pr, qu = probes[:, lanes], queries[:, lanes]
        outer = jnp.concatenate([left(pr), right(pr), left(qu), right(qu)], axis=0)
        inner = jnp.concatenate([back_removal[:, lanes], back_keys[:, lanes]], axis=0)
        products = dot_nt(outer, inner)
        strict_parts.append(jnp.where(strict, products[0:rows, 0:rows], 0.0))
        strict_parts.append(jnp.where(strict, products[rows : 2 * rows, 0:rows], 0.0))
        pair_keys = jnp.concatenate(
            [
                jnp.where(strict, products[0:rows, rows:], 0.0),
                jnp.where(strict, products[rows : 2 * rows, rows:], 0.0),
            ],
            axis=1,
        ).astype(BF16)
        read_keys = jnp.concatenate(
            [
                jnp.where(inclusive, products[2 * rows : 3 * rows, rows:], 0.0),
                jnp.where(inclusive, products[3 * rows :, rows:], 0.0),
            ],
            axis=1,
        ).astype(BF16)
        read_removal = jnp.concatenate(
            [
                jnp.where(inclusive, products[2 * rows : 3 * rows, 0:rows], 0.0),
                jnp.where(inclusive, products[3 * rows :, 0:rows], 0.0),
            ],
            axis=1,
        ).astype(BF16)
        va = values[:, lanes]
        stacked = jnp.concatenate([left(va), right(va)], axis=0)
        sums = dot(jnp.concatenate([pair_keys, read_keys], axis=0), stacked)
        kept.append((read_removal, sums))

    inverses = unit_lower_inverses(strict_parts)

    for p in range(pairs):
        lanes = slice(p * PAIR, (p + 1) * PAIR)
        read_removal, sums = kept[p]
        weights = sums[:rows].astype(BF16)
        carry = carried_in[:, lanes]
        sides = jnp.concatenate(
            [
                jnp.concatenate([left(carry), left(weights)], axis=1),
                jnp.concatenate([right(carry), right(weights)], axis=1),
            ],
            axis=0,
        )
        inverse = jnp.concatenate([inverses[2 * p], inverses[2 * p + 1]], axis=1)
        solved = dot(inverse.astype(BF16), sides).astype(BF16)
        carried, local = solved[:, :PAIR], solved[:, PAIR:]
        halves = jnp.concatenate(
            [
                jnp.concatenate([left(carried), left(local)], axis=1),
                jnp.concatenate([right(carried), right(local)], axis=1),
            ],
            axis=0,
        )
        taken = dot(read_removal, halves)
        reader_ref[:, lanes] = (read_in[:, lanes] - taken[:, :PAIR]).astype(BF16)
        local_ref[:, lanes] = sums[rows:] - taken[:, PAIR:]
        ends = dot_tn(solved, tail_removal[:, lanes])
        gathered = jnp.where(same, ends[:PAIR], 0.0).astype(BF16)
        added = jnp.where(
            same, dot_tn(values[:, lanes], tail_keys[:, lanes]) - ends[PAIR:], 0.0
        )
        gather_ref[0, p] = gathered
        add_ref[0, p] = added
        maps = maps_ref[p]
        maps = maps * fade[:, lanes] - dot(maps.astype(BF16), gathered)
        maps_ref[p, :PAIR, :] = maps[:PAIR]
        maps_ref[p, PAIR:, :] = maps[PAIR:] + added
    total_ref[...] = total_ref[...] * fade

    @pl.when(step == pl.num_programs(0) - 1)
    def _():
        low = iota((PAIR, PAIR), 1) < HEAD
        low_row = iota((1, PAIR), 1) < HEAD
        for p in range(pairs):
            lanes = slice(p * PAIR, (p + 1) * PAIR)
            total = total_ref[:, lanes]
            lost = eye * total - maps_ref[p, :PAIR, :]
            gained = maps_ref[p, PAIR:, :]
            lost = lost + pltpu.roll(lost, HEAD, 1)
            gained = gained + pltpu.roll(gained, HEAD, 1)
            both = jnp.where(low, lost, gained).astype(BF16)
            msg_ref[2 * p, :HEAD, :] = both[:HEAD]
            msg_ref[2 * p + 1, :HEAD, :] = both[HEAD:]
            for side in range(2):
                own = jnp.where(low_row == (side == 0), total, 0.0)
                own = jnp.broadcast_to(own, (16, PAIR))
                own = own + pltpu.roll(own, HEAD, 1)
                high, rest = two_parts(own)
                msg_ref[2 * p + side, HEAD:, :] = jnp.where(
                    iota((16, PAIR), 1) < HEAD, high.astype(F32), rest.astype(F32)
                ).astype(BF16)
        for s in range(GROUPS):
            sent_refs[s][...] = msg_ref[lax.rem(here_ref[0] + s, GROUPS)]


def message_parts(message):
    lost = message[:HEAD, :HEAD]
    gained = message[:HEAD, HEAD:].astype(F32)
    fades = message[HEAD : HEAD + 1, :].astype(F32)
    return lost, gained, fades[:, :HEAD] + fades[:, HEAD:]


def group_kernel(here_ref, *refs):
    in_refs, (prefix_ref, out_ref, met_ref) = refs[:GROUPS], refs[GROUPS:]
    for s in range(GROUPS):
        met_ref[lax.rem(here_ref[0] + GROUPS - s, GROUPS)] = in_refs[s][...]
    rows, cols = iota((HEAD, HEAD), 0), iota((HEAD, HEAD), 1)
    eye = (rows == cols).astype(F32)
    maps = jnp.concatenate([eye, jnp.zeros((HEAD, HEAD), F32)], axis=0)
    total = jnp.ones((1, HEAD), F32)
    for m in range(GROUPS):
        lost, gained, fade = message_parts(met_ref[m])
        prefix_ref[m] = maps
        moved = maps * fade - dot(maps.astype(BF16), lost)
        maps = jnp.concatenate([moved[:HEAD], moved[HEAD:] + gained], axis=0)
        total = total * fade
    both = jnp.concatenate([eye * total - maps[:HEAD], maps[HEAD:]], axis=1).astype(BF16)
    high, rest = two_parts(jnp.broadcast_to(total, (16, HEAD)))
    ends = jnp.concatenate([high.astype(F32), rest.astype(F32)], axis=1).astype(BF16)
    for z in range(out_ref.shape[0]):
        out_ref[z, :HEAD, :] = both
        out_ref[z, HEAD:, :] = ends


def enter_kernel(here_ref, in_ref, prefix_ref, out_ref):
    state = jnp.zeros((HEAD, HEAD), F32)
    for z in range(in_ref.shape[0]):
        lost, gained, fade = message_parts(in_ref[z])
        passed = state * fade - dot(state.astype(BF16), lost) + gained
        state = jnp.where(z < here_ref[0], passed, state)
    narrow = state.astype(BF16)
    for m in range(out_ref.shape[0]):
        entering = dot(narrow, prefix_ref[m, :HEAD, :].astype(BF16)) + prefix_ref[m, HEAD:, :]
        out_ref[m] = jnp.concatenate([entering, entering], axis=1).astype(BF16)


def readout_kernel(
    here_ref, enter_ref, reader_ref, local_ref, gather_ref, add_ref, fade_ref, gain_ref,
    weight_ref, *refs,
):
    out_refs, state_ref = refs[:-1], refs[-1]
    step = pl.program_id(0)
    spans = len(out_refs)
    channels = reader_ref.shape[1]
    pairs = channels // PAIR
    same = block_ones()
    means = jnp.where(same, 1.0 / HEAD, 0.0).astype(BF16)

    @pl.when(step == 0)
    def _():
        for p in range(pairs):
            entering = jnp.concatenate([enter_ref[2 * p], enter_ref[2 * p + 1]], axis=0)
            state_ref[p] = jnp.where(same, entering.astype(F32), 0.0)

    pieces = []
    for p in range(pairs):
        lanes = slice(p * PAIR, (p + 1) * PAIR)
        state = state_ref[p]
        narrow = state.astype(BF16)
        read = dot_nt(reader_ref[:, lanes], narrow) + local_ref[:, lanes]
        state_ref[p] = state * fade_ref[0, :, lanes] - dot(narrow, gather_ref[0, p]) + add_ref[0, p]
        centred = read - dot(read.astype(BF16), means)
        spread = dot((centred * centred).astype(BF16), means)
        pieces.append(
            (centred * lax.rsqrt(spread + GROUP_EPS) * gain_ref[:, lanes]).astype(BF16)
        )
    normed = jnp.concatenate(pieces, axis=1)
    result = dot(normed, weight_ref[...]).astype(BF16)
    for s in range(spans):

        @pl.when(lax.rem(step + spans - here_ref[0], spans) == s)
        def _():
            out_refs[s][...] = result


def hidden_kernel(x_hbm, *refs):
    weights, (out_ref, x_ref, weight_refs, sems) = refs[:8], refs[8:]
    fetch_x = pltpu.make_async_copy(x_hbm, x_ref, sems.at[8])
    fetch_x.start()
    fetches = [
        pltpu.make_async_copy(w, weight_refs.at[n], sems.at[n]) for n, w in enumerate(weights)
    ]
    for fetch in fetches:
        fetch.start()
    fetch_x.wait()
    units = weight_refs.shape[2]
    for q in range(4):
        fetches[2 * q].wait()
        fetches[2 * q + 1].wait()
        gates = dot(x_ref[...], weight_refs[2 * q])
        uppers = dot(x_ref[...], weight_refs[2 * q + 1])
        out_ref[:, q * units : (q + 1) * units] = (
            gates / (1.0 + jnp.exp(-gates)) * uppers
        ).astype(BF16)


def down_early_kernel(
    hidden_ref, own, before_0, before_1, after_0, after_1, out_ref, weight_ref, sems
):
    units, width = own.shape
    half = width // 2
    places = (
        (own, 0, 0, width),
        (before_0, 1, 0, half),
        (after_0, 2, 0, half),
        (before_1, 1, half, half),
        (after_1, 2, half, half),
    )
    fetches = [
        pltpu.make_async_copy(
            w, weight_ref.at[row * units : (row + 1) * units, low : low + size], sems.at[n]
        )
        for n, (w, row, low, size) in enumerate(places)
    ]
    for fetch in fetches:
        fetch.start()
    for part, waits in ((0, fetches[:3]), (1, fetches[3:])):
        for fetch in waits:
            fetch.wait()
        lanes = slice(part * half, (part + 1) * half)
        out_ref[:, lanes] = dot(hidden_ref[:, : 3 * units], weight_ref[:, lanes]).astype(BF16)


def down_late_kernel(
    early_ref, hidden_hbm, far_0, far_1, out_hbm, hidden_ref, made_ref, hidden_sem, sems
):
    units = hidden_ref.shape[1]
    width = made_ref.shape[1]
    parts = 4
    tile = width // parts
    fetch = pltpu.make_async_copy(
        hidden_hbm.at[:, hidden_hbm.shape[1] - units :], hidden_ref, hidden_sem
    )
    fetch.start()
    fetch.wait()
    stores = []
    for part in range(parts):
        far = (far_0, far_1)[part // 2]
        low = (part % 2) * tile
        lanes = slice(part * tile, (part + 1) * tile)
        made_ref[:, lanes] = (
            early_ref[:, lanes].astype(F32) + dot(hidden_ref[...], far[:, low : low + tile])
        ).astype(BF16)
        store = pltpu.make_async_copy(made_ref.at[:, lanes], out_hbm.at[:, lanes], sems.at[part])
        store.start()
        stores.append(store)
    for store in stores:
        store.wait()


def pack_kernel(x_ref, gain_ref, routes_ref, mix_ref, out_ref, mix_out_ref):
    tokens = x_ref.shape[0]
    places = out_ref.shape[0]
    x = x_ref[...].astype(F32)
    normed = (
        x * lax.rsqrt(jnp.mean(x * x, axis=1, keepdims=True) + NORM_EPS) * gain_ref[...]
    ).astype(BF16)
    experts = places // CAPACITY
    listed = iota((experts, tokens), 0)
    first, second = routes_ref[0:1, :], routes_ref[1:2, :]
    first_mark = (first == listed).astype(F32)
    second_mark = (second == listed).astype(F32)
    before = (iota((tokens, tokens), 0) < iota((tokens, tokens), 1)).astype(F32).astype(BF16)
    earlier = dot((first_mark + second_mark).astype(BF16), before)
    rows = iota((places, tokens), 0)
    table = jnp.zeros((places, tokens), F32)
    mix = jnp.zeros((places, tokens), F32)
    for named, mark, weight in (
        (first, first_mark, mix_ref[0:1, :]),
        (second, second_mark, mix_ref[1:2, :]),
    ):
        slot = jnp.sum(earlier * mark, axis=0, keepdims=True).astype(jnp.int32)
        here = rows == named * CAPACITY + slot
        table = table + here.astype(F32)
        mix = jnp.where(here, weight, mix)
    out_ref[...] = dot(table.astype(BF16), normed).astype(BF16)
    high, rest = two_parts(jnp.transpose(mix))
    mix_out_ref[:tokens, :] = high
    mix_out_ref[tokens:, :] = rest


def combine_kernel(mix_ref, rows_ref, out_ref):
    tokens = out_ref.shape[0]
    both = dot(mix_ref[...], rows_ref[...])
    out_ref[...] = (both[:tokens] + both[tokens:]).astype(BF16)


def whole(shape):
    return pl.BlockSpec(shape, lambda *_: (0,) * len(shape))


def estimate(flops, moved, transcendentals=0):
    return pl.CostEstimate(
        flops=int(flops), bytes_accessed=int(moved), transcendentals=int(transcendentals)
    )


SCALARS = pl.BlockSpec(memory_space=pltpu.SMEM)


def summarize(here, q, k, v, di, li, base, shift):
    rows, channels = q.shape
    heads = shift.shape[0]
    pairs = heads // 2
    spans = rows // SPAN
    block = pl.BlockSpec((SPAN, channels), lambda i: (i, 0))
    square = (1, pairs, PAIR, PAIR)
    return pl.pallas_call(
        summary_kernel,
        grid=(spans,),
        in_specs=[SCALARS]
        + [block] * 5
        + [whole((1, channels)), pl.BlockSpec((heads, SPAN), lambda i: (0, i))],
        out_specs=[
            block,
            block,
            pl.BlockSpec(square, lambda i: (i, 0, 0, 0)),
            pl.BlockSpec(square, lambda i: (i, 0, 0, 0)),
            pl.BlockSpec((1, 1, channels), lambda i: (i, 0, 0)),
        ]
        + [whole((MSG_ROWS, PAIR))] * GROUPS,
        out_shape=[
            jax.ShapeDtypeStruct((rows, channels), BF16),
            jax.ShapeDtypeStruct((rows, channels), F32),
            jax.ShapeDtypeStruct((spans, pairs, PAIR, PAIR), BF16),
            jax.ShapeDtypeStruct((spans, pairs, PAIR, PAIR), F32),
            jax.ShapeDtypeStruct((spans, 1, channels), F32),
        ]
        + [jax.ShapeDtypeStruct((MSG_ROWS, PAIR), BF16)] * GROUPS,
        scratch_shapes=[
            pltpu.VMEM((pairs, 2 * PAIR, PAIR), F32),
            pltpu.VMEM((1, channels), F32),
            pltpu.VMEM((heads, MSG_ROWS, PAIR), BF16),
        ],
        compiler_params=pltpu.CompilerParams(dimension_semantics=("arbitrary",)),
        cost_estimate=estimate(2.0e10, 6 << 20, 2 << 20),
        name="summary",
    )(here, q, k, v, di, li, base, shift)


def group_scan(here, messages, copies):
    return pl.pallas_call(
        group_kernel,
        in_specs=[SCALARS] + [pl.BlockSpec(memory_space=pltpu.VMEM)] * GROUPS,
        out_shape=[
            jax.ShapeDtypeStruct((GROUPS, 2 * HEAD, HEAD), F32),
            jax.ShapeDtypeStruct((copies, MSG_ROWS, PAIR), BF16),
        ],
        scratch_shapes=[pltpu.VMEM((GROUPS, MSG_ROWS, PAIR), BF16)],
        cost_estimate=estimate(2.0e9, 1 << 20),
        name="group_scan",
    )(here, *map(in_vmem, messages))


def enter_states(here, totals, prefixes):
    return pl.pallas_call(
        enter_kernel,
        in_specs=[SCALARS] + [pl.BlockSpec(memory_space=pltpu.VMEM)] * 2,
        out_shape=jax.ShapeDtypeStruct((prefixes.shape[0], HEAD, PAIR), BF16),
        cost_estimate=estimate(2.0e9, 1 << 20),
        name="enter_states",
    )(here, in_vmem(totals), prefixes)


def read_and_project(here, entering, reader, local, gather, add, fade, gain, weight):
    rows, channels = reader.shape
    pairs = channels // PAIR
    spans = rows // SPAN
    width = weight.shape[1]
    block = pl.BlockSpec((SPAN, channels), lambda i: (i, 0))
    square = pl.BlockSpec((1, pairs, PAIR, PAIR), lambda i: (i, 0, 0, 0))
    return pl.pallas_call(
        readout_kernel,
        grid=(spans,),
        in_specs=[
            SCALARS,
            IN_VMEM,
            block,
            block,
            square,
            square,
            pl.BlockSpec((1, 1, channels), lambda i: (i, 0, 0)),
            whole((1, channels)),
            whole(weight.shape),
        ],
        out_specs=[whole((SPAN, width))] * spans,
        out_shape=[jax.ShapeDtypeStruct((SPAN, width), BF16)] * spans,
        scratch_shapes=[pltpu.VMEM((pairs, PAIR, PAIR), F32)],
        compiler_params=pltpu.CompilerParams(dimension_semantics=("arbitrary",)),
        cost_estimate=estimate(5.0e9, 8 << 20),
        name="readout",
    )(here, in_vmem(entering), reader, local, gather, add, fade, gain, weight)


IN_HBM = pl.BlockSpec(memory_space=pltpu.HBM)
IN_VMEM = pl.BlockSpec(memory_space=pltpu.VMEM)


def expert_hidden(x, weights):
    rows, width = x.shape
    units = weights[0].shape[1]
    count = len(weights)
    return pl.pallas_call(
        hidden_kernel,
        in_specs=[IN_HBM] * (1 + count),
        out_specs=IN_VMEM,
        out_shape=jax.ShapeDtypeStruct((rows, units * count // 2), BF16),
        scratch_shapes=[
            pltpu.VMEM((rows, width), BF16),
            pltpu.VMEM((count, width, units), BF16),
            pltpu.SemaphoreType.DMA((count + 1,)),
        ],
        cost_estimate=estimate(2 * rows * width * units * count, 11 << 20, rows * units * 4),
        name="hidden",
    )(pltpu.with_memory_space_constraint(x, pltpu.HBM), *weights)


def expert_down_early(hidden, own, before, after):
    rows = hidden.shape[0]
    units, width = own.shape
    return pl.pallas_call(
        down_early_kernel,
        in_specs=[IN_VMEM] + [IN_HBM] * 5,
        out_specs=IN_VMEM,
        out_shape=pltpu.VMEM((rows, width), BF16),
        scratch_shapes=[
            pltpu.VMEM((3 * units, width), BF16),
            pltpu.SemaphoreType.DMA((5,)),
        ],
        cost_estimate=estimate(6 * rows * units * width, 6 << 20),
        name="down_early",
    )(hidden, own, *before, *after)


def expert_down_late(early, hidden, far):
    rows, width = early.shape
    units = far[0].shape[0]
    return pl.pallas_call(
        down_late_kernel,
        in_specs=[IN_VMEM, IN_HBM, IN_VMEM, IN_VMEM],
        out_specs=IN_HBM,
        out_shape=jax.ShapeDtypeStruct((rows, width), BF16),
        scratch_shapes=[
            pltpu.VMEM((rows, units), BF16),
            pltpu.VMEM((rows, width), BF16),
            pltpu.SemaphoreType.DMA,
            pltpu.SemaphoreType.DMA((4,)),
        ],
        cost_estimate=estimate(2 * rows * units * width, 5 << 20),
        name="down_late",
    )(in_vmem(early), hidden, *map(in_vmem, far))


def pack_rows(x, gain, routes, mix, places):
    tokens, width = x.shape
    return pl.pallas_call(
        pack_kernel,
        out_shape=[
            jax.ShapeDtypeStruct((places, width), BF16),
            jax.ShapeDtypeStruct((2 * tokens, places), BF16),
        ],
        cost_estimate=estimate(2.0e9, 3 << 20),
        name="pack",
    )(x, gain, routes, mix)


def combine_rows(mix, rows):
    tokens = mix.shape[0] // 2
    return pl.pallas_call(
        combine_kernel,
        in_specs=[IN_VMEM, IN_VMEM],
        out_specs=IN_VMEM,
        out_shape=jax.ShapeDtypeStruct((tokens, rows.shape[1]), BF16),
        cost_estimate=estimate(1.0e9, 3 << 20),
        name="combine",
    )(mix, in_vmem(rows))


def ring(x, shift, axis="tp"):
    count = lax.axis_size(axis)
    return lax.ppermute(x, axis, [(i, (i + shift) % count) for i in range(count)])


def around(parts, axis):
    return [parts[0]] + [ring(part, n, axis) for n, part in enumerate(parts) if n]


def in_vmem(x):
    return pltpu.with_memory_space_constraint(x, pltpu.VMEM)


def exchange(x, axis):
    return lax.all_to_all(x, axis, 0, 0, tiled=True)


def on_device(
    receptance,
    key_rows,
    value_rows,
    decay_input,
    learn_input,
    decay_base,
    decay_shift,
    channel_gain,
    out_weight,
    expert_input,
    expert_gain,
    routes,
    route_weight,
    gate_weight,
    up_weight,
    down_weight,
):
    ep_count = lax.axis_size(EP)
    _, model_width = expert_input.shape
    experts = gate_weight.shape[0] * ep_count
    places = experts * CAPACITY

    w_gate = gate_weight[0]
    w_up = up_weight[0]
    w_down = down_weight[0]
    cut = model_width // 2
    down_0, down_1 = w_down[:, :cut], w_down[:, cut:]
    gate_r, up_l = ring(w_gate, 1), ring(w_up, -1)
    up_r, gate_l = ring(w_up, 1), ring(w_gate, -1)
    gate_f, up_f = ring(gate_r, 1), ring(up_l, -1)
    down_0r, down_1l = ring(down_0, 1), ring(down_1, -1)
    down_1r, down_0l = ring(down_1, 1), ring(down_0, -1)
    down_0f, down_1f = ring(down_0r, 1), ring(down_1l, -1)

    outgoing, mix = pack_rows(
        expert_input, expert_gain.reshape(1, -1), routes.T, route_weight.T, places
    )
    arrived = exchange(
        outgoing.reshape(experts, CAPACITY, model_width), EP
    ).reshape(places, model_width)

    def here(axis):
        return lax.axis_index(axis).astype(jnp.int32).reshape(1)

    reader, local, gather, add, fade, *messages = summarize(
        here(GROUP),
        receptance,
        key_rows,
        value_rows,
        decay_input,
        learn_input,
        decay_base.reshape(1, -1),
        decay_shift.T,
    )
    prefixes, totals = group_scan(
        here(GROUP), around(messages, GROUP), lax.axis_size("ep_0")
    )
    entered = enter_states(here("ep_0"), exchange(totals, "ep_0"), prefixes)
    partial = read_and_project(
        here("tp"),
        exchange(entered, GROUP),
        reader,
        local,
        gather,
        add,
        fade,
        channel_gain.reshape(1, -1),
        out_weight,
    )
    shares = around(partial, "tp")
    mixer_out = sum(share.astype(F32) for share in shares).astype(BF16)

    hiddens = expert_hidden(
        arrived, [w_gate, w_up, gate_r, up_r, gate_l, up_l, gate_f, up_f]
    )
    early = expert_down_early(hiddens, w_down, (down_0r, down_1r), (down_0l, down_1l))
    returning = expert_down_late(early, hiddens, (down_0f, down_1f))
    returned = exchange(returning.reshape(ep_count, CAPACITY, model_width), EP)
    return (mixer_out, combine_rows(mix, returned.reshape(places, model_width)))


def solution(mesh):
    finer = Mesh(mesh.devices.reshape(8, 4, 2, mesh.shape["tp"]), ("ep_0", "ep_1", "ep_2", "tp"))
    placed = (
        P(EP, "tp"),
        P(EP, "tp"),
        P(EP, "tp"),
        P(EP, "tp"),
        P(EP, "tp"),
        P("tp"),
        P(EP, "tp"),
        P("tp"),
        P("tp", None),
        P(EP_TP, None),
        P(),
        P(EP_TP, None),
        P(EP_TP, None),
        P(EP, None, "tp"),
        P(EP, None, "tp"),
        P(EP, "tp", None),
    )

    return jax.shard_map(
        on_device,
        mesh=finer,
        in_specs=placed,
        out_specs=(P(EP_TP, None), P(EP_TP, None)),
        check_vma=False,
    )
```

```python
import jax
import jax.numpy as jnp
from jax import lax
from jax.experimental import pallas as pl
from jax.experimental.pallas import tpu as pltpu
from jax.sharding import Mesh
from jax.sharding import PartitionSpec as P


SPAN = 128
EP = ("ep_0", "ep_1", "ep_2")
GROUP = ("ep_1", "ep_2")
EP_TP = ("ep_0", "ep_1", "ep_2", "tp")
GROUPS = 8
HEAD = 64
PAIR = 128
MSG_ROWS = 80
CAPACITY = 8

NORM_EPS = 1e-06
GROUP_EPS = 0.00064
KEY_EPS = 1e-06
DECAY_SCALE = 0.6065306597126334

F32 = jnp.float32
BF16 = jnp.bfloat16


def dot(a, b):
    return lax.dot_general(a, b, (((1,), (0,)), ((), ())), preferred_element_type=F32)


def dot_nt(a, b):
    return lax.dot_general(a, b, (((1,), (1,)), ((), ())), preferred_element_type=F32)


def dot_tn(a, b):
    return lax.dot_general(a, b, (((0,), (0,)), ((), ())), preferred_element_type=F32)


def two_parts(x):
    high = x.astype(BF16)
    return high, (x - high.astype(F32)).astype(BF16)


def iota(shape, dim):
    return lax.broadcasted_iota(jnp.int32, shape, dim)


def block_ones():
    rows, cols = iota((PAIR, PAIR), 0), iota((PAIR, PAIR), 1)
    return (rows // HEAD) == (cols // HEAD)


def unit_lower_inverses(parts):
    size = parts[0].shape[0]
    rows, cols = iota((size, size), 0), iota((size, size), 1)
    eye = (rows == cols).astype(F32)
    start = 16
    inside = (rows // start) == (cols // start)
    powers = [jnp.where(inside, -a, 0.0) for a in parts]
    inverses = [eye + p for p in powers]
    reach = 2
    while reach < start:
        narrow = [p.astype(BF16) for p in powers]
        powers = [dot(p, p) for p in narrow]
        inverses = [
            inv + dot(inv.astype(BF16), p.astype(BF16))
            for inv, p in zip(inverses, powers)
        ]
        reach *= 2
    block = start
    while block < size:
        joined = ((rows // (2 * block)) == (cols // (2 * block))) & (
            (rows // block) != (cols // block)
        )
        narrow = [inv.astype(BF16) for inv in inverses]
        corners = [jnp.where(joined, a, 0.0).astype(BF16) for a in parts]
        moved = [dot(c, inv).astype(BF16) for c, inv in zip(corners, narrow)]
        inverses = [
            inv - dot(short, m) for inv, short, m in zip(inverses, narrow, moved)
        ]
        block *= 2
    return inverses


def summary_kernel(
    here_ref, q_ref, k_ref, v_ref, di_ref, li_ref, base_ref, shift_ref,
    reader_ref, local_ref, gather_ref, add_ref, fade_ref, *rest_refs,
):
    sent_refs, (maps_ref, total_ref, msg_ref) = rest_refs[:GROUPS], rest_refs[GROUPS:]
    step = pl.program_id(0)
    rows, channels = q_ref.shape
    heads = shift_ref.shape[0]
    pairs = heads // 2
    same = block_ones()
    same_f = same.astype(F32)
    same_b = same_f.astype(BF16)
    row2, col2 = iota((PAIR, PAIR), 0), iota((PAIR, PAIR), 1)
    eye = (row2 == col2).astype(F32)

    @pl.when(step == 0)
    def _():
        for p in range(pairs):
            maps_ref[p, :PAIR, :] = eye
            maps_ref[p, PAIR:, :] = jnp.zeros((PAIR, PAIR), F32)
        total_ref[...] = jnp.ones_like(total_ref)

    spread = (
        (iota((heads, channels), 1) // HEAD) == iota((heads, channels), 0)
    ).astype(F32).astype(BF16)
    shift_high, shift_low = two_parts(shift_ref[...])
    pre = (
        di_ref[...].astype(F32)
        + base_ref[...]
        + (dot_tn(shift_high, spread) + dot_tn(shift_low, spread))
    )
    log_decay = -DECAY_SCALE / (1.0 + jnp.exp(-pre))
    tri_rows, tri_cols = iota((rows, rows), 0), iota((rows, rows), 1)
    inclusive = tri_rows >= tri_cols
    strict = tri_rows > tri_cols
    tri = inclusive.astype(F32).astype(BF16)
    decay_high, decay_low = two_parts(log_decay)
    cum = dot(tri, decay_high) + dot(tri, decay_low)
    middle = cum[rows // 2 - 1 : rows // 2, :]
    ending = cum[rows - 1 : rows, :]
    grow = jnp.exp(cum - middle)
    grow_before = grow * jnp.exp(-log_decay)
    shrink = jnp.exp(middle - cum)
    from_start = jnp.exp(middle)
    to_end = jnp.exp(ending - middle)
    fade = jnp.exp(ending)
    fade_ref[0] = fade

    keys = k_ref[...].astype(F32)
    recept = q_ref[...].astype(F32)
    squares_high, squares_low = two_parts(keys * keys)
    lengths = jnp.concatenate(
        [
            dot(squares_high[:, p * PAIR : (p + 1) * PAIR], same_b)
            + dot(squares_low[:, p * PAIR : (p + 1) * PAIR], same_b)
            for p in range(pairs)
        ],
        axis=1,
    )
    unit = keys * lax.rsqrt(lengths + KEY_EPS)
    removal = unit / (1.0 + jnp.exp(-li_ref[...].astype(F32)))

    probes_f = unit * grow_before
    queries_f = recept * grow
    back_removal_f = removal * shrink
    back_keys_f = keys * shrink
    probes = probes_f.astype(BF16)
    queries = queries_f.astype(BF16)
    back_removal = back_removal_f.astype(BF16)
    back_keys = back_keys_f.astype(BF16)
    carried_in = (probes_f * from_start).astype(BF16)
    read_in = queries_f * from_start
    tail_removal = (back_removal_f * to_end).astype(BF16)
    tail_keys = (back_keys_f * to_end).astype(BF16)
    values = v_ref[...]

    first = iota((rows, PAIR), 1) < HEAD
    none = jnp.zeros((rows, PAIR), BF16)

    def left(x):
        return jnp.where(first, x, none)

    def right(x):
        return jnp.where(first, none, x)

    kept = []
    strict_parts = []
    for p in range(pairs):
        lanes = slice(p * PAIR, (p + 1) * PAIR)
        pr, qu = probes[:, lanes], queries[:, lanes]
        outer = jnp.concatenate([left(pr), right(pr), left(qu), right(qu)], axis=0)
        inner = jnp.concatenate([back_removal[:, lanes], back_keys[:, lanes]], axis=0)
        products = dot_nt(outer, inner)
        strict_parts.append(jnp.where(strict, products[0:rows, 0:rows], 0.0))
        strict_parts.append(jnp.where(strict, products[rows : 2 * rows, 0:rows], 0.0))
        pair_keys = jnp.concatenate(
            [
                jnp.where(strict, products[0:rows, rows:], 0.0),
                jnp.where(strict, products[rows : 2 * rows, rows:], 0.0),
            ],
            axis=1,
        ).astype(BF16)
        read_keys = jnp.concatenate(
            [
                jnp.where(inclusive, products[2 * rows : 3 * rows, rows:], 0.0),
                jnp.where(inclusive, products[3 * rows :, rows:], 0.0),
            ],
            axis=1,
        ).astype(BF16)
        read_removal = jnp.concatenate(
            [
                jnp.where(inclusive, products[2 * rows : 3 * rows, 0:rows], 0.0),
                jnp.where(inclusive, products[3 * rows :, 0:rows], 0.0),
            ],
            axis=1,
        ).astype(BF16)
        va = values[:, lanes]
        stacked = jnp.concatenate([left(va), right(va)], axis=0)
        sums = dot(jnp.concatenate([pair_keys, read_keys], axis=0), stacked)
        kept.append((read_removal, sums))

    inverses = unit_lower_inverses(strict_parts)

    for p in range(pairs):
        lanes = slice(p * PAIR, (p + 1) * PAIR)
        read_removal, sums = kept[p]
        weights = sums[:rows].astype(BF16)
        carry = carried_in[:, lanes]
        sides = jnp.concatenate(
            [
                jnp.concatenate([left(carry), left(weights)], axis=1),
                jnp.concatenate([right(carry), right(weights)], axis=1),
            ],
            axis=0,
        )
        inverse = jnp.concatenate([inverses[2 * p], inverses[2 * p + 1]], axis=1)
        solved = dot(inverse.astype(BF16), sides).astype(BF16)
        carried, local = solved[:, :PAIR], solved[:, PAIR:]
        halves = jnp.concatenate(
            [
                jnp.concatenate([left(carried), left(local)], axis=1),
                jnp.concatenate([right(carried), right(local)], axis=1),
            ],
            axis=0,
        )
        taken = dot(read_removal, halves)
        reader_ref[:, lanes] = (read_in[:, lanes] - taken[:, :PAIR]).astype(BF16)
        local_ref[:, lanes] = sums[rows:] - taken[:, PAIR:]
        ends = dot_tn(solved, tail_removal[:, lanes])
        gathered = jnp.where(same, ends[:PAIR], 0.0).astype(BF16)
        added = jnp.where(
            same, dot_tn(values[:, lanes], tail_keys[:, lanes]) - ends[PAIR:], 0.0
        )
        gather_ref[0, p] = gathered
        add_ref[0, p] = added
        maps = maps_ref[p]
        maps = maps * fade[:, lanes] - dot(maps.astype(BF16), gathered)
        maps_ref[p, :PAIR, :] = maps[:PAIR]
        maps_ref[p, PAIR:, :] = maps[PAIR:] + added
    total_ref[...] = total_ref[...] * fade

    @pl.when(step == pl.num_programs(0) - 1)
    def _():
        low = iota((PAIR, PAIR), 1) < HEAD
        low_row = iota((1, PAIR), 1) < HEAD
        for p in range(pairs):
            lanes = slice(p * PAIR, (p + 1) * PAIR)
            total = total_ref[:, lanes]
            lost = eye * total - maps_ref[p, :PAIR, :]
            gained = maps_ref[p, PAIR:, :]
            lost = lost + pltpu.roll(lost, HEAD, 1)
            gained = gained + pltpu.roll(gained, HEAD, 1)
            both = jnp.where(low, lost, gained).astype(BF16)
            msg_ref[2 * p, :HEAD, :] = both[:HEAD]
            msg_ref[2 * p + 1, :HEAD, :] = both[HEAD:]
            for side in range(2):
                own = jnp.where(low_row == (side == 0), total, 0.0)
                own = jnp.broadcast_to(own, (16, PAIR))
                own = own + pltpu.roll(own, HEAD, 1)
                high, rest = two_parts(own)
                msg_ref[2 * p + side, HEAD:, :] = jnp.where(
                    iota((16, PAIR), 1) < HEAD, high.astype(F32), rest.astype(F32)
                ).astype(BF16)
        for s in range(GROUPS):
            sent_refs[s][...] = msg_ref[lax.rem(here_ref[0] + s, GROUPS)]


def message_parts(message):
    lost = message[:HEAD, :HEAD]
    gained = message[:HEAD, HEAD:].astype(F32)
    fades = message[HEAD : HEAD + 1, :].astype(F32)
    return lost, gained, fades[:, :HEAD] + fades[:, HEAD:]


def group_kernel(here_ref, *refs):
    in_refs, (prefix_ref, out_ref, met_ref) = refs[:GROUPS], refs[GROUPS:]
    for s in range(GROUPS):
        met_ref[lax.rem(here_ref[0] + GROUPS - s, GROUPS)] = in_refs[s][...]
    rows, cols = iota((HEAD, HEAD), 0), iota((HEAD, HEAD), 1)
    eye = (rows == cols).astype(F32)
    maps = jnp.concatenate([eye, jnp.zeros((HEAD, HEAD), F32)], axis=0)
    total = jnp.ones((1, HEAD), F32)
    for m in range(GROUPS):
        lost, gained, fade = message_parts(met_ref[m])
        prefix_ref[m] = maps
        moved = maps * fade - dot(maps.astype(BF16), lost)
        maps = jnp.concatenate([moved[:HEAD], moved[HEAD:] + gained], axis=0)
        total = total * fade
    both = jnp.concatenate([eye * total - maps[:HEAD], maps[HEAD:]], axis=1).astype(BF16)
    high, rest = two_parts(jnp.broadcast_to(total, (16, HEAD)))
    ends = jnp.concatenate([high.astype(F32), rest.astype(F32)], axis=1).astype(BF16)
    for z in range(out_ref.shape[0]):
        out_ref[z, :HEAD, :] = both
        out_ref[z, HEAD:, :] = ends


def enter_kernel(here_ref, in_ref, prefix_ref, out_ref):
    state = jnp.zeros((HEAD, HEAD), F32)
    for z in range(in_ref.shape[0]):
        lost, gained, fade = message_parts(in_ref[z])
        passed = state * fade - dot(state.astype(BF16), lost) + gained
        state = jnp.where(z < here_ref[0], passed, state)
    narrow = state.astype(BF16)
    for m in range(out_ref.shape[0]):
        entering = dot(narrow, prefix_ref[m, :HEAD, :].astype(BF16)) + prefix_ref[m, HEAD:, :]
        out_ref[m] = jnp.concatenate([entering, entering], axis=1).astype(BF16)


def readout_kernel(
    here_ref, enter_ref, reader_ref, local_ref, gather_ref, add_ref, fade_ref, gain_ref,
    weight_ref, *refs,
):
    out_refs, state_ref = refs[:-1], refs[-1]
    step = pl.program_id(0)
    spans = len(out_refs)
    channels = reader_ref.shape[1]
    pairs = channels // PAIR
    same = block_ones()
    means = jnp.where(same, 1.0 / HEAD, 0.0).astype(BF16)

    @pl.when(step == 0)
    def _():
        for p in range(pairs):
            entering = jnp.concatenate([enter_ref[2 * p], enter_ref[2 * p + 1]], axis=0)
            state_ref[p] = jnp.where(same, entering.astype(F32), 0.0)

    pieces = []
    for p in range(pairs):
        lanes = slice(p * PAIR, (p + 1) * PAIR)
        state = state_ref[p]
        narrow = state.astype(BF16)
        read = dot_nt(reader_ref[:, lanes], narrow) + local_ref[:, lanes]
        state_ref[p] = state * fade_ref[0, :, lanes] - dot(narrow, gather_ref[0, p]) + add_ref[0, p]
        centred = read - dot(read.astype(BF16), means)
        spread = dot((centred * centred).astype(BF16), means)
        pieces.append(
            (centred * lax.rsqrt(spread + GROUP_EPS) * gain_ref[:, lanes]).astype(BF16)
        )
    normed = jnp.concatenate(pieces, axis=1)
    result = dot(normed, weight_ref[...]).astype(BF16)
    for s in range(spans):

        @pl.when(lax.rem(step + spans - here_ref[0], spans) == s)
        def _():
            out_refs[s][...] = result


def hidden_kernel(x_hbm, *refs):
    weights, (out_ref, x_ref, weight_refs, sems) = refs[:8], refs[8:]
    fetch_x = pltpu.make_async_copy(x_hbm, x_ref, sems.at[8])
    fetch_x.start()
    fetches = [
        pltpu.make_async_copy(w, weight_refs.at[n], sems.at[n]) for n, w in enumerate(weights)
    ]
    for fetch in fetches:
        fetch.start()
    fetch_x.wait()
    units = weight_refs.shape[2]
    for q in range(4):
        fetches[2 * q].wait()
        fetches[2 * q + 1].wait()
        gates = dot(x_ref[...], weight_refs[2 * q])
        uppers = dot(x_ref[...], weight_refs[2 * q + 1])
        out_ref[:, q * units : (q + 1) * units] = (
            gates / (1.0 + jnp.exp(-gates)) * uppers
        ).astype(BF16)


def down_early_kernel(
    hidden_ref, own, before_0, before_1, after_0, after_1, out_ref, last_ref, weight_ref, sems
):
    units, width = own.shape
    half = width // 2
    places = (
        (own, 0, 0, width),
        (before_0, 1, 0, half),
        (after_0, 2, 0, half),
        (before_1, 1, half, half),
        (after_1, 2, half, half),
    )
    fetches = [
        pltpu.make_async_copy(
            w, weight_ref.at[row * units : (row + 1) * units, low : low + size], sems.at[n]
        )
        for n, (w, row, low, size) in enumerate(places)
    ]
    for fetch in fetches:
        fetch.start()
    last_ref[...] = hidden_ref[:, 3 * units :]
    for part, waits in ((0, fetches[:3]), (1, fetches[3:])):
        for fetch in waits:
            fetch.wait()
        lanes = slice(part * half, (part + 1) * half)
        out_ref[:, lanes] = dot(hidden_ref[:, : 3 * units], weight_ref[:, lanes]).astype(BF16)


def down_late_kernel(early_ref, hidden_ref, far_0, far_1, out_hbm, made_ref, sems):
    width = made_ref.shape[1]
    parts = 4
    tile = width // parts
    stores = []
    for part in range(parts):
        far = (far_0, far_1)[part // 2]
        low = (part % 2) * tile
        lanes = slice(part * tile, (part + 1) * tile)
        made_ref[:, lanes] = (
            early_ref[:, lanes].astype(F32) + dot(hidden_ref[...], far[:, low : low + tile])
        ).astype(BF16)
        store = pltpu.make_async_copy(made_ref.at[:, lanes], out_hbm.at[:, lanes], sems.at[part])
        store.start()
        stores.append(store)
    for store in stores:
        store.wait()


def pack_kernel(x_ref, gain_ref, routes_ref, mix_ref, out_ref, mix_out_ref):
    tokens = x_ref.shape[0]
    places = out_ref.shape[0]
    x = x_ref[...].astype(F32)
    normed = (
        x * lax.rsqrt(jnp.mean(x * x, axis=1, keepdims=True) + NORM_EPS) * gain_ref[...]
    ).astype(BF16)
    experts = places // CAPACITY
    listed = iota((experts, tokens), 0)
    first, second = routes_ref[0:1, :], routes_ref[1:2, :]
    first_mark = (first == listed).astype(F32)
    second_mark = (second == listed).astype(F32)
    before = (iota((tokens, tokens), 0) < iota((tokens, tokens), 1)).astype(F32).astype(BF16)
    earlier = dot((first_mark + second_mark).astype(BF16), before)
    rows = iota((places, tokens), 0)
    table = jnp.zeros((places, tokens), F32)
    mix = jnp.zeros((places, tokens), F32)
    for named, mark, weight in (
        (first, first_mark, mix_ref[0:1, :]),
        (second, second_mark, mix_ref[1:2, :]),
    ):
        slot = jnp.sum(earlier * mark, axis=0, keepdims=True).astype(jnp.int32)
        here = rows == named * CAPACITY + slot
        table = table + here.astype(F32)
        mix = jnp.where(here, weight, mix)
    out_ref[...] = dot(table.astype(BF16), normed).astype(BF16)
    high, rest = two_parts(jnp.transpose(mix))
    mix_out_ref[:tokens, :] = high
    mix_out_ref[tokens:, :] = rest


def combine_kernel(mix_ref, rows_ref, out_hbm, made_ref, sems):
    tokens, width = made_ref.shape
    parts = 4
    tile = width // parts
    stores = []
    for part in range(parts):
        lanes = slice(part * tile, (part + 1) * tile)
        both = dot(mix_ref[...], rows_ref[:, lanes])
        made_ref[:, lanes] = (both[:tokens] + both[tokens:]).astype(BF16)
        store = pltpu.make_async_copy(made_ref.at[:, lanes], out_hbm.at[:, lanes], sems.at[part])
        store.start()
        stores.append(store)
    for store in stores:
        store.wait()


def whole(shape):
    return pl.BlockSpec(shape, lambda *_: (0,) * len(shape))


def estimate(flops, moved, transcendentals=0):
    return pl.CostEstimate(
        flops=int(flops), bytes_accessed=int(moved), transcendentals=int(transcendentals)
    )


SCALARS = pl.BlockSpec(memory_space=pltpu.SMEM)


def summarize(here, q, k, v, di, li, base, shift):
    rows, channels = q.shape
    heads = shift.shape[0]
    pairs = heads // 2
    spans = rows // SPAN
    block = pl.BlockSpec((SPAN, channels), lambda i: (i, 0))
    square = (1, pairs, PAIR, PAIR)
    return pl.pallas_call(
        summary_kernel,
        grid=(spans,),
        in_specs=[SCALARS]
        + [block] * 5
        + [whole((1, channels)), pl.BlockSpec((heads, SPAN), lambda i: (0, i))],
        out_specs=[
            block,
            block,
            pl.BlockSpec(square, lambda i: (i, 0, 0, 0)),
            pl.BlockSpec(square, lambda i: (i, 0, 0, 0)),
            pl.BlockSpec((1, 1, channels), lambda i: (i, 0, 0)),
        ]
        + [whole((MSG_ROWS, PAIR))] * GROUPS,
        out_shape=[
            jax.ShapeDtypeStruct((rows, channels), BF16),
            jax.ShapeDtypeStruct((rows, channels), F32),
            jax.ShapeDtypeStruct((spans, pairs, PAIR, PAIR), BF16),
            jax.ShapeDtypeStruct((spans, pairs, PAIR, PAIR), F32),
            jax.ShapeDtypeStruct((spans, 1, channels), F32),
        ]
        + [jax.ShapeDtypeStruct((MSG_ROWS, PAIR), BF16)] * GROUPS,
        scratch_shapes=[
            pltpu.VMEM((pairs, 2 * PAIR, PAIR), F32),
            pltpu.VMEM((1, channels), F32),
            pltpu.VMEM((heads, MSG_ROWS, PAIR), BF16),
        ],
        compiler_params=pltpu.CompilerParams(dimension_semantics=("arbitrary",)),
        cost_estimate=estimate(2.0e10, 6 << 20, 2 << 20),
        name="summary",
    )(here, q, k, v, di, li, base, shift)


def group_scan(here, messages, copies):
    return pl.pallas_call(
        group_kernel,
        in_specs=[SCALARS] + [pl.BlockSpec(memory_space=pltpu.VMEM)] * GROUPS,
        out_shape=[
            jax.ShapeDtypeStruct((GROUPS, 2 * HEAD, HEAD), F32),
            jax.ShapeDtypeStruct((copies, MSG_ROWS, PAIR), BF16),
        ],
        scratch_shapes=[pltpu.VMEM((GROUPS, MSG_ROWS, PAIR), BF16)],
        cost_estimate=estimate(2.0e9, 1 << 20),
        name="group_scan",
    )(here, *map(in_vmem, messages))


def enter_states(here, totals, prefixes):
    return pl.pallas_call(
        enter_kernel,
        in_specs=[SCALARS] + [pl.BlockSpec(memory_space=pltpu.VMEM)] * 2,
        out_shape=jax.ShapeDtypeStruct((prefixes.shape[0], HEAD, PAIR), BF16),
        cost_estimate=estimate(2.0e9, 1 << 20),
        name="enter_states",
    )(here, in_vmem(totals), prefixes)


def read_and_project(here, entering, reader, local, gather, add, fade, gain, weight):
    rows, channels = reader.shape
    pairs = channels // PAIR
    spans = rows // SPAN
    width = weight.shape[1]
    block = pl.BlockSpec((SPAN, channels), lambda i: (i, 0))
    square = pl.BlockSpec((1, pairs, PAIR, PAIR), lambda i: (i, 0, 0, 0))
    return pl.pallas_call(
        readout_kernel,
        grid=(spans,),
        in_specs=[
            SCALARS,
            IN_VMEM,
            block,
            block,
            square,
            square,
            pl.BlockSpec((1, 1, channels), lambda i: (i, 0, 0)),
            whole((1, channels)),
            whole(weight.shape),
        ],
        out_specs=[whole((SPAN, width))] * spans,
        out_shape=[jax.ShapeDtypeStruct((SPAN, width), BF16)] * spans,
        scratch_shapes=[pltpu.VMEM((pairs, PAIR, PAIR), F32)],
        compiler_params=pltpu.CompilerParams(dimension_semantics=("arbitrary",)),
        cost_estimate=estimate(5.0e9, 8 << 20),
        name="readout",
    )(here, in_vmem(entering), reader, local, gather, add, fade, gain, weight)


IN_HBM = pl.BlockSpec(memory_space=pltpu.HBM)
IN_VMEM = pl.BlockSpec(memory_space=pltpu.VMEM)


def expert_hidden(x, weights):
    rows, width = x.shape
    units = weights[0].shape[1]
    count = len(weights)
    return pl.pallas_call(
        hidden_kernel,
        in_specs=[IN_HBM] * (1 + count),
        out_specs=IN_VMEM,
        out_shape=jax.ShapeDtypeStruct((rows, units * count // 2), BF16),
        scratch_shapes=[
            pltpu.VMEM((rows, width), BF16),
            pltpu.VMEM((count, width, units), BF16),
            pltpu.SemaphoreType.DMA((count + 1,)),
        ],
        cost_estimate=estimate(2 * rows * width * units * count, 11 << 20, rows * units * 4),
        name="hidden",
    )(pltpu.with_memory_space_constraint(x, pltpu.HBM), *weights)


def expert_down_early(hidden, own, before, after):
    rows = hidden.shape[0]
    units, width = own.shape
    return pl.pallas_call(
        down_early_kernel,
        in_specs=[IN_VMEM] + [IN_HBM] * 5,
        out_specs=[IN_VMEM, IN_VMEM],
        out_shape=[pltpu.VMEM((rows, width), BF16), pltpu.VMEM((rows, units), BF16)],
        scratch_shapes=[
            pltpu.VMEM((3 * units, width), BF16),
            pltpu.SemaphoreType.DMA((5,)),
        ],
        cost_estimate=estimate(6 * rows * units * width, 6 << 20),
        name="down_early",
    )(hidden, own, *before, *after)


def expert_down_late(early, hidden, far):
    rows, width = early.shape
    units = far[0].shape[0]
    return pl.pallas_call(
        down_late_kernel,
        in_specs=[IN_VMEM] * 4,
        out_specs=IN_HBM,
        out_shape=jax.ShapeDtypeStruct((rows, width), BF16),
        scratch_shapes=[
            pltpu.VMEM((rows, width), BF16),
            pltpu.SemaphoreType.DMA((4,)),
        ],
        cost_estimate=estimate(2 * rows * units * width, 5 << 20),
        name="down_late",
    )(in_vmem(early), in_vmem(hidden), *map(in_vmem, far))


def pack_rows(x, gain, routes, mix, places):
    tokens, width = x.shape
    return pl.pallas_call(
        pack_kernel,
        out_shape=[
            jax.ShapeDtypeStruct((places, width), BF16),
            jax.ShapeDtypeStruct((2 * tokens, places), BF16),
        ],
        cost_estimate=estimate(2.0e9, 3 << 20),
        name="pack",
    )(x, gain, routes, mix)


def combine_rows(mix, rows):
    tokens = mix.shape[0] // 2
    width = rows.shape[1]
    return pl.pallas_call(
        combine_kernel,
        in_specs=[IN_VMEM, IN_VMEM],
        out_specs=IN_HBM,
        out_shape=jax.ShapeDtypeStruct((tokens, width), BF16),
        scratch_shapes=[pltpu.VMEM((tokens, width), BF16), pltpu.SemaphoreType.DMA((4,))],
        cost_estimate=estimate(1.0e9, 3 << 20),
        name="combine",
    )(mix, in_vmem(rows))


def ring(x, shift, axis="tp"):
    count = lax.axis_size(axis)
    return lax.ppermute(x, axis, [(i, (i + shift) % count) for i in range(count)])


def around(parts, axis):
    return [parts[0]] + [ring(part, n, axis) for n, part in enumerate(parts) if n]


def in_vmem(x):
    return pltpu.with_memory_space_constraint(x, pltpu.VMEM)


def exchange(x, axis):
    return lax.all_to_all(x, axis, 0, 0, tiled=True)


def on_device(
    receptance,
    key_rows,
    value_rows,
    decay_input,
    learn_input,
    decay_base,
    decay_shift,
    channel_gain,
    out_weight,
    expert_input,
    expert_gain,
    routes,
    route_weight,
    gate_weight,
    up_weight,
    down_weight,
):
    ep_count = lax.axis_size(EP)
    _, model_width = expert_input.shape
    experts = gate_weight.shape[0] * ep_count
    places = experts * CAPACITY

    w_gate = gate_weight[0]
    w_up = up_weight[0]
    w_down = down_weight[0]
    cut = model_width // 2
    down_0, down_1 = w_down[:, :cut], w_down[:, cut:]
    gate_r, up_l = ring(w_gate, 1), ring(w_up, -1)
    up_r, gate_l = ring(w_up, 1), ring(w_gate, -1)
    gate_f, up_f = ring(gate_r, 1), ring(up_l, -1)
    down_0r, down_1l = ring(down_0, 1), ring(down_1, -1)
    down_1r, down_0l = ring(down_1, 1), ring(down_0, -1)
    down_0f, down_1f = ring(down_0r, 1), ring(down_1l, -1)

    outgoing, mix = pack_rows(
        expert_input, expert_gain.reshape(1, -1), routes.T, route_weight.T, places
    )
    arrived = exchange(
        outgoing.reshape(experts, CAPACITY, model_width), EP
    ).reshape(places, model_width)

    def here(axis):
        return lax.axis_index(axis).astype(jnp.int32).reshape(1)

    reader, local, gather, add, fade, *messages = summarize(
        here(GROUP),
        receptance,
        key_rows,
        value_rows,
        decay_input,
        learn_input,
        decay_base.reshape(1, -1),
        decay_shift.T,
    )
    prefixes, totals = group_scan(here(GROUP), around(messages, GROUP), lax.axis_size("ep_0"))
    entered = enter_states(here("ep_0"), exchange(totals, "ep_0"), prefixes)
    partial = read_and_project(
        here("tp"),
        exchange(entered, GROUP),
        reader,
        local,
        gather,
        add,
        fade,
        channel_gain.reshape(1, -1),
        out_weight,
    )
    shares = around(partial, "tp")
    mixer_out = sum(share.astype(F32) for share in shares).astype(BF16)

    hiddens = expert_hidden(
        arrived, [w_gate, w_up, gate_r, up_r, gate_l, up_l, gate_f, up_f]
    )
    early, last = expert_down_early(hiddens, w_down, (down_0r, down_1r), (down_0l, down_1l))
    returning = expert_down_late(early, last, (down_0f, down_1f))
    returned = exchange(returning.reshape(ep_count, CAPACITY, model_width), EP)
    return (mixer_out, combine_rows(mix, returned.reshape(places, model_width)))


def solution(mesh):
    finer = Mesh(mesh.devices.reshape(8, 4, 2, mesh.shape["tp"]), ("ep_0", "ep_1", "ep_2", "tp"))
    placed = (
        P(EP, "tp"),
        P(EP, "tp"),
        P(EP, "tp"),
        P(EP, "tp"),
        P(EP, "tp"),
        P("tp"),
        P(EP, "tp"),
        P("tp"),
        P("tp", None),
        P(EP_TP, None),
        P(),
        P(EP_TP, None),
        P(EP_TP, None),
        P(EP, None, "tp"),
        P(EP, None, "tp"),
        P(EP, "tp", None),
    )

    return jax.shard_map(
        on_device,
        mesh=finer,
        in_specs=placed,
        out_specs=(P(EP_TP, None), P(EP_TP, None)),
        check_vma=False,
    )
```

```python
import jax
import jax.numpy as jnp
from jax import lax
from jax.experimental import pallas as pl
from jax.experimental.pallas import tpu as pltpu
from jax.sharding import Mesh
from jax.sharding import PartitionSpec as P


SPAN = 128
EP = ("ep_0", "ep_1", "ep_2")
GROUP = ("ep_1", "ep_2")
EP_TP = ("ep_0", "ep_1", "ep_2", "tp")
GROUPS = 8
HEAD = 64
PAIR = 128
MSG_ROWS = 80
CAPACITY = 8

NORM_EPS = 1e-06
GROUP_EPS = 0.00064
KEY_EPS = 1e-06
DECAY_SCALE = 0.6065306597126334

F32 = jnp.float32
BF16 = jnp.bfloat16


def dot(a, b):
    return lax.dot_general(a, b, (((1,), (0,)), ((), ())), preferred_element_type=F32)


def dot_nt(a, b):
    return lax.dot_general(a, b, (((1,), (1,)), ((), ())), preferred_element_type=F32)


def dot_tn(a, b):
    return lax.dot_general(a, b, (((0,), (0,)), ((), ())), preferred_element_type=F32)


def two_parts(x):
    high = x.astype(BF16)
    return high, (x - high.astype(F32)).astype(BF16)


def iota(shape, dim):
    return lax.broadcasted_iota(jnp.int32, shape, dim)


def block_ones():
    rows, cols = iota((PAIR, PAIR), 0), iota((PAIR, PAIR), 1)
    return (rows // HEAD) == (cols // HEAD)


def unit_lower_inverses(parts):
    size = parts[0].shape[0]
    rows, cols = iota((size, size), 0), iota((size, size), 1)
    eye = (rows == cols).astype(F32)
    start = 16
    inside = (rows // start) == (cols // start)
    powers = [jnp.where(inside, -a, 0.0) for a in parts]
    inverses = [eye + p for p in powers]
    reach = 2
    while reach < start:
        narrow = [p.astype(BF16) for p in powers]
        powers = [dot(p, p) for p in narrow]
        inverses = [
            inv + dot(inv.astype(BF16), p.astype(BF16))
            for inv, p in zip(inverses, powers)
        ]
        reach *= 2
    block = start
    while block < size:
        joined = ((rows // (2 * block)) == (cols // (2 * block))) & (
            (rows // block) != (cols // block)
        )
        narrow = [inv.astype(BF16) for inv in inverses]
        corners = [jnp.where(joined, a, 0.0).astype(BF16) for a in parts]
        moved = [dot(c, inv).astype(BF16) for c, inv in zip(corners, narrow)]
        inverses = [
            inv - dot(short, m) for inv, short, m in zip(inverses, narrow, moved)
        ]
        block *= 2
    return inverses


def summary_kernel(
    here_ref, q_ref, k_ref, v_ref, di_ref, li_ref, base_ref, shift_ref,
    reader_ref, local_ref, gather_ref, add_ref, fade_ref, *rest_refs,
):
    sent_refs, (maps_ref, total_ref, msg_ref) = rest_refs[:GROUPS], rest_refs[GROUPS:]
    step = pl.program_id(0)
    rows, channels = q_ref.shape
    heads = shift_ref.shape[0]
    pairs = heads // 2
    same = block_ones()
    same_f = same.astype(F32)
    same_b = same_f.astype(BF16)
    row2, col2 = iota((PAIR, PAIR), 0), iota((PAIR, PAIR), 1)
    eye = (row2 == col2).astype(F32)

    @pl.when(step == 0)
    def _():
        for p in range(pairs):
            maps_ref[p, :PAIR, :] = eye
            maps_ref[p, PAIR:, :] = jnp.zeros((PAIR, PAIR), F32)
        total_ref[...] = jnp.ones_like(total_ref)

    spread = (
        (iota((heads, channels), 1) // HEAD) == iota((heads, channels), 0)
    ).astype(F32).astype(BF16)
    shift_high, shift_low = two_parts(shift_ref[...])
    pre = (
        di_ref[...].astype(F32)
        + base_ref[...]
        + (dot_tn(shift_high, spread) + dot_tn(shift_low, spread))
    )
    log_decay = -DECAY_SCALE / (1.0 + jnp.exp(-pre))
    tri_rows, tri_cols = iota((rows, rows), 0), iota((rows, rows), 1)
    inclusive = tri_rows >= tri_cols
    strict = tri_rows > tri_cols
    tri = inclusive.astype(F32).astype(BF16)
    decay_high, decay_low = two_parts(log_decay)
    cum = dot(tri, decay_high) + dot(tri, decay_low)
    middle = cum[rows // 2 - 1 : rows // 2, :]
    ending = cum[rows - 1 : rows, :]
    grow = jnp.exp(cum - middle)
    grow_before = grow * jnp.exp(-log_decay)
    shrink = jnp.exp(middle - cum)
    from_start = jnp.exp(middle)
    to_end = jnp.exp(ending - middle)
    fade = jnp.exp(ending)
    fade_ref[0] = fade

    keys = k_ref[...].astype(F32)
    recept = q_ref[...].astype(F32)
    squares_high, squares_low = two_parts(keys * keys)
    lengths = jnp.concatenate(
        [
            dot(squares_high[:, p * PAIR : (p + 1) * PAIR], same_b)
            + dot(squares_low[:, p * PAIR : (p + 1) * PAIR], same_b)
            for p in range(pairs)
        ],
        axis=1,
    )
    unit = keys * lax.rsqrt(lengths + KEY_EPS)
    removal = unit / (1.0 + jnp.exp(-li_ref[...].astype(F32)))

    probes_f = unit * grow_before
    queries_f = recept * grow
    back_removal_f = removal * shrink
    back_keys_f = keys * shrink
    probes = probes_f.astype(BF16)
    queries = queries_f.astype(BF16)
    back_removal = back_removal_f.astype(BF16)
    back_keys = back_keys_f.astype(BF16)
    carried_in = (probes_f * from_start).astype(BF16)
    read_in = queries_f * from_start
    tail_removal = (back_removal_f * to_end).astype(BF16)
    tail_keys = (back_keys_f * to_end).astype(BF16)
    values = v_ref[...]

    first = iota((rows, PAIR), 1) < HEAD
    none = jnp.zeros((rows, PAIR), BF16)

    def left(x):
        return jnp.where(first, x, none)

    def right(x):
        return jnp.where(first, none, x)

    kept = []
    strict_parts = []
    for p in range(pairs):
        lanes = slice(p * PAIR, (p + 1) * PAIR)
        pr, qu = probes[:, lanes], queries[:, lanes]
        outer = jnp.concatenate([left(pr), right(pr), left(qu), right(qu)], axis=0)
        inner = jnp.concatenate([back_removal[:, lanes], back_keys[:, lanes]], axis=0)
        products = dot_nt(outer, inner)
        strict_parts.append(jnp.where(strict, products[0:rows, 0:rows], 0.0))
        strict_parts.append(jnp.where(strict, products[rows : 2 * rows, 0:rows], 0.0))
        pair_keys = jnp.concatenate(
            [
                jnp.where(strict, products[0:rows, rows:], 0.0),
                jnp.where(strict, products[rows : 2 * rows, rows:], 0.0),
            ],
            axis=1,
        ).astype(BF16)
        read_keys = jnp.concatenate(
            [
                jnp.where(inclusive, products[2 * rows : 3 * rows, rows:], 0.0),
                jnp.where(inclusive, products[3 * rows :, rows:], 0.0),
            ],
            axis=1,
        ).astype(BF16)
        read_removal = jnp.concatenate(
            [
                jnp.where(inclusive, products[2 * rows : 3 * rows, 0:rows], 0.0),
                jnp.where(inclusive, products[3 * rows :, 0:rows], 0.0),
            ],
            axis=1,
        ).astype(BF16)
        va = values[:, lanes]
        stacked = jnp.concatenate([left(va), right(va)], axis=0)
        sums = dot(jnp.concatenate([pair_keys, read_keys], axis=0), stacked)
        kept.append((read_removal, sums))

    inverses = unit_lower_inverses(strict_parts)

    for p in range(pairs):
        lanes = slice(p * PAIR, (p + 1) * PAIR)
        read_removal, sums = kept[p]
        weights = sums[:rows].astype(BF16)
        carry = carried_in[:, lanes]
        sides = jnp.concatenate(
            [
                jnp.concatenate([left(carry), left(weights)], axis=1),
                jnp.concatenate([right(carry), right(weights)], axis=1),
            ],
            axis=0,
        )
        inverse = jnp.concatenate([inverses[2 * p], inverses[2 * p + 1]], axis=1)
        solved = dot(inverse.astype(BF16), sides).astype(BF16)
        carried, local = solved[:, :PAIR], solved[:, PAIR:]
        halves = jnp.concatenate(
            [
                jnp.concatenate([left(carried), left(local)], axis=1),
                jnp.concatenate([right(carried), right(local)], axis=1),
            ],
            axis=0,
        )
        taken = dot(read_removal, halves)
        reader_ref[:, lanes] = (read_in[:, lanes] - taken[:, :PAIR]).astype(BF16)
        local_ref[:, lanes] = sums[rows:] - taken[:, PAIR:]
        ends = dot_tn(solved, tail_removal[:, lanes])
        gathered = jnp.where(same, ends[:PAIR], 0.0).astype(BF16)
        added = jnp.where(
            same, dot_tn(values[:, lanes], tail_keys[:, lanes]) - ends[PAIR:], 0.0
        )
        gather_ref[0, p] = gathered
        add_ref[0, p] = added
        maps = maps_ref[p]
        maps = maps * fade[:, lanes] - dot(maps.astype(BF16), gathered)
        maps_ref[p, :PAIR, :] = maps[:PAIR]
        maps_ref[p, PAIR:, :] = maps[PAIR:] + added
    total_ref[...] = total_ref[...] * fade

    @pl.when(step == pl.num_programs(0) - 1)
    def _():
        low = iota((PAIR, PAIR), 1) < HEAD
        low_row = iota((1, PAIR), 1) < HEAD
        for p in range(pairs):
            lanes = slice(p * PAIR, (p + 1) * PAIR)
            total = total_ref[:, lanes]
            lost = eye * total - maps_ref[p, :PAIR, :]
            gained = maps_ref[p, PAIR:, :]
            lost = lost + pltpu.roll(lost, HEAD, 1)
            gained = gained + pltpu.roll(gained, HEAD, 1)
            both = jnp.where(low, lost, gained).astype(BF16)
            msg_ref[2 * p, :HEAD, :] = both[:HEAD]
            msg_ref[2 * p + 1, :HEAD, :] = both[HEAD:]
            for side in range(2):
                own = jnp.where(low_row == (side == 0), total, 0.0)
                own = jnp.broadcast_to(own, (16, PAIR))
                own = own + pltpu.roll(own, HEAD, 1)
                high, rest = two_parts(own)
                msg_ref[2 * p + side, HEAD:, :] = jnp.where(
                    iota((16, PAIR), 1) < HEAD, high.astype(F32), rest.astype(F32)
                ).astype(BF16)
        for s in range(GROUPS):
            sent_refs[s][...] = msg_ref[lax.rem(here_ref[0] + s, GROUPS)]


def message_parts(message):
    lost = message[:HEAD, :HEAD]
    gained = message[:HEAD, HEAD:].astype(F32)
    fades = message[HEAD : HEAD + 1, :].astype(F32)
    return lost, gained, fades[:, :HEAD] + fades[:, HEAD:]


def group_kernel(here_ref, *refs):
    in_refs, (prefix_ref, out_ref, met_ref) = refs[:GROUPS], refs[GROUPS:]
    for s in range(GROUPS):
        met_ref[lax.rem(here_ref[0] + GROUPS - s, GROUPS)] = in_refs[s][...]
    rows, cols = iota((HEAD, HEAD), 0), iota((HEAD, HEAD), 1)
    eye = (rows == cols).astype(F32)
    maps = jnp.concatenate([eye, jnp.zeros((HEAD, HEAD), F32)], axis=0)
    total = jnp.ones((1, HEAD), F32)
    for m in range(GROUPS):
        lost, gained, fade = message_parts(met_ref[m])
        prefix_ref[m] = maps
        moved = maps * fade - dot(maps.astype(BF16), lost)
        maps = jnp.concatenate([moved[:HEAD], moved[HEAD:] + gained], axis=0)
        total = total * fade
    both = jnp.concatenate([eye * total - maps[:HEAD], maps[HEAD:]], axis=1).astype(BF16)
    high, rest = two_parts(jnp.broadcast_to(total, (16, HEAD)))
    ends = jnp.concatenate([high.astype(F32), rest.astype(F32)], axis=1).astype(BF16)
    for z in range(out_ref.shape[0]):
        out_ref[z, :HEAD, :] = both
        out_ref[z, HEAD:, :] = ends


def enter_kernel(here_ref, in_ref, prefix_ref, out_ref):
    state = jnp.zeros((HEAD, HEAD), F32)
    for z in range(in_ref.shape[0]):
        lost, gained, fade = message_parts(in_ref[z])
        passed = state * fade - dot(state.astype(BF16), lost) + gained
        state = jnp.where(z < here_ref[0], passed, state)
    narrow = state.astype(BF16)
    for m in range(out_ref.shape[0]):
        entering = dot(narrow, prefix_ref[m, :HEAD, :].astype(BF16)) + prefix_ref[m, HEAD:, :]
        out_ref[m] = jnp.concatenate([entering, entering], axis=1).astype(BF16)


def readout_kernel(
    here_ref, enter_ref, reader_ref, local_ref, gather_ref, add_ref, fade_ref, gain_ref,
    weight_ref, *refs,
):
    out_refs, state_ref = refs[:-1], refs[-1]
    step = pl.program_id(0)
    spans = len(out_refs)
    channels = reader_ref.shape[1]
    pairs = channels // PAIR
    same = block_ones()
    means = jnp.where(same, 1.0 / HEAD, 0.0).astype(BF16)

    @pl.when(step == 0)
    def _():
        for p in range(pairs):
            entering = jnp.concatenate([enter_ref[2 * p], enter_ref[2 * p + 1]], axis=0)
            state_ref[p] = jnp.where(same, entering.astype(F32), 0.0)

    pieces = []
    for p in range(pairs):
        lanes = slice(p * PAIR, (p + 1) * PAIR)
        state = state_ref[p]
        narrow = state.astype(BF16)
        read = dot_nt(reader_ref[:, lanes], narrow) + local_ref[:, lanes]
        state_ref[p] = state * fade_ref[0, :, lanes] - dot(narrow, gather_ref[0, p]) + add_ref[0, p]
        centred = read - dot(read.astype(BF16), means)
        spread = dot((centred * centred).astype(BF16), means)
        pieces.append(
            (centred * lax.rsqrt(spread + GROUP_EPS) * gain_ref[:, lanes]).astype(BF16)
        )
    normed = jnp.concatenate(pieces, axis=1)
    result = dot(normed, weight_ref[...]).astype(BF16)
    for s in range(spans):

        @pl.when(lax.rem(step + spans - here_ref[0], spans) == s)
        def _():
            out_refs[s][...] = result


def hidden_kernel(x_hbm, *refs):
    weights, (out_ref, x_ref, weight_refs, sems) = refs[:8], refs[8:]
    fetch_x = pltpu.make_async_copy(x_hbm, x_ref, sems.at[8])
    fetch_x.start()
    fetches = [
        pltpu.make_async_copy(w, weight_refs.at[n], sems.at[n]) for n, w in enumerate(weights)
    ]
    for fetch in fetches:
        fetch.start()
    fetch_x.wait()
    units = weight_refs.shape[2]
    for q in range(4):
        fetches[2 * q].wait()
        fetches[2 * q + 1].wait()
        gates = dot(x_ref[...], weight_refs[2 * q])
        uppers = dot(x_ref[...], weight_refs[2 * q + 1])
        out_ref[:, q * units : (q + 1) * units] = (
            gates / (1.0 + jnp.exp(-gates)) * uppers
        ).astype(BF16)


def down_early_kernel(
    hidden_ref, own, before_0, before_1, after_0, after_1, out_ref, last_ref, weight_ref, sems
):
    units, width = own.shape
    half = width // 2
    places = (
        (own, 0, 0, width),
        (before_0, 1, 0, half),
        (after_0, 2, 0, half),
        (before_1, 1, half, half),
        (after_1, 2, half, half),
    )
    fetches = [
        pltpu.make_async_copy(
            w, weight_ref.at[row * units : (row + 1) * units, low : low + size], sems.at[n]
        )
        for n, (w, row, low, size) in enumerate(places)
    ]
    for fetch in fetches:
        fetch.start()
    last_ref[...] = hidden_ref[:, 3 * units :]
    for part, waits in ((0, fetches[:3]), (1, fetches[3:])):
        for fetch in waits:
            fetch.wait()
        lanes = slice(part * half, (part + 1) * half)
        out_ref[:, lanes] = dot(hidden_ref[:, : 3 * units], weight_ref[:, lanes]).astype(BF16)


def down_late_kernel(early_ref, hidden_ref, far_0, far_1, out_hbm, made_ref, sems):
    width = made_ref.shape[1]
    parts = 4
    tile = width // parts
    stores = []
    for part in range(parts):
        far = (far_0, far_1)[part // 2]
        low = (part % 2) * tile
        lanes = slice(part * tile, (part + 1) * tile)
        made_ref[:, lanes] = (
            early_ref[:, lanes].astype(F32) + dot(hidden_ref[...], far[:, low : low + tile])
        ).astype(BF16)
        store = pltpu.make_async_copy(made_ref.at[:, lanes], out_hbm.at[:, lanes], sems.at[part])
        store.start()
        stores.append(store)
    for store in stores:
        store.wait()


def pack_kernel(x_ref, gain_ref, routes_ref, mix_ref, out_ref, mix_out_ref):
    tokens = x_ref.shape[0]
    places = out_ref.shape[0]
    x = x_ref[...].astype(F32)
    normed = (
        x * lax.rsqrt(jnp.mean(x * x, axis=1, keepdims=True) + NORM_EPS) * gain_ref[...]
    ).astype(BF16)
    experts = places // CAPACITY
    listed = iota((experts, tokens), 0)
    first, second = routes_ref[0:1, :], routes_ref[1:2, :]
    first_mark = (first == listed).astype(F32)
    second_mark = (second == listed).astype(F32)
    before = (iota((tokens, tokens), 0) < iota((tokens, tokens), 1)).astype(F32).astype(BF16)
    earlier = dot((first_mark + second_mark).astype(BF16), before)
    rows = iota((places, tokens), 0)
    table = jnp.zeros((places, tokens), F32)
    mix = jnp.zeros((places, tokens), F32)
    for named, mark, weight in (
        (first, first_mark, mix_ref[0:1, :]),
        (second, second_mark, mix_ref[1:2, :]),
    ):
        slot = jnp.sum(earlier * mark, axis=0, keepdims=True).astype(jnp.int32)
        here = rows == named * CAPACITY + slot
        table = table + here.astype(F32)
        mix = jnp.where(here, weight, mix)
    out_ref[...] = dot(table.astype(BF16), normed).astype(BF16)
    mix_out_ref[...] = jnp.transpose(mix).astype(BF16)


def combine_kernel(mix_ref, rows_ref, out_hbm, made_ref, sems):
    width = made_ref.shape[1]
    parts = 4
    tile = width // parts
    stores = []
    for part in range(parts):
        lanes = slice(part * tile, (part + 1) * tile)
        made_ref[:, lanes] = dot(mix_ref[...], rows_ref[:, lanes]).astype(BF16)
        store = pltpu.make_async_copy(made_ref.at[:, lanes], out_hbm.at[:, lanes], sems.at[part])
        store.start()
        stores.append(store)
    for store in stores:
        store.wait()


def whole(shape):
    return pl.BlockSpec(shape, lambda *_: (0,) * len(shape))


def estimate(flops, moved, transcendentals=0):
    return pl.CostEstimate(
        flops=int(flops), bytes_accessed=int(moved), transcendentals=int(transcendentals)
    )


SCALARS = pl.BlockSpec(memory_space=pltpu.SMEM)


def summarize(here, q, k, v, di, li, base, shift):
    rows, channels = q.shape
    heads = shift.shape[0]
    pairs = heads // 2
    spans = rows // SPAN
    block = pl.BlockSpec((SPAN, channels), lambda i: (i, 0))
    square = (1, pairs, PAIR, PAIR)
    return pl.pallas_call(
        summary_kernel,
        grid=(spans,),
        in_specs=[SCALARS]
        + [block] * 5
        + [whole((1, channels)), pl.BlockSpec((heads, SPAN), lambda i: (0, i))],
        out_specs=[
            block,
            block,
            pl.BlockSpec(square, lambda i: (i, 0, 0, 0)),
            pl.BlockSpec(square, lambda i: (i, 0, 0, 0)),
            pl.BlockSpec((1, 1, channels), lambda i: (i, 0, 0)),
        ]
        + [whole((MSG_ROWS, PAIR))] * GROUPS,
        out_shape=[
            jax.ShapeDtypeStruct((rows, channels), BF16),
            jax.ShapeDtypeStruct((rows, channels), F32),
            jax.ShapeDtypeStruct((spans, pairs, PAIR, PAIR), BF16),
            jax.ShapeDtypeStruct((spans, pairs, PAIR, PAIR), F32),
            jax.ShapeDtypeStruct((spans, 1, channels), F32),
        ]
        + [jax.ShapeDtypeStruct((MSG_ROWS, PAIR), BF16)] * GROUPS,
        scratch_shapes=[
            pltpu.VMEM((pairs, 2 * PAIR, PAIR), F32),
            pltpu.VMEM((1, channels), F32),
            pltpu.VMEM((heads, MSG_ROWS, PAIR), BF16),
        ],
        compiler_params=pltpu.CompilerParams(dimension_semantics=("arbitrary",)),
        cost_estimate=estimate(2.0e10, 6 << 20, 2 << 20),
        name="summary",
    )(here, q, k, v, di, li, base, shift)


def group_scan(here, messages, copies):
    return pl.pallas_call(
        group_kernel,
        in_specs=[SCALARS] + [pl.BlockSpec(memory_space=pltpu.VMEM)] * GROUPS,
        out_shape=[
            jax.ShapeDtypeStruct((GROUPS, 2 * HEAD, HEAD), F32),
            jax.ShapeDtypeStruct((copies, MSG_ROWS, PAIR), BF16),
        ],
        scratch_shapes=[pltpu.VMEM((GROUPS, MSG_ROWS, PAIR), BF16)],
        cost_estimate=estimate(2.0e9, 1 << 20),
        name="group_scan",
    )(here, *map(in_vmem, messages))


def enter_states(here, totals, prefixes):
    return pl.pallas_call(
        enter_kernel,
        in_specs=[SCALARS] + [pl.BlockSpec(memory_space=pltpu.VMEM)] * 2,
        out_shape=jax.ShapeDtypeStruct((prefixes.shape[0], HEAD, PAIR), BF16),
        cost_estimate=estimate(2.0e9, 1 << 20),
        name="enter_states",
    )(here, in_vmem(totals), prefixes)


def read_and_project(here, entering, reader, local, gather, add, fade, gain, weight):
    rows, channels = reader.shape
    pairs = channels // PAIR
    spans = rows // SPAN
    width = weight.shape[1]
    block = pl.BlockSpec((SPAN, channels), lambda i: (i, 0))
    square = pl.BlockSpec((1, pairs, PAIR, PAIR), lambda i: (i, 0, 0, 0))
    return pl.pallas_call(
        readout_kernel,
        grid=(spans,),
        in_specs=[
            SCALARS,
            IN_VMEM,
            block,
            block,
            square,
            square,
            pl.BlockSpec((1, 1, channels), lambda i: (i, 0, 0)),
            whole((1, channels)),
            whole(weight.shape),
        ],
        out_specs=[whole((SPAN, width))] * spans,
        out_shape=[jax.ShapeDtypeStruct((SPAN, width), BF16)] * spans,
        scratch_shapes=[pltpu.VMEM((pairs, PAIR, PAIR), F32)],
        compiler_params=pltpu.CompilerParams(dimension_semantics=("arbitrary",)),
        cost_estimate=estimate(5.0e9, 8 << 20),
        name="readout",
    )(here, in_vmem(entering), reader, local, gather, add, fade, gain, weight)


IN_HBM = pl.BlockSpec(memory_space=pltpu.HBM)
IN_VMEM = pl.BlockSpec(memory_space=pltpu.VMEM)


def expert_hidden(x, weights):
    rows, width = x.shape
    units = weights[0].shape[1]
    count = len(weights)
    return pl.pallas_call(
        hidden_kernel,
        in_specs=[IN_HBM] * (1 + count),
        out_specs=IN_VMEM,
        out_shape=jax.ShapeDtypeStruct((rows, units * count // 2), BF16),
        scratch_shapes=[
            pltpu.VMEM((rows, width), BF16),
            pltpu.VMEM((count, width, units), BF16),
            pltpu.SemaphoreType.DMA((count + 1,)),
        ],
        cost_estimate=estimate(2 * rows * width * units * count, 11 << 20, rows * units * 4),
        name="hidden",
    )(pltpu.with_memory_space_constraint(x, pltpu.HBM), *weights)


def expert_down_early(hidden, own, before, after):
    rows = hidden.shape[0]
    units, width = own.shape
    return pl.pallas_call(
        down_early_kernel,
        in_specs=[IN_VMEM] + [IN_HBM] * 5,
        out_specs=[IN_VMEM, IN_VMEM],
        out_shape=[pltpu.VMEM((rows, width), BF16), pltpu.VMEM((rows, units), BF16)],
        scratch_shapes=[
            pltpu.VMEM((3 * units, width), BF16),
            pltpu.SemaphoreType.DMA((5,)),
        ],
        cost_estimate=estimate(6 * rows * units * width, 6 << 20),
        name="down_early",
    )(hidden, own, *before, *after)


def expert_down_late(early, hidden, far):
    rows, width = early.shape
    units = far[0].shape[0]
    return pl.pallas_call(
        down_late_kernel,
        in_specs=[IN_VMEM] * 4,
        out_specs=IN_HBM,
        out_shape=jax.ShapeDtypeStruct((rows, width), BF16),
        scratch_shapes=[
            pltpu.VMEM((rows, width), BF16),
            pltpu.SemaphoreType.DMA((4,)),
        ],
        cost_estimate=estimate(2 * rows * units * width, 5 << 20),
        name="down_late",
    )(in_vmem(early), in_vmem(hidden), *map(in_vmem, far))


def pack_rows(x, gain, routes, mix, places):
    tokens, width = x.shape
    return pl.pallas_call(
        pack_kernel,
        out_shape=[
            jax.ShapeDtypeStruct((places, width), BF16),
            jax.ShapeDtypeStruct((tokens, places), BF16),
        ],
        cost_estimate=estimate(2.0e9, 3 << 20),
        name="pack",
    )(x, gain, routes, mix)


def combine_rows(mix, rows):
    tokens = mix.shape[0]
    width = rows.shape[1]
    return pl.pallas_call(
        combine_kernel,
        in_specs=[IN_VMEM, IN_VMEM],
        out_specs=IN_HBM,
        out_shape=jax.ShapeDtypeStruct((tokens, width), BF16),
        scratch_shapes=[pltpu.VMEM((tokens, width), BF16), pltpu.SemaphoreType.DMA((4,))],
        cost_estimate=estimate(1.0e9, 3 << 20),
        name="combine",
    )(mix, in_vmem(rows))


def ring(x, shift, axis="tp"):
    count = lax.axis_size(axis)
    return lax.ppermute(x, axis, [(i, (i + shift) % count) for i in range(count)])


def around(parts, axis):
    return [parts[0]] + [ring(part, n, axis) for n, part in enumerate(parts) if n]


def in_vmem(x):
    return pltpu.with_memory_space_constraint(x, pltpu.VMEM)


def exchange(x, axis):
    return lax.all_to_all(x, axis, 0, 0, tiled=True)


def on_device(
    receptance,
    key_rows,
    value_rows,
    decay_input,
    learn_input,
    decay_base,
    decay_shift,
    channel_gain,
    out_weight,
    expert_input,
    expert_gain,
    routes,
    route_weight,
    gate_weight,
    up_weight,
    down_weight,
):
    ep_count = lax.axis_size(EP)
    _, model_width = expert_input.shape
    experts = gate_weight.shape[0] * ep_count
    places = experts * CAPACITY

    w_gate = gate_weight[0]
    w_up = up_weight[0]
    w_down = down_weight[0]
    cut = model_width // 2
    down_0, down_1 = w_down[:, :cut], w_down[:, cut:]
    gate_r, up_l = ring(w_gate, 1), ring(w_up, -1)
    up_r, gate_l = ring(w_up, 1), ring(w_gate, -1)
    gate_f, up_f = ring(gate_r, 1), ring(up_l, -1)
    down_0r, down_1l = ring(down_0, 1), ring(down_1, -1)
    down_1r, down_0l = ring(down_1, 1), ring(down_0, -1)
    down_0f, down_1f = ring(down_0r, 1), ring(down_1l, -1)

    outgoing, mix = pack_rows(
        expert_input, expert_gain.reshape(1, -1), routes.T, route_weight.T, places
    )
    arrived = exchange(
        outgoing.reshape(experts, CAPACITY, model_width), EP
    ).reshape(places, model_width)

    def here(axis):
        return lax.axis_index(axis).astype(jnp.int32).reshape(1)

    reader, local, gather, add, fade, *messages = summarize(
        here(GROUP),
        receptance,
        key_rows,
        value_rows,
        decay_input,
        learn_input,
        decay_base.reshape(1, -1),
        decay_shift.T,
    )
    prefixes, totals = group_scan(here(GROUP), around(messages, GROUP), lax.axis_size("ep_0"))
    entered = enter_states(here("ep_0"), exchange(totals, "ep_0"), prefixes)
    partial = read_and_project(
        here("tp"),
        exchange(entered, GROUP),
        reader,
        local,
        gather,
        add,
        fade,
        channel_gain.reshape(1, -1),
        out_weight,
    )
    shares = around(partial, "tp")
    mixer_out = sum(share.astype(F32) for share in shares).astype(BF16)

    hiddens = expert_hidden(
        arrived, [w_gate, w_up, gate_r, up_r, gate_l, up_l, gate_f, up_f]
    )
    early, last = expert_down_early(hiddens, w_down, (down_0r, down_1r), (down_0l, down_1l))
    returning = expert_down_late(early, last, (down_0f, down_1f))
    returned = exchange(returning.reshape(ep_count, CAPACITY, model_width), EP)
    return (mixer_out, combine_rows(mix, returned.reshape(places, model_width)))


def solution(mesh):
    finer = Mesh(mesh.devices.reshape(8, 4, 2, mesh.shape["tp"]), ("ep_0", "ep_1", "ep_2", "tp"))
    placed = (
        P(EP, "tp"),
        P(EP, "tp"),
        P(EP, "tp"),
        P(EP, "tp"),
        P(EP, "tp"),
        P("tp"),
        P(EP, "tp"),
        P("tp"),
        P("tp", None),
        P(EP_TP, None),
        P(),
        P(EP_TP, None),
        P(EP_TP, None),
        P(EP, None, "tp"),
        P(EP, None, "tp"),
        P(EP, "tp", None),
    )

    return jax.shard_map(
        on_device,
        mesh=finer,
        in_specs=placed,
        out_specs=(P(EP_TP, None), P(EP_TP, None)),
        check_vma=False,
    )
```
